32 devices in a mesh: ep: 8 (over z, x), tp: 4 (over y, core).
Axes of the slice: x: 2, y: 2, z: 4, core: 2. Of those that a mesh axis runs over, the one named last changes fastest.
Arguments:
- mixer_input: bfloat16 [4096, 2048], P('ep', 'tp'), may hold values from -6 to 6
- mixer_gain: float32 [2048], replicated, may hold values from 0.1 to 1.9
- w_query: bfloat16 [2048, 1024], P(None, 'tp'), may hold values from -0.125 to 0.125
- w_key: bfloat16 [2048, 128], replicated, may hold values from -0.125 to 0.125
- w_value: bfloat16 [2048, 128], replicated, may hold values from -0.125 to 0.125
- query_gain: float32 [64], replicated, may hold values from 0.5 to 10
- key_gain: float32 [64], replicated, may hold values from 0.5 to 10
- sink_logit: float32 [16], P('tp'), may hold values from 1 to 5
- w_output: bfloat16 [1024, 2048], P('tp'), may hold values from -0.1875 to 0.1875
- expert_input: bfloat16 [1024, 2048], P('ep'), may hold values from -6 to 6
- expert_gain: float32 [2048], replicated, may hold values from 0.1 to 1.9
- route_ids: int32 [1024, 4], P('ep'), may hold values from 0 to 7, all different within a row; in each aligned block of 128 rows (0 to 127, 128 to 255, ...) at most 128 rows name the same one
- route_weight: float32 [1024, 4], P('ep'), may hold values from 0.2 to 1.2
- expert_gate: bfloat16 [8, 2048, 2048], P('ep', None, 'tp'), may hold values from -0.125 to 0.125
- expert_up: bfloat16 [8, 2048, 2048], P('ep', None, 'tp'), may hold values from -0.125 to 0.125
- expert_down: bfloat16 [8, 2048, 2048], P('ep', None, 'tp'), may hold values from -0.125 to 0.125
- shared_gate: bfloat16 [2048, 1024], P(None, 'tp'), may hold values from -0.125 to 0.125
- shared_up: bfloat16 [2048, 1024], P(None, 'tp'), may hold values from -0.125 to 0.125
- shared_down: bfloat16 [1024, 2048], P(None, 'tp'), may hold values from -0.1875 to 0.1875
Outputs:
- mixer_output: bfloat16 [4096, 2048], P('ep', 'tp')
- expert_output: bfloat16 [1024, 2048], P('ep', 'tp')
The draws below stay inside these ranges and needn't reach their ends.
Inputs may be any that keep to these rules, and one draw needn't show every extreme that they name: `route_ids`: each row names 4 different experts. In the rows of one index of ep (aligned blocks of 128 rows) no expert is named by more than 128 rows, a bound that some block reaches.
All inputs are finite; a program needn't handle non-finite values.
Results may differ from the reference program's by a relative error of at most 0.018.
The reference program's roundings to bfloat16 on the way count: a program that leaves them out, or rounds other values in their place, can miss the bound.
Values may be sent and summed in bfloat16 or wider, within the bound.
A program may use at most 64 MiB of HBM per device.

```python
import math
import jax
import jax.numpy as jnp
import numpy as np
from jax import lax

D = 2048
HEAD = 64
Q_HEADS = 16
KV_HEADS = 2
WINDOW = 128
TOK_B = 128
TOPK = 4
FF = 2048
SHARED_FF = 1024
EXPERTS = 8
CAP = 128
TOKENS_A = 4096
TOKENS_B = 1024
N_EP = 8


def gain_draw(key):
    return jax.random.uniform(key, (HEAD,), jnp.float32, 0.6, 1.6)


def draw_query_gain(key, part):
    return gain_draw(jax.random.fold_in(key, 11))


def draw_key_gain(key, part):
    return gain_draw(jax.random.fold_in(key, 23))


def level_of(rng, extent, shards, low, largest):
    loudness = 1.0
    for position, shards_of in shards:
        steps = jax.random.uniform(jax.random.fold_in(jax.random.fold_in(rng, 6), position), (shards_of,), jnp.float32, low / len(shards), largest / len(shards))
        loudness = loudness * jnp.repeat(jnp.exp(steps), extent[position] // shards_of).reshape((-1,) + (1,) * (len(extent) - 1 - position))
    return loudness


def deal_out(stream_key, own, number, rows, count, top, most, skew):
    ranking = jax.random.permutation(stream_key, count)
    heavy_load, ordinary = portions_of(count, rows * top, most, skew, True), portions_of(count, rows * top, most, skew, False)
    places = jnp.arange(count)

    def named(sizes, rotation):
        used = int((sizes > 0).sum())
        fixed = max(1, used // 4)
        shifted = fixed + (places - fixed + rotation * (used - fixed)) % max(1, count - fixed)
        return jnp.zeros((count,), jnp.int32).at[ranking[jnp.where(places < fixed, places, shifted)]].set(jnp.asarray(sizes, jnp.int32))

    sizes = jnp.where(number % 4 == 0, named(heavy_load, number // 4), named(ordinary, number - number // 4 - 1))
    mixed = jax.random.permutation(jax.random.fold_in(own, 3), count)
    donor, taker = mixed[0:count // 2 * 2:2], mixed[1:count // 2 * 2:2]
    room = jnp.minimum(sizes[donor] - 1, most - sizes[taker]) // 2
    room = jnp.where((donor == ranking[0]) | (taker == ranking[0]) | (sizes[taker] == 0), 0, jnp.maximum(room, 0))
    shifted = jax.random.randint(jax.random.fold_in(own, 4), (count // 2,), 0, 1 << 20) % (room + 1)
    sizes = sizes.at[donor].add(-shifted).at[taker].add(shifted)
    items = jnp.searchsorted(jnp.cumsum(sizes), jnp.arange(rows * top), side="right").astype(jnp.int32)
    listing = items.reshape(top, rows).T
    listing = listing[jax.random.permutation(jax.random.fold_in(own, 1), rows)]
    rotation = jax.random.randint(jax.random.fold_in(own, 2), (rows, 1), 0, top)
    return jnp.take_along_axis(listing, (jnp.arange(top)[None, :] + rotation) % top, axis=1)


def portions_of(count, total, limit, skew, full):
    loads = [(1 << 20) // math.isqrt(grade ** skew) + 1 for grade in range(1, count + 1)]
    largest = limit if full else min(limit, max(-(-total // count), total * loads[0] // sum(loads)))
    least = 1 if total - largest >= count - 1 else 0
    holding, spare = [largest] + [least] * (count - 1), total - largest - least * (count - 1)
    while spare > 0:
        movable = [i for i in range(1, count) if holding[i] < largest] or [i for i in range(1, count) if holding[i] < limit]
        mass, remaining = sum([loads[i] for i in movable]), spare
        for i in movable:
            more = min(limit - holding[i], max(1, remaining * loads[i] // mass), spare)
            holding[i] = holding[i] + more
            spare = spare - more
    return np.array(holding)


def centred(stream_key, extent, width, bound, split=(), kind=jnp.bfloat16):
    array = jax.random.normal(stream_key, extent, jnp.float32) * width
    if len(split) > 0:
        array = level_of(stream_key, extent, split, -0.22, 0.18) * array
    return jnp.clip(array, min=-bound, max=bound).astype(kind)


def setup_inputs(seed: int = 0) -> dict:
    streams_of = jax.random.split(jax.random.key(seed), 20)
    mixer_input = centred(streams_of[0], (TOKENS_A, D), 1.0, 6.0, ((0, 8), (1, 4)))
    mixer_gain = jnp.clip(1.0 + 0.18 * jax.random.normal(streams_of[1], (D,), jnp.float32), 0.1, 1.9)
    w_query = centred(streams_of[2], (D, Q_HEADS * HEAD), D ** -0.5, 0.125, ((1, 4),))
    w_key = centred(streams_of[3], (D, KV_HEADS * HEAD), D ** -0.5, 0.125)
    w_value = centred(streams_of[4], (D, KV_HEADS * HEAD), D ** -0.5, 0.125)
    query_gain = draw_query_gain(jax.random.fold_in(streams_of[19], 71), 0)
    key_gain = draw_key_gain(jax.random.fold_in(streams_of[19], 71), 0)
    sink_logit = jnp.clip(1.0 + 4.0 * jax.random.uniform(streams_of[7], (Q_HEADS,), jnp.float32) ** level_of(streams_of[7], (Q_HEADS,), ((0, 4),), -0.2, 0.2), 1.0, 5.0)
    w_output = centred(streams_of[8], (Q_HEADS * HEAD, D), (Q_HEADS * HEAD) ** -0.5, 0.1875, ((0, 4),))
    expert_input = centred(streams_of[9], (TOKENS_B, D), 1.0, 6.0, ((0, 8),))
    expert_gain = jnp.clip(1.0 + 0.18 * jax.random.normal(streams_of[10], (D,), jnp.float32), 0.1, 1.9)
    route_ids_keys = jax.random.split(jax.random.fold_in(streams_of[11], 1), TOKENS_B // TOK_B)
    route_ids_turns = jax.random.permutation(jax.random.fold_in(streams_of[11], 3), TOKENS_B // TOK_B)
    route_ids = jax.vmap(lambda own, number: deal_out(jax.random.fold_in(streams_of[11], 2), own, number, TOK_B, EXPERTS, TOPK, CAP, 1))(route_ids_keys, route_ids_turns).reshape((TOKENS_B, TOPK))
    route_weight = jnp.clip(0.2 + 1 * jax.random.uniform(streams_of[12], (TOKENS_B, TOPK), jnp.float32) ** level_of(streams_of[12], (TOKENS_B, TOPK), ((0, 8),), -0.2, 0.2), 0.2, 1.2)
    expert_gate = centred(streams_of[13], (EXPERTS, D, FF), D ** -0.5, 0.125, ((0, 8), (2, 4)))
    expert_up = centred(streams_of[14], (EXPERTS, D, FF), D ** -0.5, 0.125, ((0, 8), (2, 4)))
    expert_down = centred(streams_of[15], (EXPERTS, FF, D), FF ** -0.5, 0.125, ((0, 8), (2, 4)))
    shared_gate = centred(streams_of[16], (D, SHARED_FF), D ** -0.5, 0.125, ((1, 4),))
    shared_up = centred(streams_of[17], (D, SHARED_FF), D ** -0.5, 0.125, ((1, 4),))
    shared_down = centred(streams_of[18], (SHARED_FF, D), SHARED_FF ** -0.5, 0.1875, ((1, 4),))
    return dict(mixer_input=mixer_input, mixer_gain=mixer_gain, w_query=w_query, w_key=w_key, w_value=w_value, query_gain=query_gain, key_gain=key_gain, sink_logit=sink_logit, w_output=w_output, expert_input=expert_input, expert_gain=expert_gain, route_ids=route_ids, route_weight=route_weight, expert_gate=expert_gate, expert_up=expert_up, expert_down=expert_down, shared_gate=shared_gate, shared_up=shared_up, shared_down=shared_down)


EPSILON = 1e-06

def head_norm(matrix, gain_vector):
    return matrix * lax.rsqrt(lax.optimization_barrier(jnp.mean(matrix * matrix, axis=-1, keepdims=True)) + EPSILON) * gain_vector

def band_attend(queries, keys_own, values_own, keys_prev, values_prev, sink_logit, first_row):
    row_count = queries.shape[0]
    head_count = queries.shape[1]
    blocks = row_count // WINDOW
    keys_all = jnp.concatenate([keys_prev, keys_own], axis=0)
    values_all = jnp.concatenate([values_prev, values_own], axis=0)
    key_band = jnp.concatenate([keys_all[:row_count].reshape(blocks, WINDOW, HEAD), keys_own.reshape(blocks, WINDOW, HEAD)], axis=1)
    value_band = jnp.concatenate([values_all[:row_count].reshape(blocks, WINDOW, HEAD), values_own.reshape(blocks, WINDOW, HEAD)], axis=1)
    query_blocks = queries.reshape(blocks, WINDOW, head_count, HEAD)
    scores = jnp.einsum('nqhd,nkd->nhqk', query_blocks.astype(jnp.float32), key_band.astype(jnp.float32)) * HEAD ** (-0.5)
    query_idx = jnp.arange(WINDOW, dtype=jnp.int32)[:, None]
    key_idx = jnp.arange(2 * WINDOW, dtype=jnp.int32)[None, :]
    relative = query_idx + WINDOW - key_idx
    block_idx = jnp.arange(blocks, dtype=jnp.int32)[:, None, None]
    key_pos = first_row + block_idx * WINDOW - WINDOW + key_idx[None]
    allowed = ((relative >= 0) & (relative < WINDOW))[None] & (key_pos >= 0)
    allowed = allowed[:, None]
    masked = jnp.where(allowed, scores, -jnp.inf)
    sink_column = sink_logit.astype(jnp.float32).reshape(1, head_count, 1, 1)
    peak_score = jnp.maximum(lax.optimization_barrier(jnp.max(masked, axis=-1, keepdims=True)), sink_column)
    exponent = jnp.exp(masked - peak_score)
    denominator = lax.optimization_barrier(jnp.sum(exponent, axis=-1, keepdims=True)) + jnp.exp(sink_column - peak_score)
    probability = (exponent / denominator).astype(jnp.bfloat16)
    mixed_rows = jnp.einsum('nhqk,nkd->nqhd', probability.astype(jnp.float32), value_band.astype(jnp.float32))
    return mixed_rows.reshape(row_count, head_count * HEAD).astype(jnp.bfloat16)

def reference(mixer_input, mixer_gain, w_query, w_key, w_value, query_gain, key_gain, sink_logit, w_output, expert_input, expert_gain, route_ids, route_weight, expert_gate, expert_up, expert_down, shared_gate, shared_up, shared_down):
    rows_float = mixer_input.astype(jnp.float32)
    scaled = (rows_float * mixer_gain).astype(jnp.bfloat16)
    inv_rms = lax.rsqrt(lax.optimization_barrier(jnp.mean(rows_float * rows_float, axis=-1, keepdims=True)) + EPSILON)
    query_raw = jnp.dot(scaled, w_query, preferred_element_type=jnp.float32)
    key_raw = jnp.dot(scaled, w_key, preferred_element_type=jnp.float32)
    value_raw = jnp.dot(scaled, w_value, preferred_element_type=jnp.float32)
    queries = head_norm(query_raw.reshape(TOKENS_A, Q_HEADS, HEAD), query_gain).astype(jnp.bfloat16)
    keys_all = head_norm(key_raw.reshape(TOKENS_A, KV_HEADS, HEAD), key_gain).astype(jnp.bfloat16)
    values_all = (value_raw * inv_rms).astype(jnp.bfloat16).reshape(TOKENS_A, KV_HEADS, HEAD)
    group_size = Q_HEADS // KV_HEADS
    zero_rows = jnp.zeros((WINDOW, HEAD), jnp.bfloat16)

    def one_head(head_index):
        kv_index = head_index // group_size
        head_query = queries[:, head_index][:, None, :]
        head_keys = keys_all[:, kv_index]
        head_values = values_all[:, kv_index]
        sink_one = sink_logit[head_index].reshape(1)
        return band_attend(head_query, head_keys, head_values, zero_rows, zero_rows, sink_one, jnp.int32(0))
    per_head = lax.map(one_head, jnp.arange(Q_HEADS, dtype=jnp.int32))
    attended = jnp.transpose(per_head, (1, 0, 2)).reshape(TOKENS_A, Q_HEADS * HEAD)
    mixer_output = jnp.dot(attended, w_output, preferred_element_type=jnp.float32).astype(jnp.bfloat16)
    expert_float = expert_input.astype(jnp.float32)
    normed = (expert_float * lax.rsqrt(lax.optimization_barrier(jnp.mean(expert_float * expert_float, axis=-1, keepdims=True)) + EPSILON) * expert_gain).astype(jnp.bfloat16)
    shared_hidden = (jax.nn.silu(jnp.dot(normed, shared_gate, preferred_element_type=jnp.float32)) * jnp.dot(normed, shared_up, preferred_element_type=jnp.float32)).astype(jnp.bfloat16)
    shared_out = jnp.dot(shared_hidden, shared_down, preferred_element_type=jnp.float32)
    ids_blocks = route_ids.reshape(N_EP, TOK_B * TOPK)
    onehot = (ids_blocks[:, :, None] == jnp.arange(EXPERTS, dtype=jnp.int32)[None, None, :]).astype(jnp.int32)
    earlier = jnp.cumsum(onehot, axis=1) - onehot
    slot_index = lax.optimization_barrier(jnp.sum(earlier * onehot, axis=-1))
    block_ids = jnp.arange(N_EP, dtype=jnp.int32)[:, None]
    slot_column = (block_ids * CAP + slot_index).astype(jnp.int32)
    token_ids = (block_ids * TOK_B + jnp.arange(TOK_B * TOPK, dtype=jnp.int32)[None] // TOPK).astype(jnp.int32)
    slot_table = jnp.full((EXPERTS, N_EP * CAP), TOKENS_B, jnp.int32).at[ids_blocks, slot_column].set(token_ids)
    padded = jnp.concatenate([normed, jnp.zeros((1, D), jnp.bfloat16)], axis=0)

    def one_expert(expert_index):
        chosen = padded[slot_table[expert_index]]
        gate_pre = jnp.dot(chosen, expert_gate[expert_index], preferred_element_type=jnp.float32)
        up_pre = jnp.dot(chosen, expert_up[expert_index], preferred_element_type=jnp.float32)
        hidden = (jax.nn.silu(gate_pre) * up_pre).astype(jnp.bfloat16)
        return jnp.dot(hidden, expert_down[expert_index], preferred_element_type=jnp.float32).astype(jnp.bfloat16)
    routed = lax.map(one_expert, jnp.arange(EXPERTS, dtype=jnp.int32))
    picked = routed[ids_blocks, slot_column].reshape(TOKENS_B, TOPK, D).astype(jnp.float32)
    expert_output = (shared_out + lax.optimization_barrier(jnp.sum(picked * route_weight[:, :, None], axis=1))).astype(jnp.bfloat16)
    return (mixer_output, expert_output)
```

```python
import functools

import jax
import jax.numpy as jnp
from jax import lax
from jax.experimental import pallas as pl
from jax.experimental.pallas import tpu as pltpu
from jax.sharding import PartitionSpec as P

D = 2048
HEAD = 64
KV_HEADS = 2
WINDOW = 128
TOPK = 4


EPSILON = 1e-06


def from_behind(value, axis, steps):
    count = lax.axis_size(axis)
    first, last = (max(0, -steps), min(count, count - steps))
    return lax.ppermute(value, axis, [(source, source + steps) for source in range(first, last)])


def head_norm(matrix, gain_vector):
    return (
        matrix
        * lax.rsqrt(jnp.mean(matrix * matrix, axis=-1, keepdims=True) + EPSILON)
        * gain_vector
    )


def band_attend(queries, keys_own, values_own, keys_prev, values_prev, sink_logit, first_row):
    row_count = queries.shape[0]
    head_count = queries.shape[1]
    blocks = row_count // WINDOW
    keys_all = jnp.concatenate([keys_prev, keys_own], axis=0)
    values_all = jnp.concatenate([values_prev, values_own], axis=0)
    key_band = jnp.concatenate(
        [
            keys_all[:row_count].reshape(blocks, WINDOW, HEAD),
            keys_own.reshape(blocks, WINDOW, HEAD),
        ],
        axis=1,
    )
    value_band = jnp.concatenate(
        [
            values_all[:row_count].reshape(blocks, WINDOW, HEAD),
            values_own.reshape(blocks, WINDOW, HEAD),
        ],
        axis=1,
    )
    query_blocks = queries.reshape(blocks, WINDOW, head_count, HEAD)
    scores = jnp.einsum(
        "nqhd,nkd->nhqk", query_blocks, key_band, preferred_element_type=jnp.float32
    ) * HEAD ** (-0.5)
    query_idx = jnp.arange(WINDOW, dtype=jnp.int32)[:, None]
    key_idx = jnp.arange(2 * WINDOW, dtype=jnp.int32)[None, :]
    relative = query_idx + WINDOW - key_idx
    block_idx = jnp.arange(blocks, dtype=jnp.int32)[:, None, None]
    key_pos = first_row + block_idx * WINDOW - WINDOW + key_idx[None]
    allowed = ((relative >= 0) & (relative < WINDOW))[None] & (key_pos >= 0)
    allowed = allowed[:, None]
    masked = jnp.where(allowed, scores, -jnp.inf)
    sink_column = sink_logit.reshape(1, head_count, 1, 1)
    peak_score = jnp.maximum(jnp.max(masked, axis=-1, keepdims=True), sink_column)
    exponent = jnp.exp(masked - peak_score)
    denominator = jnp.sum(exponent, axis=-1, keepdims=True) + jnp.exp(sink_column - peak_score)
    probability = (exponent / denominator).astype(jnp.bfloat16)
    mixed_rows = jnp.einsum(
        "nhqk,nkd->nqhd", probability, value_band, preferred_element_type=jnp.float32
    )
    return mixed_rows.reshape(row_count, head_count * HEAD).astype(jnp.bfloat16)


def shards_routed(
    mixer_input,
    mixer_gain,
    w_query,
    w_key,
    w_value,
    query_gain,
    key_gain,
    sink_logit,
    w_output,
    expert_input,
    expert_gain,
    route_ids,
    route_weight,
    expert_gate,
    expert_up,
    expert_down,
    shared_gate,
    shared_up,
    shared_down,
):
    tp_count = lax.axis_size("tp")
    ep_count = lax.axis_size("ep")
    rows_local = mixer_input.shape[0]
    heads_local = w_query.shape[1] // HEAD
    kv_index = lax.axis_index("tp") // (tp_count // KV_HEADS)
    key_cols = lax.dynamic_slice_in_dim(w_key, kv_index * HEAD, HEAD, 1)
    value_cols = lax.dynamic_slice_in_dim(w_value, kv_index * HEAD, HEAD, 1)
    portion_float = lax.all_gather(mixer_input, "tp", axis=1, tiled=True).astype(jnp.float32)
    scaled = (portion_float * mixer_gain).astype(jnp.bfloat16)
    query_raw = jnp.dot(scaled, w_query, preferred_element_type=jnp.float32)
    key_raw = jnp.dot(scaled, key_cols, preferred_element_type=jnp.float32)
    value_raw = jnp.dot(scaled, value_cols, preferred_element_type=jnp.float32)
    squares = jnp.sum(portion_float * portion_float, axis=1)
    inv_rms = lax.rsqrt(squares / D + EPSILON)[:, None]
    queries = head_norm(query_raw.reshape(rows_local, heads_local, HEAD), query_gain).astype(
        jnp.bfloat16
    )
    keys_own = head_norm(key_raw, key_gain).astype(jnp.bfloat16)
    values_own = (value_raw * inv_rms).astype(jnp.bfloat16)
    keys_prev, values_prev = from_behind(
        (keys_own[rows_local - WINDOW :], values_own[rows_local - WINDOW :]), "ep", 1
    )
    first_row = lax.axis_index("ep") * rows_local
    attended = band_attend(
        queries, keys_own, values_own, keys_prev, values_prev, sink_logit, first_row
    )
    head_partial = jnp.dot(attended, w_output, preferred_element_type=jnp.float32)
    mixer_output = lax.psum_scatter(
        head_partial.astype(jnp.bfloat16), "tp", scatter_dimension=1, tiled=True
    )
    tokens_local = expert_input.shape[0]
    expert_float = expert_input.astype(jnp.float32)
    normed = (
        expert_float
        * lax.rsqrt(jnp.mean(expert_float * expert_float, axis=-1, keepdims=True) + EPSILON)
        * expert_gain
    ).astype(jnp.bfloat16)
    capacity = 2 * tokens_local * TOPK // ep_count
    flat_ids = route_ids.reshape(-1)
    onehot = (flat_ids[:, None] == jnp.arange(ep_count, dtype=jnp.int32)[None, :]).astype(jnp.int32)
    earlier = jnp.cumsum(onehot, axis=0) - onehot
    slot_index = jnp.sum(earlier * onehot, axis=-1)
    slot_column = flat_ids * capacity + slot_index
    token_ids = jnp.arange(tokens_local * TOPK, dtype=jnp.int32) // TOPK
    slot_table = (
        jnp.full((ep_count * capacity,), tokens_local, jnp.int32).at[slot_column].set(token_ids)
    )
    col_width = expert_down.shape[2]
    arrived_rows = ep_count * capacity
    own_columns = lax.dynamic_slice_in_dim(normed, lax.axis_index("tp") * col_width, col_width, 1)
    padded = jnp.concatenate([own_columns, jnp.zeros((1, col_width), jnp.bfloat16)], axis=0)
    outgoing = padded[slot_table].reshape(ep_count, capacity, col_width)
    arrived = lax.all_to_all(outgoing, "ep", split_axis=0, concat_axis=0, tiled=True).reshape(
        arrived_rows, col_width
    )
    portion = lax.all_gather(arrived, "tp", axis=1, tiled=True)
    gate_part = expert_gate[0]
    up_part = expert_up[0]
    gate_pre = jnp.dot(portion, gate_part, preferred_element_type=jnp.float32)
    up_pre = jnp.dot(portion, up_part, preferred_element_type=jnp.float32)
    routed_hidden = (jax.nn.silu(gate_pre) * up_pre).astype(jnp.bfloat16)
    shared_hidden = (
        jax.nn.silu(jnp.dot(normed, shared_gate, preferred_element_type=jnp.float32))
        * jnp.dot(normed, shared_up, preferred_element_type=jnp.float32)
    ).astype(jnp.bfloat16)
    routed_part = expert_down[0]
    routed_sum = jnp.dot(
        lax.all_gather(routed_hidden, "tp", axis=1, tiled=True),
        routed_part,
        preferred_element_type=jnp.float32,
    )
    shared_sum = jnp.dot(
        lax.all_gather(shared_hidden, "tp", axis=1, tiled=True),
        shared_down,
        preferred_element_type=jnp.float32,
    )
    expert_rows = routed_sum.astype(jnp.bfloat16).reshape(ep_count, capacity, col_width)
    returned = lax.all_to_all(expert_rows, "ep", split_axis=0, concat_axis=0, tiled=True).reshape(
        arrived_rows, col_width
    )
    picked = returned[slot_column].reshape(tokens_local, TOPK, col_width).astype(jnp.float32)
    expert_output = (shared_sum + jnp.sum(picked * route_weight[:, :, None], axis=1)).astype(
        jnp.bfloat16
    )
    return (mixer_output, expert_output)


CHUNKS = 2
VMEM_LIMIT = 62 * 1024 * 1024
PARTS_BACK = 4
COLUMNS_X = 2


def place_of(slot, ring):
    half = ring // 2
    return 0 if slot == 0 else 2 * slot - 1 if slot <= half else 2 * (ring - slot)


def ring_position(index, ring):
    row, side = index // COLUMNS_X, index % COLUMNS_X
    return row + side * (ring - 1 - 2 * row)


def ring_index(position, ring):
    side = position // (ring // COLUMNS_X)
    return 2 * position + side * (2 * ring - 1 - 4 * position)


def remote(source, target, send, receive, device):
    return pltpu.make_async_remote_copy(
        src_ref=source,
        dst_ref=target,
        send_sem=send,
        recv_sem=receive,
        device_id=device,
        device_id_type=pl.DeviceIdType.MESH,
    )


def limit(direction, chunk, ring):
    return ring // 2 if direction == chunk else ring // 2 - 1


def slot_at(direction, distance, ring):
    return distance if direction == 0 else ring - distance


def layer_kernel(
    ring,
    rows_hbm,
    gain_hbm,
    ids_hbm,
    weight_hbm,
    mixer_hbm,
    mixer_gain_hbm,
    query_gain_hbm,
    key_gain_hbm,
    sink_hbm,
    gate_hbm,
    up_hbm,
    shared_gate_hbm,
    shared_up_hbm,
    query_hbm,
    key_hbm,
    value_hbm,
    w_out_hbm,
    down_hbm,
    shared_down_hbm,
    mixer_result,
    expert_result,
    rows_v,
    gain_v,
    ids_v,
    weight_v,
    mixer_gain_v,
    query_gain_v,
    key_gain_v,
    sink_v,
    mixer_all,
    hidden_all,
    shared_all,
    att_all,
    dense_all,
    tok,
    gate_v,
    up_v,
    shared_gate_v,
    shared_up_v,
    qkv_v,
    down_v,
    shared_down_v,
    out_cols,
    out_stage,
    scaled_v,
    heads_v,
    band_v,
    bias_v,
    ready,
    going,
    coming,
    mixer_v,
    expert_v,
    load_sem,
    store_sem,
    ring_send,
    ring_recv,
    sib_send,
    sib_recv,
    mix_send,
    mix_recv,
    hid_send,
    hid_recv,
    sh_send,
    sh_recv,
    att_send,
    att_recv,
    dense_send,
    dense_recv,
    halo_send,
    halo_recv,
    wcol_send,
    wcol_recv,
    wring_send,
    wring_recv,
    back_send,
    back_recv,
):
    scope = jax.named_scope
    f32, bf16 = jnp.float32, jnp.bfloat16
    index, part = lax.axis_index("ep"), lax.axis_index("tp")
    far, core = part // 2, part % 2
    position = ring_position(index, ring)
    peer_index = [ring_index((position + k) % ring, ring) for k in range(ring)]
    peers = [(peer_index[k], part) for k in range(1, ring)]
    ahead, behind = peers[0], peers[-1]
    sib_part = 2 * far + 1 - core
    across_part = 2 * (1 - far) + core
    corner_part = 2 * (1 - far) + 1 - core
    sibling, across = (index, sib_part), (index, across_part)
    block, width = rows_v.shape
    half_width = width // 2
    piece = block // CHUNKS
    steps = ring // 2
    parts, rows_local, mixer_cols = mixer_all.shape
    pieces = rows_local // WINDOW
    out_width = down_v.shape[1]
    inner = hidden_all.shape[2]
    shared_width = shared_all.shape[2]
    head_rows = out_cols.shape[1]
    share_rows = head_rows // ring
    share_piece = share_rows // CHUNKS

    barrier = pltpu.get_barrier_semaphore()
    for device in peers + [sibling, across]:
        pl.semaphore_signal(barrier, inc=1, device_id=device, device_id_type=pl.DeviceIdType.MESH)

    pending, stores = [], []

    def start(copy):
        copy.start()
        pending.append(copy)

    loads = {}

    def load(name, source, target):
        loads[name] = pltpu.make_async_copy(source, target, load_sem.at[len(loads)])
        loads[name].start()

    own_cols = pl.ds(pl.multiple_of(part * out_width, out_width), out_width)
    load("rows", rows_hbm, rows_v)
    load("gain", gain_hbm, gain_v)
    load("mixer", mixer_hbm, mixer_all.at[part])
    load("shared_gate", shared_gate_hbm, shared_gate_v)
    load("shared_up", shared_up_hbm, shared_up_v)
    load("gate", gate_hbm, gate_v)
    load("up", up_hbm, up_v)
    load("ids", ids_hbm, ids_v)
    load("weight", weight_hbm, weight_v)
    load("mixer_gain", mixer_gain_hbm, mixer_gain_v)
    load("query_gain", query_gain_hbm, query_gain_v)
    load("key_gain", key_gain_hbm, key_gain_v)
    load("sink", sink_hbm, sink_v)
    load("query", query_hbm, qkv_v.at[:, pl.ds(0, query_hbm.shape[1])])
    load("key", key_hbm, qkv_v.at[:, pl.ds(query_hbm.shape[1], key_hbm.shape[1])])
    load(
        "value",
        value_hbm,
        qkv_v.at[:, pl.ds(query_hbm.shape[1] + key_hbm.shape[1], value_hbm.shape[1])],
    )
    load("out_own", w_out_hbm.at[:, own_cols], out_cols.at[part])
    load("down", down_hbm, down_v)
    load("shared_down", shared_down_hbm, shared_down_v)

    relative = (
        lax.broadcasted_iota(jnp.int32, (WINDOW, 2 * WINDOW), 0)
        + WINDOW
        - lax.broadcasted_iota(jnp.int32, (WINDOW, 2 * WINDOW), 1)
    )
    bias_v[...] = jnp.where((relative >= 0) & (relative < WINDOW), 0.0, -jnp.inf)
    low = lax.broadcasted_iota(jnp.int32, (WINDOW, 2 * HEAD), 1) < HEAD

    with scope("norm"):
        loads["rows"].wait()
        loads["gain"].wait()
        value = rows_v[...].astype(f32)
        normed = (
            value
            * lax.rsqrt(jnp.mean(value * value, axis=-1, keepdims=True) + EPSILON)
            * gain_v[...]
        ).astype(bf16)
        tok[0, pl.ds(0, block), :] = normed[:, :half_width]
        tok[1, pl.ds(0, block), :] = normed[:, half_width:]
        loads["mixer"].wait()

    with scope("greet"):
        pl.semaphore_wait(barrier, ring + 1)

    def chunk_ref(half, slot, chunk):
        return tok.at[half, pl.ds(place_of(slot, ring) * block + chunk * piece, piece), :]

    def hop(direction, distance, chunk):
        start(
            remote(
                chunk_ref(core, slot_at(direction, distance - 1, ring) % ring, chunk),
                chunk_ref(core, slot_at(direction, distance, ring), chunk),
                ring_send.at[direction, distance, chunk],
                ring_recv.at[direction, distance, chunk],
                ahead if direction == 0 else behind,
            )
        )

    def arrive(distance, chunk):
        for direction in range(2):
            if distance > limit(direction, chunk, ring):
                continue
            here = chunk_ref(core, slot_at(direction, distance, ring), chunk)
            at = (direction, distance, chunk)
            remote(here, here, ring_send.at[at], ring_recv.at[at], sibling).wait_recv()
            if distance < limit(direction, chunk, ring):
                hop(direction, distance + 1, chunk)
            start(remote(here, here, sib_send.at[at], sib_recv.at[at], sibling))

    def swapped(distance):
        for chunk in range(CHUNKS):
            for direction in range(2):
                if distance > limit(direction, chunk, ring):
                    continue
                there = chunk_ref(1 - core, slot_at(direction, distance, ring), chunk)
                at = (direction, distance, chunk)
                remote(there, there, sib_send.at[at], sib_recv.at[at], sibling).wait_recv()

    class Share:
        def __init__(self, view, send, receive):
            self.view, self.send, self.receive = view, send, receive

        def copy(self, owner, i, path, device):
            here = self.view(owner, i)
            return remote(here, here, self.send.at[path, i], self.receive.at[path, i], device)

        def to_across(self, i):
            start(self.copy(part, i, 0, across))

        def to_sibling(self, i):
            start(self.copy(part, i, 1, sibling))

        def both(self, i):
            self.to_across(i)
            self.to_sibling(i)

        def forward(self, i):
            self.copy(across_part, i, 0, sibling).wait_recv()
            start(self.copy(across_part, i, 2, sibling))

        def rest(self, i):
            self.copy(sib_part, i, 1, sibling).wait_recv()
            self.copy(corner_part, i, 2, sibling).wait_recv()

    mixer = Share(
        lambda owner, i: mixer_all.at[owner, pl.ds(i * WINDOW, WINDOW), :], mix_send, mix_recv
    )
    shared = Share(lambda owner, i: shared_all.at[owner], sh_send, sh_recv)
    hidden = Share(
        lambda owner, i: hidden_all.at[owner, pl.ds(place_of(i, ring) * block, block), :],
        hid_send,
        hid_recv,
    )
    att = Share(
        lambda owner, i: att_all.at[owner, pl.ds(i * WINDOW, WINDOW), :], att_send, att_recv
    )

    for chunk in range(CHUNKS):
        for direction in range(2):
            hop(direction, 1, chunk)
    mixer.both(3)
    mixer.both(2)
    mixer.to_sibling(1)
    mixer.to_sibling(0)

    loads["ids"].wait()
    loads["weight"].wait()
    experts = lax.broadcasted_iota(jnp.int32, (ring, block), 0)
    dense = jnp.zeros((ring, block), f32)
    for k in range(TOPK):
        dense = dense + jnp.where(ids_v[k : k + 1, :] == experts, weight_v[k : k + 1, :], 0.0)
    dense_all[0] = dense
    for k in range(1, ring):
        start(
            remote(
                dense_all.at[0], dense_all.at[k], dense_send.at[k], dense_recv.at[k], peers[k - 1]
            )
        )

    def product(first, count, weights, columns):
        lower = tok[0, pl.ds(first, count), :]
        upper = tok[1, pl.ds(first, count), :]
        return jnp.dot(
            lower, weights[pl.ds(0, half_width), columns], preferred_element_type=f32
        ) + jnp.dot(
            upper, weights[pl.ds(half_width, half_width), columns], preferred_element_type=f32
        )

    with scope("c_shared"):
        loads["shared_gate"].wait()
        loads["shared_up"].wait()
        everything = pl.ds(0, shared_width)
        shared_all[part] = (
            jax.nn.silu(product(0, block, shared_gate_v, everything))
            * product(0, block, shared_up_v, everything)
        ).astype(bf16)
        shared.both(0)

    tile = 256

    def compute(slots):
        first = min(place_of(slot, ring) for slot in slots) * block
        count = len(slots) * block

        def one(j, carry):
            columns = pl.ds(pl.multiple_of(j * tile, tile), tile)
            hidden_all[part, pl.ds(first, count), columns] = (
                jax.nn.silu(product(first, count, gate_v, columns))
                * product(first, count, up_v, columns)
            ).astype(bf16)
            return carry

        lax.fori_loop(0, inner // tile, one, 0)
        for slot in slots:
            hidden.both(slot)

    def project(i):
        rows = pl.ds(i * WINDOW, WINDOW)
        mixer.rest(i)
        squares = jnp.zeros((WINDOW, 1), f32)
        for owner in range(parts):
            columns = pl.ds(owner * mixer_cols, mixer_cols)
            value = mixer_all[owner, rows, :].astype(f32)
            squares = squares + jnp.sum(value * value, axis=1, keepdims=True)
            scaled_v[:, columns] = (value * mixer_gain_v[:, columns]).astype(bf16)
        raw = jnp.dot(scaled_v[...], qkv_v[...], preferred_element_type=f32)
        lanes = 2 * HEAD
        heads = heads_v.shape[0]
        gain = query_gain_v[...] * HEAD ** (-0.5)
        gain = jnp.concatenate([gain, gain], axis=1)
        for pair in range(heads // 2):
            two = raw[:, pair * lanes : (pair + 1) * lanes]
            square = two * two
            first_sum = jnp.sum(jnp.where(low, square, 0.0), axis=1, keepdims=True)
            second_sum = jnp.sum(jnp.where(low, 0.0, square), axis=1, keepdims=True)
            inverse = lax.rsqrt(jnp.where(low, first_sum, second_sum) / HEAD + EPSILON)
            two = two * inverse * gain
            heads_v[2 * pair, rows, :] = jnp.where(low, two, 0.0).astype(bf16)
            heads_v[2 * pair + 1, rows, :] = jnp.where(low, 0.0, two).astype(bf16)
        queries_end = heads * HEAD
        second = part // (parts // KV_HEADS)
        mine = low == (second == 0)

        def twice(columns):
            return jnp.where(mine, columns, pltpu.roll(columns, HEAD, 1))

        key = twice(raw[:, queries_end : queries_end + lanes])
        gain = jnp.concatenate([key_gain_v[...], key_gain_v[...]], axis=1)
        key = key * lax.rsqrt(jnp.mean(key * key, axis=1, keepdims=True) + EPSILON) * gain
        val = twice(raw[:, queries_end + lanes : queries_end + 2 * lanes])
        val = val * lax.rsqrt(squares / D + EPSILON)
        band_v[pl.ds(WINDOW + i * WINDOW, WINDOW), :] = jnp.concatenate(
            [key, val], axis=1
        ).astype(bf16)

    halo = band_v.at[pl.ds(0, WINDOW), :]

    def send_halo():
        start(
            remote(
                band_v.at[pl.ds(rows_local, WINDOW), :],
                halo,
                halo_send.at[0],
                halo_recv.at[0],
                ((index + 1) % ring, part),
            )
        )

    def wait_halo():
        remote(halo, halo, halo_send.at[0], halo_recv.at[0], sibling).wait_recv()

    def attend(i):
        rows = pl.ds(i * WINDOW, WINDOW)
        keys = band_v[pl.ds(i * WINDOW, 2 * WINDOW), pl.ds(0, 2 * HEAD)]
        values = band_v[pl.ds(i * WINDOW, 2 * WINDOW), pl.ds(2 * HEAD, 2 * HEAD)]
        bias = bias_v[...]
        if i == 0:
            before = lax.broadcasted_iota(jnp.int32, (WINDOW, 2 * WINDOW), 1) < WINDOW
            bias = jnp.where(before & (index == 0), -jnp.inf, bias)
        mixed = []
        for head in range(heads_v.shape[0]):
            scores = lax.dot_general(
                heads_v[head, rows, :],
                keys,
                (((1,), (1,)), ((), ())),
                preferred_element_type=f32,
            )
            masked = scores + bias
            sink = sink_v[:, head : head + 1]
            peak = jnp.maximum(jnp.max(masked, axis=1, keepdims=True), sink)
            exponent = jnp.exp(masked - peak)
            denominator = jnp.sum(exponent, axis=1, keepdims=True) + jnp.exp(sink - peak)
            probability = (exponent * (1.0 / denominator)).astype(bf16)
            mixed.append(jnp.dot(probability, values, preferred_element_type=f32))
        for pair in range(len(mixed) // 2):
            att_all[part, rows, pl.ds(pair * 2 * HEAD, 2 * HEAD)] = jnp.where(
                low, mixed[2 * pair], mixed[2 * pair + 1]
            ).astype(bf16)

    chip_cols = 2 * out_width

    def spread_columns():
        start(
            remote(
                w_out_hbm.at[:, pl.ds(pl.multiple_of(sib_part * out_width, out_width), out_width)],
                out_cols.at[part],
                wcol_send.at[0],
                wcol_recv.at[0],
                sibling,
            )
        )
        mine = pl.ds(pl.multiple_of(index * share_rows, share_rows), share_rows)
        start(
            remote(
                w_out_hbm.at[
                    mine, pl.ds(pl.multiple_of((1 - far) * chip_cols, chip_cols), chip_cols)
                ],
                out_stage.at[mine, :],
                wcol_send.at[1],
                wcol_recv.at[1],
                across,
            )
        )

    def stage_ref(slot, chunk):
        owner = peer_index[(ring - slot) % ring]
        first = owner * share_rows + chunk * share_piece
        return out_stage.at[pl.ds(pl.multiple_of(first, share_piece), share_piece), :]

    def column_hop(direction, distance, chunk):
        here = stage_ref(slot_at(direction, distance - 1, ring) % ring, chunk)
        at = (direction, distance, chunk)
        start(
            remote(
                here,
                here,
                wring_send.at[at],
                wring_recv.at[at],
                ahead if direction == 0 else behind,
            )
        )

    def column_start():
        mine = out_stage.at[pl.ds(pl.multiple_of(index * share_rows, share_rows), share_rows), :]
        remote(mine, mine, wcol_send.at[1], wcol_recv.at[1], across).wait_recv()
        for chunk in range(CHUNKS):
            for direction in range(2):
                column_hop(direction, 1, chunk)

    def column_arrive(distance):
        for chunk in range(CHUNKS):
            for direction in range(2):
                if distance > limit(direction, chunk, ring):
                    continue
                here = stage_ref(slot_at(direction, distance, ring), chunk)
                at = (direction, distance, chunk)
                remote(here, here, wring_send.at[at], wring_recv.at[at], sibling).wait_recv()
                if distance < limit(direction, chunk, ring):
                    column_hop(direction, distance + 1, chunk)

    def column_swap():
        start(
            remote(
                out_stage.at[
                    :, pl.ds(pl.multiple_of((1 - core) * out_width, out_width), out_width)
                ],
                out_cols.at[across_part],
                wcol_send.at[2],
                wcol_recv.at[2],
                sibling,
            )
        )

    def column_wait():
        loads["out_own"].wait()
        for i, owner in ((0, sib_part), (2, corner_part)):
            here = out_cols.at[owner]
            remote(here, here, wcol_send.at[i], wcol_recv.at[i], sibling).wait_recv()

    def finish_mixer(i):
        rows = pl.ds(i * WINDOW, WINDOW)
        att.rest(i)
        total = jnp.dot(
            att_all[across_part, rows, :],
            out_stage[:, pl.ds(pl.multiple_of(core * out_width, out_width), out_width)],
            preferred_element_type=f32,
        )
        for owner in (part, sib_part, corner_part):
            total = total + jnp.dot(
                att_all[owner, rows, :], out_cols[owner], preferred_element_type=f32
            )
        mixer_v[rows, :] = total.astype(bf16)
        stores.append(
            pltpu.make_async_copy(mixer_v.at[rows, :], mixer_result.at[rows, :], store_sem.at[i])
        )
        stores[-1].start()

    diagonal = lax.broadcasted_iota(jnp.int32, (block, block), 0) == lax.broadcasted_iota(
        jnp.int32, (block, block), 1
    )

    def weight_column(slot):
        row = dense_all[slot, pl.ds(index, 1), :]
        return jnp.sum(jnp.where(diagonal, row, 0.0), axis=1, keepdims=True)

    def weighted(slots):
        for slot in slots:
            hidden.rest(slot)
        first = min(place_of(slot, ring) for slot in slots) * block
        count = len(slots) * block
        total = jnp.dot(
            hidden_all[0, pl.ds(first, count), :],
            down_v[pl.ds(0, inner), :],
            preferred_element_type=f32,
        )
        for owner in range(1, parts):
            total = total + jnp.dot(
                hidden_all[owner, pl.ds(first, count), :],
                down_v[pl.ds(owner * inner, inner), :],
                preferred_element_type=f32,
            )
        rounded = total.astype(bf16).astype(f32)
        ordered = sorted(slots, key=lambda slot: place_of(slot, ring))
        ready[pl.ds(first, count), :] = rounded * jnp.concatenate(
            [weight_column(slot) for slot in ordered], axis=0
        )

    def own_rows():
        weighted([0])
        shared.rest(0)
        own = ready[pl.ds(0, block), :]
        for owner in range(parts):
            own = own + jnp.dot(
                shared_all[owner],
                shared_down_v[pl.ds(owner * shared_width, shared_width), :],
                preferred_element_type=f32,
            )
        ready[pl.ds(0, block), :] = own

    back_rows = block // PARTS_BACK

    def longest(direction, part_back):
        return limit(direction, part_back * CHUNKS // PARTS_BACK, ring)

    def back_wait(direction, distance, b):
        here = coming.at[direction, distance, pl.ds(b * back_rows, back_rows), :]
        at = (direction, distance, b)
        remote(here, here, back_send.at[at], back_recv.at[at], ahead).wait_recv()
        return here[...].astype(f32)

    def push(distance, final):
        for b in range(PARTS_BACK):
            for direction in range(2):
                if longest(direction, b) != final:
                    continue
                slot = slot_at(1 - direction, distance, ring)
                first = place_of(slot, ring) * block + b * back_rows
                value = ready[pl.ds(first, back_rows), :]
                if distance < final:
                    value = value + back_wait(direction, distance + 1, b)
                rows = pl.ds(b * back_rows, back_rows)
                going[direction, distance, rows, :] = value.astype(bf16)
                at = (direction, distance, b)
                start(
                    remote(
                        going.at[direction, distance, rows, :],
                        coming.at[direction, distance, rows, :],
                        back_send.at[at],
                        back_recv.at[at],
                        ahead if direction == 0 else behind,
                    )
                )

    def finish_expert(b):
        rows = pl.ds(b * back_rows, back_rows)
        expert_v[rows, :] = (
            ready[rows, :] + back_wait(0, 1, b) + back_wait(1, 1, b)
        ).astype(bf16)

    with scope("c_h0"):
        loads["gate"].wait()
        loads["up"].wait()
        compute([0])
    spread_columns()
    with scope("A1c0"):
        arrive(1, 0)
    with scope("fwd_m3"):
        mixer.forward(3)
    with scope("A1c1"):
        arrive(1, 1)
    with scope("fwd_m2"):
        mixer.forward(2)
    with scope("S1"):
        swapped(1)
    with scope("c_h1"):
        compute([1, ring - 1])
    with scope("A2c0"):
        arrive(2, 0)
    with scope("w_qkv"):
        for name in ("mixer_gain", "query_gain", "key_gain", "sink", "query", "key", "value"):
            loads[name].wait()
    with scope("qkv3"):
        project(3)
        send_halo()
    with scope("qkv2"):
        project(2)
    with scope("A2c1"):
        arrive(2, 1)
    with scope("S2"):
        swapped(2)
    with scope("c_h2"):
        compute([2, ring - 2])
    with scope("A3c0"):
        arrive(3, 0)
    with scope("att3"):
        attend(3)
        att.to_sibling(3)
    with scope("fwd_sh_h0"):
        shared.forward(0)
        hidden.forward(0)
    with scope("A3c1"):
        arrive(3, 1)
    with scope("S3"):
        swapped(3)
    with scope("c_h3"):
        compute([3, ring - 3])
    with scope("A4"):
        arrive(4, 0)
        arrive(4, 1)
    with scope("w0"):
        column_start()
    with scope("fwd_h1"):
        hidden.forward(1)
        hidden.forward(ring - 1)
    with scope("S4"):
        swapped(4)
    with scope("c_h4"):
        compute([4])
    mixer.to_across(1)
    att.to_across(3)
    mixer.to_across(0)
    with scope("own"):
        loads["down"].wait()
        loads["shared_down"].wait()
        for peer in range(1, ring):
            here = dense_all.at[peer]
            remote(here, here, dense_send.at[peer], dense_recv.at[peer], sibling).wait_recv()
        own_rows()
    with scope("w1"):
        column_arrive(1)
    with scope("down1"):
        weighted([1, ring - 1])
    with scope("fwd_h2"):
        hidden.forward(2)
        hidden.forward(ring - 2)
    with scope("w2"):
        column_arrive(2)
    with scope("down2"):
        weighted([2, ring - 2])
    with scope("w3"):
        column_arrive(3)
    with scope("fwd_h3"):
        hidden.forward(3)
        hidden.forward(ring - 3)
    with scope("down3"):
        weighted([3, ring - 3])
        push(3, 3)
    with scope("w4"):
        column_arrive(4)
        column_swap()
    with scope("fwd_h4"):
        hidden.forward(4)
    with scope("down4"):
        weighted([4])
        push(4, 4)
    with scope("fwd_m1"):
        mixer.forward(1)
    with scope("push2_3"):
        push(2, 3)
    with scope("qkv1"):
        project(1)
    with scope("att2"):
        attend(2)
        att.both(2)
    with scope("push3_4"):
        push(3, 4)
    with scope("fwd_a3m0"):
        att.forward(3)
        mixer.forward(0)
    with scope("halo"):
        wait_halo()
    with scope("push1_3"):
        push(1, 3)
    with scope("qkv0"):
        project(0)
    with scope("att1"):
        attend(1)
        att.both(1)
    with scope("att0"):
        attend(0)
        att.both(0)
    with scope("push2_4"):
        push(2, 4)
    with scope("fwd_a2"):
        att.forward(2)
    with scope("out3"):
        column_wait()
        finish_mixer(3)
    with scope("push1_4"):
        push(1, 4)
    with scope("fwd_a10"):
        att.forward(1)
        att.forward(0)
    with scope("out21"):
        finish_mixer(2)
        finish_mixer(1)
    with scope("out0"):
        finish_mixer(0)
    with scope("fin_exp"):
        for b in range(PARTS_BACK):
            finish_expert(b)
        stores.append(pltpu.make_async_copy(expert_v, expert_result, store_sem.at[pieces]))
        stores[-1].start()
    with scope("w_end"):
        for copy in stores:
            copy.wait()
        for copy in pending:
            copy.wait_send()


def shards(
    mixer_input,
    mixer_gain,
    w_query,
    w_key,
    w_value,
    query_gain,
    key_gain,
    sink_logit,
    w_output,
    expert_input,
    expert_gain,
    route_ids,
    route_weight,
    expert_gate,
    expert_up,
    expert_down,
    shared_gate,
    shared_up,
    shared_down,
):
    ring = lax.axis_size("ep")
    parts = lax.axis_size("tp")
    rows_local, mixer_cols = mixer_input.shape
    tokens_local, width = expert_input.shape
    hidden_width = expert_gate.shape[2]
    shared_width = shared_gate.shape[1]
    out_width = expert_down.shape[2]
    head_width = w_query.shape[1]
    pieces = rows_local // WINDOW
    half = ring // 2
    hbm = pl.BlockSpec(memory_space=pl.ANY)
    bf16, f32 = jnp.bfloat16, jnp.float32
    vm = pltpu.VMEM

    def sems(*shape):
        return [pltpu.SemaphoreType.DMA(shape)] * 2

    outputs = pl.pallas_call(
        functools.partial(layer_kernel, ring),
        out_shape=(
            jax.ShapeDtypeStruct((rows_local, out_width), bf16),
            jax.ShapeDtypeStruct((tokens_local, out_width), bf16),
        ),
        in_specs=[hbm] * 19,
        out_specs=(hbm,) * 2,
        scratch_shapes=[
            vm((tokens_local, width), bf16),
            vm((1, width), f32),
            vm((TOPK, tokens_local), jnp.int32),
            vm((TOPK, tokens_local), f32),
            vm((1, parts * mixer_cols), f32),
            vm((1, HEAD), f32),
            vm((1, HEAD), f32),
            vm((1, sink_logit.shape[0]), f32),
            vm((parts, rows_local, mixer_cols), bf16),
            vm((parts, ring * tokens_local, hidden_width), bf16),
            vm((parts, tokens_local, shared_width), bf16),
            vm((parts, rows_local, head_width), bf16),
            vm((ring, ring, tokens_local), f32),
            vm((2, ring * tokens_local, width // 2), bf16),
            vm((width, hidden_width), bf16),
            vm((width, hidden_width), bf16),
            vm((width, shared_width), bf16),
            vm((width, shared_width), bf16),
            vm((width, head_width + w_key.shape[1] + w_value.shape[1]), bf16),
            vm(expert_down.shape[1:], bf16),
            vm(shared_down.shape, bf16),
            vm((parts, head_width, out_width), bf16),
            vm((head_width, 2 * out_width), bf16),
            vm((WINDOW, parts * mixer_cols), bf16),
            vm((head_width // HEAD, rows_local, 2 * HEAD), bf16),
            vm((WINDOW + rows_local, 4 * HEAD), bf16),
            vm((WINDOW, 2 * WINDOW), f32),
            vm((ring * tokens_local, out_width), f32),
            vm((2, half + 1, tokens_local, out_width), bf16),
            vm((2, half + 1, tokens_local, out_width), bf16),
            vm((rows_local, out_width), bf16),
            vm((tokens_local, out_width), bf16),
            pltpu.SemaphoreType.DMA((19,)),
            pltpu.SemaphoreType.DMA((pieces + 1,)),
            *sems(2, half + 1, CHUNKS),
            *sems(2, half + 1, CHUNKS),
            *sems(3, pieces),
            *sems(3, ring),
            *sems(3, 1),
            *sems(3, pieces),
            *sems(ring),
            *sems(1),
            *sems(3),
            *sems(2, half + 1, CHUNKS),
            *sems(2, half + 1, PARTS_BACK),
        ],
        compiler_params=pltpu.CompilerParams(
            collective_id=0, has_side_effects=True, vmem_limit_bytes=VMEM_LIMIT
        ),
        name="layer",
    )(
        expert_input,
        expert_gain[None, :],
        route_ids.T,
        route_weight.T,
        mixer_input,
        mixer_gain[None, :],
        query_gain[None, :],
        key_gain[None, :],
        sink_logit[None, :],
        expert_gate[0],
        expert_up[0],
        shared_gate,
        shared_up,
        w_query,
        w_key,
        w_value,
        w_output,
        expert_down[0],
        shared_down,
    )
    return outputs


def plan(*arrays):
    route_ids = arrays[11]
    capacity = 2 * route_ids.size // lax.axis_size("ep")
    whole_blocks = capacity >= route_ids.shape[0]
    if whole_blocks and lax.axis_size("tp") == 4:
        return shards(*arrays)
    return shards_routed(*arrays)


def solution(mesh):
    in_specs = (
        P("ep", "tp"),
        P(),
        P(None, "tp"),
        P(),
        P(),
        P(),
        P(),
        P("tp"),
        P("tp", None),
        P("ep", None),
        P(),
        P("ep", None),
        P("ep", None),
        P("ep", None, "tp"),
        P("ep", None, "tp"),
        P("ep", None, "tp"),
        P(None, "tp"),
        P(None, "tp"),
        P(None, "tp"),
    )
    out_specs = (P("ep", "tp"), P("ep", "tp"))
    return jax.shard_map(plan, mesh=mesh, in_specs=in_specs, out_specs=out_specs, check_vma=False)
```

```python
import functools

import jax
import jax.numpy as jnp
from jax import lax
from jax.experimental import pallas as pl
from jax.experimental.pallas import tpu as pltpu
from jax.sharding import PartitionSpec as P

D = 2048
HEAD = 64
KV_HEADS = 2
WINDOW = 128
TOPK = 4


EPSILON = 1e-06


def from_behind(value, axis, steps):
    count = lax.axis_size(axis)
    first, last = (max(0, -steps), min(count, count - steps))
    return lax.ppermute(value, axis, [(source, source + steps) for source in range(first, last)])


def head_norm(matrix, gain_vector):
    return (
        matrix
        * lax.rsqrt(jnp.mean(matrix * matrix, axis=-1, keepdims=True) + EPSILON)
        * gain_vector
    )


def band_attend(queries, keys_own, values_own, keys_prev, values_prev, sink_logit, first_row):
    row_count = queries.shape[0]
    head_count = queries.shape[1]
    blocks = row_count // WINDOW
    keys_all = jnp.concatenate([keys_prev, keys_own], axis=0)
    values_all = jnp.concatenate([values_prev, values_own], axis=0)
    key_band = jnp.concatenate(
        [
            keys_all[:row_count].reshape(blocks, WINDOW, HEAD),
            keys_own.reshape(blocks, WINDOW, HEAD),
        ],
        axis=1,
    )
    value_band = jnp.concatenate(
        [
            values_all[:row_count].reshape(blocks, WINDOW, HEAD),
            values_own.reshape(blocks, WINDOW, HEAD),
        ],
        axis=1,
    )
    query_blocks = queries.reshape(blocks, WINDOW, head_count, HEAD)
    scores = jnp.einsum(
        "nqhd,nkd->nhqk", query_blocks, key_band, preferred_element_type=jnp.float32
    ) * HEAD ** (-0.5)
    query_idx = jnp.arange(WINDOW, dtype=jnp.int32)[:, None]
    key_idx = jnp.arange(2 * WINDOW, dtype=jnp.int32)[None, :]
    relative = query_idx + WINDOW - key_idx
    block_idx = jnp.arange(blocks, dtype=jnp.int32)[:, None, None]
    key_pos = first_row + block_idx * WINDOW - WINDOW + key_idx[None]
    allowed = ((relative >= 0) & (relative < WINDOW))[None] & (key_pos >= 0)
    allowed = allowed[:, None]
    masked = jnp.where(allowed, scores, -jnp.inf)
    sink_column = sink_logit.reshape(1, head_count, 1, 1)
    peak_score = jnp.maximum(jnp.max(masked, axis=-1, keepdims=True), sink_column)
    exponent = jnp.exp(masked - peak_score)
    denominator = jnp.sum(exponent, axis=-1, keepdims=True) + jnp.exp(sink_column - peak_score)
    probability = (exponent / denominator).astype(jnp.bfloat16)
    mixed_rows = jnp.einsum(
        "nhqk,nkd->nqhd", probability, value_band, preferred_element_type=jnp.float32
    )
    return mixed_rows.reshape(row_count, head_count * HEAD).astype(jnp.bfloat16)


def shards_routed(
    mixer_input,
    mixer_gain,
    w_query,
    w_key,
    w_value,
    query_gain,
    key_gain,
    sink_logit,
    w_output,
    expert_input,
    expert_gain,
    route_ids,
    route_weight,
    expert_gate,
    expert_up,
    expert_down,
    shared_gate,
    shared_up,
    shared_down,
):
    tp_count = lax.axis_size("tp")
    ep_count = lax.axis_size("ep")
    rows_local = mixer_input.shape[0]
    heads_local = w_query.shape[1] // HEAD
    kv_index = lax.axis_index("tp") // (tp_count // KV_HEADS)
    key_cols = lax.dynamic_slice_in_dim(w_key, kv_index * HEAD, HEAD, 1)
    value_cols = lax.dynamic_slice_in_dim(w_value, kv_index * HEAD, HEAD, 1)
    portion_float = lax.all_gather(mixer_input, "tp", axis=1, tiled=True).astype(jnp.float32)
    scaled = (portion_float * mixer_gain).astype(jnp.bfloat16)
    query_raw = jnp.dot(scaled, w_query, preferred_element_type=jnp.float32)
    key_raw = jnp.dot(scaled, key_cols, preferred_element_type=jnp.float32)
    value_raw = jnp.dot(scaled, value_cols, preferred_element_type=jnp.float32)
    squares = jnp.sum(portion_float * portion_float, axis=1)
    inv_rms = lax.rsqrt(squares / D + EPSILON)[:, None]
    queries = head_norm(query_raw.reshape(rows_local, heads_local, HEAD), query_gain).astype(
        jnp.bfloat16
    )
    keys_own = head_norm(key_raw, key_gain).astype(jnp.bfloat16)
    values_own = (value_raw * inv_rms).astype(jnp.bfloat16)
    keys_prev, values_prev = from_behind(
        (keys_own[rows_local - WINDOW :], values_own[rows_local - WINDOW :]), "ep", 1
    )
    first_row = lax.axis_index("ep") * rows_local
    attended = band_attend(
        queries, keys_own, values_own, keys_prev, values_prev, sink_logit, first_row
    )
    head_partial = jnp.dot(attended, w_output, preferred_element_type=jnp.float32)
    mixer_output = lax.psum_scatter(
        head_partial.astype(jnp.bfloat16), "tp", scatter_dimension=1, tiled=True
    )
    tokens_local = expert_input.shape[0]
    expert_float = expert_input.astype(jnp.float32)
    normed = (
        expert_float
        * lax.rsqrt(jnp.mean(expert_float * expert_float, axis=-1, keepdims=True) + EPSILON)
        * expert_gain
    ).astype(jnp.bfloat16)
    capacity = 2 * tokens_local * TOPK // ep_count
    flat_ids = route_ids.reshape(-1)
    onehot = (flat_ids[:, None] == jnp.arange(ep_count, dtype=jnp.int32)[None, :]).astype(jnp.int32)
    earlier = jnp.cumsum(onehot, axis=0) - onehot
    slot_index = jnp.sum(earlier * onehot, axis=-1)
    slot_column = flat_ids * capacity + slot_index
    token_ids = jnp.arange(tokens_local * TOPK, dtype=jnp.int32) // TOPK
    slot_table = (
        jnp.full((ep_count * capacity,), tokens_local, jnp.int32).at[slot_column].set(token_ids)
    )
    col_width = expert_down.shape[2]
    arrived_rows = ep_count * capacity
    own_columns = lax.dynamic_slice_in_dim(normed, lax.axis_index("tp") * col_width, col_width, 1)
    padded = jnp.concatenate([own_columns, jnp.zeros((1, col_width), jnp.bfloat16)], axis=0)
    outgoing = padded[slot_table].reshape(ep_count, capacity, col_width)
    arrived = lax.all_to_all(outgoing, "ep", split_axis=0, concat_axis=0, tiled=True).reshape(
        arrived_rows, col_width
    )
    portion = lax.all_gather(arrived, "tp", axis=1, tiled=True)
    gate_part = expert_gate[0]
    up_part = expert_up[0]
    gate_pre = jnp.dot(portion, gate_part, preferred_element_type=jnp.float32)
    up_pre = jnp.dot(portion, up_part, preferred_element_type=jnp.float32)
    routed_hidden = (jax.nn.silu(gate_pre) * up_pre).astype(jnp.bfloat16)
    shared_hidden = (
        jax.nn.silu(jnp.dot(normed, shared_gate, preferred_element_type=jnp.float32))
        * jnp.dot(normed, shared_up, preferred_element_type=jnp.float32)
    ).astype(jnp.bfloat16)
    routed_part = expert_down[0]
    routed_sum = jnp.dot(
        lax.all_gather(routed_hidden, "tp", axis=1, tiled=True),
        routed_part,
        preferred_element_type=jnp.float32,
    )
    shared_sum = jnp.dot(
        lax.all_gather(shared_hidden, "tp", axis=1, tiled=True),
        shared_down,
        preferred_element_type=jnp.float32,
    )
    expert_rows = routed_sum.astype(jnp.bfloat16).reshape(ep_count, capacity, col_width)
    returned = lax.all_to_all(expert_rows, "ep", split_axis=0, concat_axis=0, tiled=True).reshape(
        arrived_rows, col_width
    )
    picked = returned[slot_column].reshape(tokens_local, TOPK, col_width).astype(jnp.float32)
    expert_output = (shared_sum + jnp.sum(picked * route_weight[:, :, None], axis=1)).astype(
        jnp.bfloat16
    )
    return (mixer_output, expert_output)


CHUNKS = 2
VMEM_LIMIT = 62 * 1024 * 1024
PARTS_BACK = 4
COLUMNS_X = 2


def place_of(slot, ring):
    half = ring // 2
    return 0 if slot == 0 else 2 * slot - 1 if slot <= half else 2 * (ring - slot)


def ring_position(index, ring):
    row, side = index // COLUMNS_X, index % COLUMNS_X
    return row + side * (ring - 1 - 2 * row)


def ring_index(position, ring):
    side = position // (ring // COLUMNS_X)
    return 2 * position + side * (2 * ring - 1 - 4 * position)


def remote(source, target, send, receive, device):
    return pltpu.make_async_remote_copy(
        src_ref=source,
        dst_ref=target,
        send_sem=send,
        recv_sem=receive,
        device_id=device,
        device_id_type=pl.DeviceIdType.MESH,
    )


def limit(direction, chunk, ring):
    return ring // 2 if direction == chunk else ring // 2 - 1


def slot_at(direction, distance, ring):
    return distance if direction == 0 else ring - distance


def layer_kernel(
    ring,
    rows_hbm,
    gain_hbm,
    ids_hbm,
    weight_hbm,
    mixer_hbm,
    mixer_gain_hbm,
    query_gain_hbm,
    key_gain_hbm,
    sink_hbm,
    gate_hbm,
    up_hbm,
    shared_gate_hbm,
    shared_up_hbm,
    query_hbm,
    key_hbm,
    value_hbm,
    w_out_hbm,
    down_hbm,
    shared_down_hbm,
    mixer_result,
    expert_result,
    rows_v,
    gain_v,
    ids_v,
    weight_v,
    mixer_gain_v,
    query_gain_v,
    key_gain_v,
    sink_v,
    mixer_all,
    hidden_all,
    shared_all,
    att_all,
    dense_all,
    tok,
    gate_v,
    up_v,
    shared_gate_v,
    shared_up_v,
    qkv_v,
    down_v,
    shared_down_v,
    out_cols,
    out_stage,
    scaled_v,
    heads_v,
    band_v,
    bias_v,
    ready,
    going,
    coming,
    mixer_v,
    expert_v,
    load_sem,
    store_sem,
    tok_send,
    ring_recv,
    sib_recv,
    mix_send,
    mix_recv,
    hid_send,
    hid_recv,
    sh_send,
    sh_recv,
    att_send,
    att_recv,
    dense_send,
    dense_recv,
    halo_send,
    halo_recv,
    wcol_send,
    wcol_recv,
    wring_send,
    wring_recv,
    back_send,
    back_recv,
):
    scope = jax.named_scope
    f32, bf16 = jnp.float32, jnp.bfloat16
    index, part = lax.axis_index("ep"), lax.axis_index("tp")
    far, core = part // 2, part % 2
    position = ring_position(index, ring)
    peer_index = [ring_index((position + k) % ring, ring) for k in range(ring)]
    peers = [(peer_index[k], part) for k in range(1, ring)]
    ahead, behind = peers[0], peers[-1]
    sib_part = 2 * far + 1 - core
    across_part = 2 * (1 - far) + core
    corner_part = 2 * (1 - far) + 1 - core
    sibling, across = (index, sib_part), (index, across_part)
    block, width = rows_v.shape
    half_width = width // 2
    piece = block // CHUNKS
    steps = ring // 2
    parts, rows_local, mixer_cols = mixer_all.shape
    pieces = rows_local // WINDOW
    out_width = down_v.shape[1]
    inner = hidden_all.shape[2]
    shared_width = shared_all.shape[2]
    head_rows = out_cols.shape[1]
    share_rows = head_rows // ring

    barrier = pltpu.get_barrier_semaphore()
    for device in peers + [sibling, across]:
        pl.semaphore_signal(barrier, inc=1, device_id=device, device_id_type=pl.DeviceIdType.MESH)

    stores = []

    def start(copy):
        copy.start()

    loads = {}

    def load(name, source, target):
        loads[name] = pltpu.make_async_copy(source, target, load_sem.at[len(loads)])
        loads[name].start()

    def load_qkv(source, first):
        target = qkv_v.at[:, pl.ds(first, source.shape[1])]
        pltpu.make_async_copy(source, target, load_sem.at[len(loads)]).start()

    own_cols = pl.ds(pl.multiple_of(part * out_width, out_width), out_width)
    load("rows", rows_hbm, rows_v)
    load("gain", gain_hbm, gain_v)
    load("mixer", mixer_hbm, mixer_all.at[part])
    load("shared_gate", shared_gate_hbm, shared_gate_v)
    load("shared_up", shared_up_hbm, shared_up_v)
    load("gate", gate_hbm, gate_v)
    load("up", up_hbm, up_v)
    load("ids", ids_hbm, ids_v)
    load("weight", weight_hbm, weight_v)
    load("mixer_gain", mixer_gain_hbm, mixer_gain_v)
    load("query_gain", query_gain_hbm, query_gain_v)
    load("key_gain", key_gain_hbm, key_gain_v)
    load("sink", sink_hbm, sink_v)
    query_cols, key_cols = query_hbm.shape[1], key_hbm.shape[1]
    load_qkv(query_hbm, 0)
    load_qkv(key_hbm, query_cols)
    load_qkv(value_hbm, query_cols + key_cols)
    loads["qkv"] = pltpu.make_async_copy(qkv_v, qkv_v, load_sem.at[len(loads)])
    load("out_own", w_out_hbm.at[:, own_cols], out_cols.at[part])
    load("down", down_hbm, down_v)
    load("shared_down", shared_down_hbm, shared_down_v)

    relative = (
        lax.broadcasted_iota(jnp.int32, (WINDOW, 2 * WINDOW), 0)
        + WINDOW
        - lax.broadcasted_iota(jnp.int32, (WINDOW, 2 * WINDOW), 1)
    )
    bias_v[...] = jnp.where((relative >= 0) & (relative < WINDOW), 0.0, -jnp.inf)
    low = lax.broadcasted_iota(jnp.int32, (WINDOW, 2 * HEAD), 1) < HEAD

    with scope("norm"):
        loads["rows"].wait()
        loads["gain"].wait()
        value = rows_v[...].astype(f32)
        normed = (
            value
            * lax.rsqrt(jnp.mean(value * value, axis=-1, keepdims=True) + EPSILON)
            * gain_v[...]
        ).astype(bf16)
        tok[0, pl.ds(0, block), :] = normed[:, :half_width]
        tok[1, pl.ds(0, block), :] = normed[:, half_width:]
        loads["mixer"].wait()

    with scope("greet"):
        pl.semaphore_wait(barrier, ring + 1)

    def chunk_ref(half, slot, chunk):
        return tok.at[half, pl.ds(place_of(slot, ring) * block + chunk * piece, piece), :]

    def hop(direction, distance, chunk):
        start(
            remote(
                chunk_ref(core, slot_at(direction, distance - 1, ring) % ring, chunk),
                chunk_ref(core, slot_at(direction, distance, ring), chunk),
                tok_send.at[0],
                ring_recv.at[direction, distance - 1, chunk],
                ahead if direction == 0 else behind,
            )
        )

    def arrive(distance, k):
        for direction in range(2):
            chunk = k if direction == 0 else CHUNKS - 1 - k
            if distance > limit(direction, chunk, ring):
                continue
            here = chunk_ref(core, slot_at(direction, distance, ring), chunk)
            got = ring_recv.at[direction, distance - 1, chunk]
            remote(here, here, tok_send.at[0], got, sibling).wait_recv()
            if distance < limit(direction, chunk, ring):
                hop(direction, distance + 1, chunk)
            start(remote(here, here, tok_send.at[0], sib_recv.at[distance - 1], sibling))

    def swapped(distance):
        count = 2 if distance < steps else 1
        there = tok.at[1 - core, pl.ds((2 * distance - 1) * block, count * block), :]
        remote(there, there, tok_send.at[0], sib_recv.at[distance - 1], sibling).wait_recv()

    class Share:
        def __init__(self, view, send, receive):
            self.view, self.send, self.receive = view, send, receive

        def copy(self, owner, i, path, device):
            here = self.view(owner, i)
            return remote(here, here, self.send.at[0], self.receive.at[path, i], device)

        def to_across(self, i):
            start(self.copy(part, i, 0, across))

        def to_sibling(self, i):
            start(self.copy(part, i, 1, sibling))

        def both(self, i):
            self.to_across(i)
            self.to_sibling(i)

        def forward(self, i):
            self.copy(across_part, i, 0, sibling).wait_recv()
            start(self.copy(across_part, i, 1, sibling))

        def rest(self, i):
            self.copy(pl.ds(0, 2), i, 1, sibling).wait_recv()

    mixer = Share(
        lambda owner, i: mixer_all.at[owner, pl.ds(i * WINDOW, WINDOW), :], mix_send, mix_recv
    )
    shared = Share(lambda owner, i: shared_all.at[owner], sh_send, sh_recv)
    hidden = Share(
        lambda owner, i: hidden_all.at[owner, pl.ds(place_of(i, ring) * block, block), :],
        hid_send,
        hid_recv,
    )
    att = Share(
        lambda owner, i: att_all.at[owner, pl.ds(i * WINDOW, WINDOW), :], att_send, att_recv
    )

    for k in range(CHUNKS):
        for direction in range(2):
            hop(direction, 1, k if direction == 0 else CHUNKS - 1 - k)
    mixer.both(3)
    mixer.both(2)
    mixer.to_sibling(1)
    mixer.to_sibling(0)

    loads["ids"].wait()
    loads["weight"].wait()
    experts = lax.broadcasted_iota(jnp.int32, (ring, block), 0)
    dense = jnp.zeros((ring, block), f32)
    for k in range(TOPK):
        dense = dense + jnp.where(ids_v[k : k + 1, :] == experts, weight_v[k : k + 1, :], 0.0)
    dense_all[0] = dense
    for k in range(1, ring):
        start(
            remote(
                dense_all.at[0], dense_all.at[k], dense_send.at[0], dense_recv.at[0], peers[k - 1]
            )
        )

    def product(first, count, weights, columns):
        lower = tok[0, pl.ds(first, count), :]
        upper = tok[1, pl.ds(first, count), :]
        return jnp.dot(
            lower, weights[pl.ds(0, half_width), columns], preferred_element_type=f32
        ) + jnp.dot(
            upper, weights[pl.ds(half_width, half_width), columns], preferred_element_type=f32
        )

    with scope("c_shared"):
        loads["shared_gate"].wait()
        loads["shared_up"].wait()
        everything = pl.ds(0, shared_width)
        shared_all[part] = (
            jax.nn.silu(product(0, block, shared_gate_v, everything))
            * product(0, block, shared_up_v, everything)
        ).astype(bf16)
        shared.both(0)

    tile = 256

    def compute(slots):
        first = min(place_of(slot, ring) for slot in slots) * block
        count = len(slots) * block

        def one(j, carry):
            columns = pl.ds(pl.multiple_of(j * tile, tile), tile)
            hidden_all[part, pl.ds(first, count), columns] = (
                jax.nn.silu(product(first, count, gate_v, columns))
                * product(first, count, up_v, columns)
            ).astype(bf16)
            return carry

        lax.fori_loop(0, inner // tile, one, 0)
        for slot in slots:
            hidden.both(slot)

    def project(i):
        rows = pl.ds(i * WINDOW, WINDOW)
        mixer.rest(i)
        squares = jnp.zeros((WINDOW, 1), f32)
        for owner in range(parts):
            columns = pl.ds(owner * mixer_cols, mixer_cols)
            value = mixer_all[owner, rows, :].astype(f32)
            squares = squares + jnp.sum(value * value, axis=1, keepdims=True)
            scaled_v[:, columns] = (value * mixer_gain_v[:, columns]).astype(bf16)
        raw = jnp.dot(scaled_v[...], qkv_v[...], preferred_element_type=f32)
        lanes = 2 * HEAD
        heads = heads_v.shape[0]
        gain = query_gain_v[...] * HEAD ** (-0.5)
        gain = jnp.concatenate([gain, gain], axis=1)
        for pair in range(heads // 2):
            two = raw[:, pair * lanes : (pair + 1) * lanes]
            square = two * two
            first_sum = jnp.sum(jnp.where(low, square, 0.0), axis=1, keepdims=True)
            second_sum = jnp.sum(jnp.where(low, 0.0, square), axis=1, keepdims=True)
            inverse = lax.rsqrt(jnp.where(low, first_sum, second_sum) / HEAD + EPSILON)
            two = two * inverse * gain
            heads_v[2 * pair, rows, :] = jnp.where(low, two, 0.0).astype(bf16)
            heads_v[2 * pair + 1, rows, :] = jnp.where(low, 0.0, two).astype(bf16)
        queries_end = heads * HEAD
        second = part // (parts // KV_HEADS)
        mine = low == (second == 0)

        def twice(columns):
            return jnp.where(mine, columns, pltpu.roll(columns, HEAD, 1))

        key = twice(raw[:, queries_end : queries_end + lanes])
        gain = jnp.concatenate([key_gain_v[...], key_gain_v[...]], axis=1)
        key = key * lax.rsqrt(jnp.mean(key * key, axis=1, keepdims=True) + EPSILON) * gain
        val = twice(raw[:, queries_end + lanes : queries_end + 2 * lanes])
        val = val * lax.rsqrt(squares / D + EPSILON)
        band_v[pl.ds(WINDOW + i * WINDOW, WINDOW), :] = jnp.concatenate(
            [key, val], axis=1
        ).astype(bf16)

    halo = band_v.at[pl.ds(0, WINDOW), :]

    def send_halo():
        start(
            remote(
                band_v.at[pl.ds(rows_local, WINDOW), :],
                halo,
                halo_send.at[0],
                halo_recv.at[0],
                ((index + 1) % ring, part),
            )
        )

    def wait_halo():
        remote(halo, halo, halo_send.at[0], halo_recv.at[0], sibling).wait_recv()

    def attend(i):
        rows = pl.ds(i * WINDOW, WINDOW)
        keys = band_v[pl.ds(i * WINDOW, 2 * WINDOW), pl.ds(0, 2 * HEAD)]
        values = band_v[pl.ds(i * WINDOW, 2 * WINDOW), pl.ds(2 * HEAD, 2 * HEAD)]
        bias = bias_v[...]
        if i == 0:
            before = lax.broadcasted_iota(jnp.int32, (WINDOW, 2 * WINDOW), 1) < WINDOW
            bias = jnp.where(before & (index == 0), -jnp.inf, bias)
        mixed = []
        for head in range(heads_v.shape[0]):
            scores = lax.dot_general(
                heads_v[head, rows, :],
                keys,
                (((1,), (1,)), ((), ())),
                preferred_element_type=f32,
            )
            masked = scores + bias
            sink = sink_v[:, head : head + 1]
            peak = jnp.maximum(jnp.max(masked, axis=1, keepdims=True), sink)
            exponent = jnp.exp(masked - peak)
            denominator = jnp.sum(exponent, axis=1, keepdims=True) + jnp.exp(sink - peak)
            probability = (exponent * (1.0 / denominator)).astype(bf16)
            mixed.append(jnp.dot(probability, values, preferred_element_type=f32))
        for pair in range(len(mixed) // 2):
            att_all[part, rows, pl.ds(pair * 2 * HEAD, 2 * HEAD)] = jnp.where(
                low, mixed[2 * pair], mixed[2 * pair + 1]
            ).astype(bf16)

    chip_cols = 2 * out_width

    def spread_columns():
        start(
            remote(
                w_out_hbm.at[:, pl.ds(pl.multiple_of(sib_part * out_width, out_width), out_width)],
                out_cols.at[part],
                wcol_send.at[0],
                wcol_recv.at[0],
                sibling,
            )
        )
        mine = pl.ds(pl.multiple_of(index * share_rows, share_rows), share_rows)
        start(
            remote(
                w_out_hbm.at[
                    mine, pl.ds(pl.multiple_of((1 - far) * chip_cols, chip_cols), chip_cols)
                ],
                out_stage.at[mine, :],
                wcol_send.at[1],
                wcol_recv.at[1],
                across,
            )
        )

    def column_start():
        mine = out_stage.at[pl.ds(pl.multiple_of(index * share_rows, share_rows), share_rows), :]
        remote(mine, mine, wcol_send.at[1], wcol_recv.at[1], across).wait_recv()
        for device in peers:
            start(remote(mine, mine, wring_send.at[0], wring_recv.at[0], device))

    def column_rest():
        here = out_stage.at[pl.ds(0, (ring - 1) * share_rows), :]
        remote(here, here, wring_send.at[0], wring_recv.at[0], sibling).wait_recv()

    def column_swap():
        start(
            remote(
                out_stage.at[
                    :, pl.ds(pl.multiple_of((1 - core) * out_width, out_width), out_width)
                ],
                out_cols.at[across_part],
                wcol_send.at[2],
                wcol_recv.at[2],
                sibling,
            )
        )

    def column_wait():
        loads["out_own"].wait()
        for i, owner in ((0, sib_part), (2, corner_part)):
            here = out_cols.at[owner]
            remote(here, here, wcol_send.at[i], wcol_recv.at[i], sibling).wait_recv()

    def finish_mixer(i):
        rows = pl.ds(i * WINDOW, WINDOW)
        att.rest(i)
        total = jnp.dot(
            att_all[across_part, rows, :],
            out_stage[:, pl.ds(pl.multiple_of(core * out_width, out_width), out_width)],
            preferred_element_type=f32,
        )
        for owner in (part, sib_part, corner_part):
            total = total + jnp.dot(
                att_all[owner, rows, :], out_cols[owner], preferred_element_type=f32
            )
        mixer_v[rows, :] = total.astype(bf16)
        stores.append(
            pltpu.make_async_copy(mixer_v.at[rows, :], mixer_result.at[rows, :], store_sem.at[i])
        )
        stores[-1].start()

    diagonal = lax.broadcasted_iota(jnp.int32, (block, block), 0) == lax.broadcasted_iota(
        jnp.int32, (block, block), 1
    )

    def weight_column(slot):
        row = dense_all[slot, pl.ds(index, 1), :]
        return jnp.sum(jnp.where(diagonal, row, 0.0), axis=1, keepdims=True)

    def weighted(slots):
        for slot in slots:
            hidden.rest(slot)
        first = min(place_of(slot, ring) for slot in slots) * block
        count = len(slots) * block
        total = jnp.dot(
            hidden_all[0, pl.ds(first, count), :],
            down_v[pl.ds(0, inner), :],
            preferred_element_type=f32,
        )
        for owner in range(1, parts):
            total = total + jnp.dot(
                hidden_all[owner, pl.ds(first, count), :],
                down_v[pl.ds(owner * inner, inner), :],
                preferred_element_type=f32,
            )
        rounded = total.astype(bf16).astype(f32)
        ordered = sorted(slots, key=lambda slot: place_of(slot, ring))
        ready[pl.ds(first, count), :] = rounded * jnp.concatenate(
            [weight_column(slot) for slot in ordered], axis=0
        )

    def own_rows():
        weighted([0])
        shared.rest(0)
        own = ready[pl.ds(0, block), :]
        for owner in range(parts):
            own = own + jnp.dot(
                shared_all[owner],
                shared_down_v[pl.ds(owner * shared_width, shared_width), :],
                preferred_element_type=f32,
            )
        ready[pl.ds(0, block), :] = own

    back_rows = block // PARTS_BACK

    def longest(direction, part_back):
        return limit(direction, part_back * CHUNKS // PARTS_BACK, ring)

    def back_wait(direction, distance, b):
        here = coming.at[direction, distance, pl.ds(b * back_rows, back_rows), :]
        got = back_recv.at[direction, distance - 1, b]
        remote(here, here, back_send.at[0], got, ahead).wait_recv()
        return here[...].astype(f32)

    def push(distance, long, directions=(0, 1)):
        for b in range(PARTS_BACK):
            for direction in directions:
                if (longest(direction, b) == steps) != long:
                    continue
                slot = slot_at(1 - direction, distance, ring)
                first = place_of(slot, ring) * block + b * back_rows
                value = ready[pl.ds(first, back_rows), :]
                hops = 1
                if long and distance == steps:
                    hops = 2
                elif long and distance == steps - 2:
                    hops = 2
                    value = value + back_wait(direction, distance + 1, b)
                    value = value + back_wait(direction, distance + 2, b)
                elif not long and distance < steps - 1:
                    value = value + back_wait(direction, distance + 1, b)
                rows = pl.ds(b * back_rows, back_rows)
                at = direction * steps + distance - 1
                going[at, rows, :] = value.astype(bf16)
                start(
                    remote(
                        going.at[at, rows, :],
                        coming.at[direction, distance, rows, :],
                        back_send.at[0],
                        back_recv.at[direction, distance - 1, b],
                        peers[hops - 1 if direction == 0 else -hops],
                    )
                )

    def finish_expert(b):
        rows = pl.ds(b * back_rows, back_rows)
        total = ready[rows, :]
        for direction in range(2):
            total = total + back_wait(direction, 1, b)
            if longest(direction, b) == steps:
                total = total + back_wait(direction, 2, b)
        expert_v[rows, :] = total.astype(bf16)

    with scope("c_h0"):
        loads["gate"].wait()
        loads["up"].wait()
        compute([0])
    spread_columns()
    mixer.to_across(1)
    with scope("A1c0"):
        arrive(1, 0)
    with scope("fwd_m3"):
        mixer.forward(3)
    with scope("A1c1"):
        arrive(1, 1)
    with scope("fwd_m2"):
        mixer.forward(2)
    with scope("w_qkv"):
        for name in ("mixer_gain", "query_gain", "key_gain", "sink", "qkv"):
            loads[name].wait()
    with scope("qkv3"):
        project(3)
        send_halo()
    with scope("S1"):
        swapped(1)
    with scope("c_h1"):
        compute([1, ring - 1])
    with scope("A2c0"):
        arrive(2, 0)
    with scope("qkv2"):
        project(2)
    with scope("att3"):
        attend(3)
        att.to_sibling(3)
    with scope("A2c1"):
        arrive(2, 1)
    with scope("fwd_sh_h0"):
        shared.forward(0)
        hidden.forward(0)
    with scope("S2"):
        swapped(2)
    with scope("c_h2"):
        compute([2, ring - 2])
    with scope("A3c0"):
        arrive(3, 0)
    with scope("fwd_m1"):
        mixer.forward(1)
    with scope("own"):
        loads["down"].wait()
        loads["shared_down"].wait()
        here = dense_all.at[pl.ds(1, ring - 1)]
        remote(here, here, dense_send.at[0], dense_recv.at[0], sibling).wait_recv()
        own_rows()
    with scope("qkv1"):
        project(1)
    with scope("A3c1"):
        arrive(3, 1)
    with scope("w0"):
        column_start()
    with scope("fwd_h1"):
        hidden.forward(1)
    with scope("S3"):
        swapped(3)
    with scope("c_h3"):
        compute([3, ring - 3])
    with scope("A4"):
        arrive(4, 0)
    with scope("fwd_h7"):
        hidden.forward(ring - 1)
    with scope("att2"):
        attend(2)
        att.to_sibling(2)
    with scope("S4"):
        swapped(4)
    with scope("c_h4"):
        compute([4])
    mixer.to_across(0)
    att.to_across(3)
    att.to_across(2)
    with scope("down1"):
        weighted([1, ring - 1])
    push(1, True)
    with scope("fwd_h2"):
        hidden.forward(2)
        hidden.forward(ring - 2)
    with scope("halo"):
        wait_halo()
    with scope("fwd_h3"):
        hidden.forward(3)
    with scope("down2"):
        weighted([2, ring - 2])
    with scope("down3"):
        weighted([3])
        push(3, False, (1,))
        push(3, True, (1,))
    with scope("fwd_h5"):
        hidden.forward(ring - 3)
    with scope("col_rest"):
        column_rest()
        column_swap()
    with scope("down5"):
        weighted([ring - 3])
        push(3, False, (0,))
        push(3, True, (0,))
    with scope("fwd_h4"):
        hidden.forward(4)
    with scope("down4"):
        weighted([4])
        push(4, True)
    with scope("fwd_m0"):
        mixer.forward(0)
    with scope("push2s"):
        push(2, False)
    with scope("qkv0"):
        project(0)
    with scope("att1"):
        attend(1)
        att.both(1)
    with scope("push2l"):
        push(2, True)
    with scope("push1s"):
        push(1, False)
    with scope("att0"):
        attend(0)
        att.both(0)
    with scope("fwd_a32"):
        att.forward(3)
        att.forward(2)
    with scope("fwd_a1"):
        att.forward(1)
    with scope("out3"):
        column_wait()
        finish_mixer(3)
    with scope("out2"):
        finish_mixer(2)
    with scope("fin_exp"):
        for b in range(PARTS_BACK):
            finish_expert(b)
        stores.append(pltpu.make_async_copy(expert_v, expert_result, store_sem.at[pieces]))
        stores[-1].start()
    with scope("fwd_a0"):
        att.forward(0)
    with scope("out1"):
        finish_mixer(1)
    with scope("out0"):
        finish_mixer(0)
    with scope("w_end"):
        for copy in stores:
            copy.wait()
        for ref, send in (
            (tok.at[:, pl.ds(0, (ring - 1) * block), :], tok_send.at[0]),
            (mixer_all.at[pl.ds(0, parts - 1)], mix_send.at[0]),
            (hidden_all.at[pl.ds(0, parts - 1)], hid_send.at[0]),
            (shared_all.at[pl.ds(0, parts - 1)], sh_send.at[0]),
            (att_all.at[pl.ds(0, parts - 1)], att_send.at[0]),
            (dense_all.at[pl.ds(0, ring - 1)], dense_send.at[0]),
            (halo, halo_send.at[0]),
            (out_cols.at[part], wcol_send.at[0]),
            (out_stage.at[pl.ds(0, share_rows), :], wcol_send.at[1]),
            (out_cols.at[part], wcol_send.at[2]),
            (out_stage.at[pl.ds(0, (ring - 1) * share_rows), :], wring_send.at[0]),
            (going.at[pl.ds(0, ring - 1)], back_send.at[0]),
        ):
            remote(ref, ref, send, halo_recv.at[0], sibling).wait_send()


def shards(
    mixer_input,
    mixer_gain,
    w_query,
    w_key,
    w_value,
    query_gain,
    key_gain,
    sink_logit,
    w_output,
    expert_input,
    expert_gain,
    route_ids,
    route_weight,
    expert_gate,
    expert_up,
    expert_down,
    shared_gate,
    shared_up,
    shared_down,
):
    ring = lax.axis_size("ep")
    parts = lax.axis_size("tp")
    rows_local, mixer_cols = mixer_input.shape
    tokens_local, width = expert_input.shape
    hidden_width = expert_gate.shape[2]
    shared_width = shared_gate.shape[1]
    out_width = expert_down.shape[2]
    head_width = w_query.shape[1]
    pieces = rows_local // WINDOW
    half = ring // 2
    hbm = pl.BlockSpec(memory_space=pl.ANY)
    bf16, f32 = jnp.bfloat16, jnp.float32
    vm = pltpu.VMEM

    dma = pltpu.SemaphoreType.DMA
    outputs = pl.pallas_call(
        functools.partial(layer_kernel, ring),
        out_shape=(
            jax.ShapeDtypeStruct((rows_local, out_width), bf16),
            jax.ShapeDtypeStruct((tokens_local, out_width), bf16),
        ),
        in_specs=[hbm] * 19,
        out_specs=(hbm,) * 2,
        scratch_shapes=[
            vm((tokens_local, width), bf16),
            vm((1, width), f32),
            vm((TOPK, tokens_local), jnp.int32),
            vm((TOPK, tokens_local), f32),
            vm((1, parts * mixer_cols), f32),
            vm((1, HEAD), f32),
            vm((1, HEAD), f32),
            vm((1, sink_logit.shape[0]), f32),
            vm((parts, rows_local, mixer_cols), bf16),
            vm((parts, ring * tokens_local, hidden_width), bf16),
            vm((parts, tokens_local, shared_width), bf16),
            vm((parts, rows_local, head_width), bf16),
            vm((ring, ring, tokens_local), f32),
            vm((2, ring * tokens_local, width // 2), bf16),
            vm((width, hidden_width), bf16),
            vm((width, hidden_width), bf16),
            vm((width, shared_width), bf16),
            vm((width, shared_width), bf16),
            vm((width, head_width + w_key.shape[1] + w_value.shape[1]), bf16),
            vm(expert_down.shape[1:], bf16),
            vm(shared_down.shape, bf16),
            vm((parts, head_width, out_width), bf16),
            vm((head_width, 2 * out_width), bf16),
            vm((WINDOW, parts * mixer_cols), bf16),
            vm((head_width // HEAD, rows_local, 2 * HEAD), bf16),
            vm((WINDOW + rows_local, 4 * HEAD), bf16),
            vm((WINDOW, 2 * WINDOW), f32),
            vm((ring * tokens_local, out_width), f32),
            vm((2 * half, tokens_local, out_width), bf16),
            vm((2, half + 1, tokens_local, out_width), bf16),
            vm((rows_local, out_width), bf16),
            vm((tokens_local, out_width), bf16),
            dma((17,)),
            dma((pieces + 1,)),
            dma((1,)),
            dma((2, half, CHUNKS)),
            dma((half,)),
            dma((1,)),
            dma((2, pieces)),
            dma((1,)),
            dma((2, ring)),
            dma((1,)),
            dma((2, 1)),
            dma((1,)),
            dma((2, pieces)),
            dma((1,)),
            dma((1,)),
            dma((1,)),
            dma((1,)),
            dma((3,)),
            dma((3,)),
            dma((1,)),
            dma((1,)),
            dma((1,)),
            dma((2, half, PARTS_BACK)),
        ],
        compiler_params=pltpu.CompilerParams(
            collective_id=0, has_side_effects=True, vmem_limit_bytes=VMEM_LIMIT
        ),
        name="layer",
    )(
        expert_input,
        expert_gain[None, :],
        route_ids.T,
        route_weight.T,
        mixer_input,
        mixer_gain[None, :],
        query_gain[None, :],
        key_gain[None, :],
        sink_logit[None, :],
        expert_gate[0],
        expert_up[0],
        shared_gate,
        shared_up,
        w_query,
        w_key,
        w_value,
        w_output,
        expert_down[0],
        shared_down,
    )
    return outputs


def plan(*arrays):
    route_ids = arrays[11]
    capacity = 2 * route_ids.size // lax.axis_size("ep")
    whole_blocks = capacity >= route_ids.shape[0]
    fits = lax.axis_size("ep") == 8 and lax.axis_size("tp") == 4
    if whole_blocks and fits and arrays[0].shape[0] == 4 * WINDOW:
        return shards(*arrays)
    return shards_routed(*arrays)


def solution(mesh):
    in_specs = (
        P("ep", "tp"),
        P(),
        P(None, "tp"),
        P(),
        P(),
        P(),
        P(),
        P("tp"),
        P("tp", None),
        P("ep", None),
        P(),
        P("ep", None),
        P("ep", None),
        P("ep", None, "tp"),
        P("ep", None, "tp"),
        P("ep", None, "tp"),
        P(None, "tp"),
        P(None, "tp"),
        P(None, "tp"),
    )
    out_specs = (P("ep", "tp"), P("ep", "tp"))
    return jax.shard_map(plan, mesh=mesh, in_specs=in_specs, out_specs=out_specs, check_vma=False)
```

```python
import functools

import jax
import jax.numpy as jnp
from jax import lax
from jax.experimental import pallas as pl
from jax.experimental.pallas import tpu as pltpu
from jax.sharding import PartitionSpec as P

D = 2048
HEAD = 64
KV_HEADS = 2
WINDOW = 128
TOPK = 4


EPSILON = 1e-06


def from_behind(value, axis, steps):
    count = lax.axis_size(axis)
    first, last = (max(0, -steps), min(count, count - steps))
    return lax.ppermute(value, axis, [(source, source + steps) for source in range(first, last)])


def head_norm(matrix, gain_vector):
    return (
        matrix
        * lax.rsqrt(jnp.mean(matrix * matrix, axis=-1, keepdims=True) + EPSILON)
        * gain_vector
    )


def band_attend(queries, keys_own, values_own, keys_prev, values_prev, sink_logit, first_row):
    row_count = queries.shape[0]
    head_count = queries.shape[1]
    blocks = row_count // WINDOW
    keys_all = jnp.concatenate([keys_prev, keys_own], axis=0)
    values_all = jnp.concatenate([values_prev, values_own], axis=0)
    key_band = jnp.concatenate(
        [
            keys_all[:row_count].reshape(blocks, WINDOW, HEAD),
            keys_own.reshape(blocks, WINDOW, HEAD),
        ],
        axis=1,
    )
    value_band = jnp.concatenate(
        [
            values_all[:row_count].reshape(blocks, WINDOW, HEAD),
            values_own.reshape(blocks, WINDOW, HEAD),
        ],
        axis=1,
    )
    query_blocks = queries.reshape(blocks, WINDOW, head_count, HEAD)
    scores = jnp.einsum(
        "nqhd,nkd->nhqk", query_blocks, key_band, preferred_element_type=jnp.float32
    ) * HEAD ** (-0.5)
    query_idx = jnp.arange(WINDOW, dtype=jnp.int32)[:, None]
    key_idx = jnp.arange(2 * WINDOW, dtype=jnp.int32)[None, :]
    relative = query_idx + WINDOW - key_idx
    block_idx = jnp.arange(blocks, dtype=jnp.int32)[:, None, None]
    key_pos = first_row + block_idx * WINDOW - WINDOW + key_idx[None]
    allowed = ((relative >= 0) & (relative < WINDOW))[None] & (key_pos >= 0)
    allowed = allowed[:, None]
    masked = jnp.where(allowed, scores, -jnp.inf)
    sink_column = sink_logit.reshape(1, head_count, 1, 1)
    peak_score = jnp.maximum(jnp.max(masked, axis=-1, keepdims=True), sink_column)
    exponent = jnp.exp(masked - peak_score)
    denominator = jnp.sum(exponent, axis=-1, keepdims=True) + jnp.exp(sink_column - peak_score)
    probability = (exponent / denominator).astype(jnp.bfloat16)
    mixed_rows = jnp.einsum(
        "nhqk,nkd->nqhd", probability, value_band, preferred_element_type=jnp.float32
    )
    return mixed_rows.reshape(row_count, head_count * HEAD).astype(jnp.bfloat16)


def shards_routed(
    mixer_input,
    mixer_gain,
    w_query,
    w_key,
    w_value,
    query_gain,
    key_gain,
    sink_logit,
    w_output,
    expert_input,
    expert_gain,
    route_ids,
    route_weight,
    expert_gate,
    expert_up,
    expert_down,
    shared_gate,
    shared_up,
    shared_down,
):
    tp_count = lax.axis_size("tp")
    ep_count = lax.axis_size("ep")
    rows_local = mixer_input.shape[0]
    heads_local = w_query.shape[1] // HEAD
    kv_index = lax.axis_index("tp") // (tp_count // KV_HEADS)
    key_cols = lax.dynamic_slice_in_dim(w_key, kv_index * HEAD, HEAD, 1)
    value_cols = lax.dynamic_slice_in_dim(w_value, kv_index * HEAD, HEAD, 1)
    portion_float = lax.all_gather(mixer_input, "tp", axis=1, tiled=True).astype(jnp.float32)
    scaled = (portion_float * mixer_gain).astype(jnp.bfloat16)
    query_raw = jnp.dot(scaled, w_query, preferred_element_type=jnp.float32)
    key_raw = jnp.dot(scaled, key_cols, preferred_element_type=jnp.float32)
    value_raw = jnp.dot(scaled, value_cols, preferred_element_type=jnp.float32)
    squares = jnp.sum(portion_float * portion_float, axis=1)
    inv_rms = lax.rsqrt(squares / D + EPSILON)[:, None]
    queries = head_norm(query_raw.reshape(rows_local, heads_local, HEAD), query_gain).astype(
        jnp.bfloat16
    )
    keys_own = head_norm(key_raw, key_gain).astype(jnp.bfloat16)
    values_own = (value_raw * inv_rms).astype(jnp.bfloat16)
    keys_prev, values_prev = from_behind(
        (keys_own[rows_local - WINDOW :], values_own[rows_local - WINDOW :]), "ep", 1
    )
    first_row = lax.axis_index("ep") * rows_local
    attended = band_attend(
        queries, keys_own, values_own, keys_prev, values_prev, sink_logit, first_row
    )
    head_partial = jnp.dot(attended, w_output, preferred_element_type=jnp.float32)
    mixer_output = lax.psum_scatter(
        head_partial.astype(jnp.bfloat16), "tp", scatter_dimension=1, tiled=True
    )
    tokens_local = expert_input.shape[0]
    expert_float = expert_input.astype(jnp.float32)
    normed = (
        expert_float
        * lax.rsqrt(jnp.mean(expert_float * expert_float, axis=-1, keepdims=True) + EPSILON)
        * expert_gain
    ).astype(jnp.bfloat16)
    capacity = 2 * tokens_local * TOPK // ep_count
    flat_ids = route_ids.reshape(-1)
    onehot = (flat_ids[:, None] == jnp.arange(ep_count, dtype=jnp.int32)[None, :]).astype(jnp.int32)
    earlier = jnp.cumsum(onehot, axis=0) - onehot
    slot_index = jnp.sum(earlier * onehot, axis=-1)
    slot_column = flat_ids * capacity + slot_index
    token_ids = jnp.arange(tokens_local * TOPK, dtype=jnp.int32) // TOPK
    slot_table = (
        jnp.full((ep_count * capacity,), tokens_local, jnp.int32).at[slot_column].set(token_ids)
    )
    col_width = expert_down.shape[2]
    arrived_rows = ep_count * capacity
    own_columns = lax.dynamic_slice_in_dim(normed, lax.axis_index("tp") * col_width, col_width, 1)
    padded = jnp.concatenate([own_columns, jnp.zeros((1, col_width), jnp.bfloat16)], axis=0)
    outgoing = padded[slot_table].reshape(ep_count, capacity, col_width)
    arrived = lax.all_to_all(outgoing, "ep", split_axis=0, concat_axis=0, tiled=True).reshape(
        arrived_rows, col_width
    )
    portion = lax.all_gather(arrived, "tp", axis=1, tiled=True)
    gate_part = expert_gate[0]
    up_part = expert_up[0]
    gate_pre = jnp.dot(portion, gate_part, preferred_element_type=jnp.float32)
    up_pre = jnp.dot(portion, up_part, preferred_element_type=jnp.float32)
    routed_hidden = (jax.nn.silu(gate_pre) * up_pre).astype(jnp.bfloat16)
    shared_hidden = (
        jax.nn.silu(jnp.dot(normed, shared_gate, preferred_element_type=jnp.float32))
        * jnp.dot(normed, shared_up, preferred_element_type=jnp.float32)
    ).astype(jnp.bfloat16)
    routed_part = expert_down[0]
    routed_sum = jnp.dot(
        lax.all_gather(routed_hidden, "tp", axis=1, tiled=True),
        routed_part,
        preferred_element_type=jnp.float32,
    )
    shared_sum = jnp.dot(
        lax.all_gather(shared_hidden, "tp", axis=1, tiled=True),
        shared_down,
        preferred_element_type=jnp.float32,
    )
    expert_rows = routed_sum.astype(jnp.bfloat16).reshape(ep_count, capacity, col_width)
    returned = lax.all_to_all(expert_rows, "ep", split_axis=0, concat_axis=0, tiled=True).reshape(
        arrived_rows, col_width
    )
    picked = returned[slot_column].reshape(tokens_local, TOPK, col_width).astype(jnp.float32)
    expert_output = (shared_sum + jnp.sum(picked * route_weight[:, :, None], axis=1)).astype(
        jnp.bfloat16
    )
    return (mixer_output, expert_output)


CHUNKS = 2
VMEM_LIMIT = 62 * 1024 * 1024
PARTS_BACK = 4
COLUMNS_X = 2


def place_of(slot, ring):
    half = ring // 2
    return 0 if slot == 0 else 2 * slot - 1 if slot <= half else 2 * (ring - slot)


def ring_position(index, ring):
    row, side = index // COLUMNS_X, index % COLUMNS_X
    return row + side * (ring - 1 - 2 * row)


def ring_index(position, ring):
    side = position // (ring // COLUMNS_X)
    return 2 * position + side * (2 * ring - 1 - 4 * position)


def remote(source, target, send, receive, device):
    return pltpu.make_async_remote_copy(
        src_ref=source,
        dst_ref=target,
        send_sem=send,
        recv_sem=receive,
        device_id=device,
        device_id_type=pl.DeviceIdType.MESH,
    )


def limit(direction, chunk, ring):
    return ring // 2 if direction == chunk else ring // 2 - 1


def slot_at(direction, distance, ring):
    return distance if direction == 0 else ring - distance


def layer_kernel(
    ring,
    rows_hbm,
    gain_hbm,
    ids_hbm,
    weight_hbm,
    mixer_hbm,
    mixer_gain_hbm,
    query_gain_hbm,
    key_gain_hbm,
    sink_hbm,
    gate_hbm,
    up_hbm,
    shared_gate_hbm,
    shared_up_hbm,
    query_hbm,
    key_hbm,
    value_hbm,
    w_out_hbm,
    down_hbm,
    shared_down_hbm,
    mixer_result,
    expert_result,
    rows_v,
    gain_v,
    ids_v,
    weight_v,
    mixer_gain_v,
    query_gain_v,
    key_gain_v,
    sink_v,
    mixer_all,
    hidden_all,
    shared_all,
    att_all,
    dense_all,
    tok,
    gate_v,
    up_v,
    shared_gate_v,
    shared_up_v,
    qkv_v,
    down_v,
    shared_down_v,
    out_cols,
    out_stage,
    scaled_v,
    heads_v,
    band_v,
    bias_v,
    ready,
    going,
    coming,
    load_sem,
    tok_send,
    ring_recv,
    sib_recv,
    mix_send,
    mix_recv,
    hid_send,
    hid_recv,
    sh_send,
    sh_recv,
    att_send,
    att_recv,
    dense_send,
    dense_recv,
    halo_send,
    halo_recv,
    wcol_send,
    wcol_recv,
    wring_send,
    wring_recv,
    back_send,
    back_recv,
):
    scope = jax.named_scope
    f32, bf16 = jnp.float32, jnp.bfloat16
    index, part = lax.axis_index("ep"), lax.axis_index("tp")
    far, core = part // 2, part % 2
    position = ring_position(index, ring)
    peer_index = [ring_index((position + k) % ring, ring) for k in range(ring)]
    peers = [(peer_index[k], part) for k in range(1, ring)]
    ahead, behind = peers[0], peers[-1]
    sib_part = 2 * far + 1 - core
    across_part = 2 * (1 - far) + core
    corner_part = 2 * (1 - far) + 1 - core
    sibling, across = (index, sib_part), (index, across_part)
    block, width = rows_v.shape
    half_width = width // 2
    piece = block // CHUNKS
    steps = ring // 2
    parts, rows_local, mixer_cols = mixer_all.shape
    pieces = rows_local // WINDOW
    out_width = down_v.shape[1]
    inner = hidden_all.shape[2]
    shared_width = shared_all.shape[2]
    head_rows = out_cols.shape[1]
    share_rows = head_rows // ring

    barrier = pltpu.get_barrier_semaphore()
    for device in peers + [sibling, across]:
        pl.semaphore_signal(barrier, inc=1, device_id=device, device_id_type=pl.DeviceIdType.MESH)


    def start(copy):
        copy.start()

    loads = {}

    def load(name, source, target):
        loads[name] = pltpu.make_async_copy(source, target, load_sem.at[len(loads)])
        loads[name].start()

    def load_qkv(source, first):
        target = qkv_v.at[:, pl.ds(first, source.shape[1])]
        pltpu.make_async_copy(source, target, load_sem.at[len(loads)]).start()

    own_cols = pl.ds(pl.multiple_of(part * out_width, out_width), out_width)
    load("rows", rows_hbm, rows_v)
    load("gain", gain_hbm, gain_v)
    load("mixer", mixer_hbm, mixer_all.at[part])
    load("shared_gate", shared_gate_hbm, shared_gate_v)
    load("shared_up", shared_up_hbm, shared_up_v)
    load("gate", gate_hbm, gate_v)
    load("up", up_hbm, up_v)
    load("ids", ids_hbm, ids_v)
    load("weight", weight_hbm, weight_v)
    load("mixer_gain", mixer_gain_hbm, mixer_gain_v)
    load("query_gain", query_gain_hbm, query_gain_v)
    load("key_gain", key_gain_hbm, key_gain_v)
    load("sink", sink_hbm, sink_v)
    query_cols, key_cols = query_hbm.shape[1], key_hbm.shape[1]
    load_qkv(query_hbm, 0)
    load_qkv(key_hbm, query_cols)
    load_qkv(value_hbm, query_cols + key_cols)
    loads["qkv"] = pltpu.make_async_copy(qkv_v, qkv_v, load_sem.at[len(loads)])
    load("out_own", w_out_hbm.at[:, own_cols], out_cols.at[part])
    load("down", down_hbm, down_v)
    load("shared_down", shared_down_hbm, shared_down_v)

    relative = (
        lax.broadcasted_iota(jnp.int32, (WINDOW, 2 * WINDOW), 0)
        + WINDOW
        - lax.broadcasted_iota(jnp.int32, (WINDOW, 2 * WINDOW), 1)
    )
    bias_v[...] = jnp.where((relative >= 0) & (relative < WINDOW), 0.0, -jnp.inf)
    low = lax.broadcasted_iota(jnp.int32, (WINDOW, 2 * HEAD), 1) < HEAD

    with scope("norm"):
        loads["rows"].wait()
        loads["gain"].wait()
        value = rows_v[...].astype(f32)
        normed = (
            value
            * lax.rsqrt(jnp.mean(value * value, axis=-1, keepdims=True) + EPSILON)
            * gain_v[...]
        ).astype(bf16)
        tok[0, pl.ds(0, block), :] = normed[:, :half_width]
        tok[1, pl.ds(0, block), :] = normed[:, half_width:]
        loads["mixer"].wait()

    with scope("greet"):
        pl.semaphore_wait(barrier, ring + 1)

    def chunk_ref(half, slot, chunk):
        return tok.at[half, pl.ds(place_of(slot, ring) * block + chunk * piece, piece), :]

    def hop(direction, distance, chunk):
        start(
            remote(
                chunk_ref(core, slot_at(direction, distance - 1, ring) % ring, chunk),
                chunk_ref(core, slot_at(direction, distance, ring), chunk),
                tok_send.at[0],
                ring_recv.at[direction, distance - 1, chunk],
                ahead if direction == 0 else behind,
            )
        )

    def arrive(distance, k):
        for direction in range(2):
            chunk = k if direction == 0 else CHUNKS - 1 - k
            if distance > limit(direction, chunk, ring):
                continue
            here = chunk_ref(core, slot_at(direction, distance, ring), chunk)
            got = ring_recv.at[direction, distance - 1, chunk]
            remote(here, here, tok_send.at[0], got, sibling).wait_recv()
            if distance < limit(direction, chunk, ring):
                hop(direction, distance + 1, chunk)
            start(remote(here, here, tok_send.at[0], sib_recv.at[distance - 1], sibling))

    def swapped(distance):
        count = 2 if distance < steps else 1
        there = tok.at[1 - core, pl.ds((2 * distance - 1) * block, count * block), :]
        remote(there, there, tok_send.at[0], sib_recv.at[distance - 1], sibling).wait_recv()

    class Share:
        def __init__(self, view, send, receive):
            self.view, self.send, self.receive = view, send, receive

        def copy(self, owner, i, path, device):
            here = self.view(owner, i)
            return remote(here, here, self.send.at[0], self.receive.at[path, i], device)

        def to_across(self, i):
            start(self.copy(part, i, 0, across))

        def to_sibling(self, i):
            start(self.copy(part, i, 1, sibling))

        def both(self, i):
            self.to_across(i)
            self.to_sibling(i)

        def forward(self, i):
            self.copy(across_part, i, 0, sibling).wait_recv()
            start(self.copy(across_part, i, 1, sibling))

        def rest(self, i):
            self.copy(pl.ds(0, 2), i, 1, sibling).wait_recv()

    mixer = Share(
        lambda owner, i: mixer_all.at[owner, pl.ds(i * WINDOW, WINDOW), :], mix_send, mix_recv
    )
    shared = Share(lambda owner, i: shared_all.at[owner], sh_send, sh_recv)
    hidden = Share(
        lambda owner, i: hidden_all.at[owner, pl.ds(place_of(i, ring) * block, block), :],
        hid_send,
        hid_recv,
    )
    att = Share(
        lambda owner, i: att_all.at[owner, pl.ds(i * WINDOW, WINDOW), :], att_send, att_recv
    )

    for k in range(CHUNKS):
        for direction in range(2):
            hop(direction, 1, k if direction == 0 else CHUNKS - 1 - k)
    mixer.both(3)
    mixer.both(2)
    mixer.to_sibling(1)
    mixer.to_sibling(0)

    loads["ids"].wait()
    loads["weight"].wait()
    experts = lax.broadcasted_iota(jnp.int32, (ring, block), 0)
    dense = jnp.zeros((ring, block), f32)
    for k in range(TOPK):
        dense = dense + jnp.where(ids_v[k : k + 1, :] == experts, weight_v[k : k + 1, :], 0.0)
    dense_all[0] = dense
    for k in range(1, ring):
        start(
            remote(
                dense_all.at[0], dense_all.at[k], dense_send.at[0], dense_recv.at[0], peers[k - 1]
            )
        )

    def product(first, count, weights, columns):
        lower = tok[0, pl.ds(first, count), :]
        upper = tok[1, pl.ds(first, count), :]
        return jnp.dot(
            lower, weights[pl.ds(0, half_width), columns], preferred_element_type=f32
        ) + jnp.dot(
            upper, weights[pl.ds(half_width, half_width), columns], preferred_element_type=f32
        )

    with scope("c_shared"):
        loads["shared_gate"].wait()
        loads["shared_up"].wait()
        everything = pl.ds(0, shared_width)
        shared_all[part] = (
            jax.nn.silu(product(0, block, shared_gate_v, everything))
            * product(0, block, shared_up_v, everything)
        ).astype(bf16)
        shared.both(0)

    tile = 256

    def compute(slots):
        first = min(place_of(slot, ring) for slot in slots) * block
        count = len(slots) * block

        def one(j, carry):
            columns = pl.ds(pl.multiple_of(j * tile, tile), tile)
            hidden_all[part, pl.ds(first, count), columns] = (
                jax.nn.silu(product(first, count, gate_v, columns))
                * product(first, count, up_v, columns)
            ).astype(bf16)
            return carry

        lax.fori_loop(0, inner // tile, one, 0)
        for slot in slots:
            hidden.both(slot)

    def project(i):
        rows = pl.ds(i * WINDOW, WINDOW)
        mixer.rest(i)
        squares = jnp.zeros((WINDOW, 1), f32)
        for owner in range(parts):
            columns = pl.ds(owner * mixer_cols, mixer_cols)
            value = mixer_all[owner, rows, :].astype(f32)
            squares = squares + jnp.sum(value * value, axis=1, keepdims=True)
            scaled_v[:, columns] = (value * mixer_gain_v[:, columns]).astype(bf16)
        raw = jnp.dot(scaled_v[...], qkv_v[...], preferred_element_type=f32)
        lanes = 2 * HEAD
        heads = heads_v.shape[0]
        gain = query_gain_v[...] * HEAD ** (-0.5)
        gain = jnp.concatenate([gain, gain], axis=1)
        for pair in range(heads // 2):
            two = raw[:, pair * lanes : (pair + 1) * lanes]
            square = two * two
            first_sum = jnp.sum(jnp.where(low, square, 0.0), axis=1, keepdims=True)
            second_sum = jnp.sum(jnp.where(low, 0.0, square), axis=1, keepdims=True)
            inverse = lax.rsqrt(jnp.where(low, first_sum, second_sum) / HEAD + EPSILON)
            two = two * inverse * gain
            heads_v[2 * pair, rows, :] = jnp.where(low, two, 0.0).astype(bf16)
            heads_v[2 * pair + 1, rows, :] = jnp.where(low, 0.0, two).astype(bf16)
        queries_end = heads * HEAD
        second = part // (parts // KV_HEADS)
        mine = low == (second == 0)

        def twice(columns):
            return jnp.where(mine, columns, pltpu.roll(columns, HEAD, 1))

        key = twice(raw[:, queries_end : queries_end + lanes])
        gain = jnp.concatenate([key_gain_v[...], key_gain_v[...]], axis=1)
        key = key * lax.rsqrt(jnp.mean(key * key, axis=1, keepdims=True) + EPSILON) * gain
        val = twice(raw[:, queries_end + lanes : queries_end + 2 * lanes])
        val = val * lax.rsqrt(squares / D + EPSILON)
        band_v[pl.ds(WINDOW + i * WINDOW, WINDOW), :] = jnp.concatenate(
            [key, val], axis=1
        ).astype(bf16)

    halo = band_v.at[pl.ds(0, WINDOW), :]

    def send_halo():
        start(
            remote(
                band_v.at[pl.ds(rows_local, WINDOW), :],
                halo,
                halo_send.at[0],
                halo_recv.at[0],
                ((index + 1) % ring, part),
            )
        )

    def wait_halo():
        remote(halo, halo, halo_send.at[0], halo_recv.at[0], sibling).wait_recv()

    def attend(i):
        rows = pl.ds(i * WINDOW, WINDOW)
        keys = band_v[pl.ds(i * WINDOW, 2 * WINDOW), pl.ds(0, 2 * HEAD)]
        values = band_v[pl.ds(i * WINDOW, 2 * WINDOW), pl.ds(2 * HEAD, 2 * HEAD)]
        bias = bias_v[...]
        if i == 0:
            before = lax.broadcasted_iota(jnp.int32, (WINDOW, 2 * WINDOW), 1) < WINDOW
            bias = jnp.where(before & (index == 0), -jnp.inf, bias)
        mixed = []
        for head in range(heads_v.shape[0]):
            scores = lax.dot_general(
                heads_v[head, rows, :],
                keys,
                (((1,), (1,)), ((), ())),
                preferred_element_type=f32,
            )
            masked = scores + bias
            sink = sink_v[:, head : head + 1]
            peak = jnp.maximum(jnp.max(masked, axis=1, keepdims=True), sink)
            exponent = jnp.exp(masked - peak)
            denominator = jnp.sum(exponent, axis=1, keepdims=True) + jnp.exp(sink - peak)
            probability = (exponent * (1.0 / denominator)).astype(bf16)
            mixed.append(jnp.dot(probability, values, preferred_element_type=f32))
        for pair in range(len(mixed) // 2):
            att_all[part, rows, pl.ds(pair * 2 * HEAD, 2 * HEAD)] = jnp.where(
                low, mixed[2 * pair], mixed[2 * pair + 1]
            ).astype(bf16)

    chip_cols = 2 * out_width

    def spread_columns():
        start(
            remote(
                w_out_hbm.at[:, pl.ds(pl.multiple_of(sib_part * out_width, out_width), out_width)],
                out_cols.at[part],
                wcol_send.at[0],
                wcol_recv.at[0],
                sibling,
            )
        )
        mine = pl.ds(pl.multiple_of(index * share_rows, share_rows), share_rows)
        start(
            remote(
                w_out_hbm.at[
                    mine, pl.ds(pl.multiple_of((1 - far) * chip_cols, chip_cols), chip_cols)
                ],
                out_stage.at[mine, :],
                wcol_send.at[1],
                wcol_recv.at[1],
                across,
            )
        )

    def column_start():
        mine = out_stage.at[pl.ds(pl.multiple_of(index * share_rows, share_rows), share_rows), :]
        remote(mine, mine, wcol_send.at[1], wcol_recv.at[1], across).wait_recv()
        for device in peers:
            start(remote(mine, mine, wring_send.at[0], wring_recv.at[0], device))

    def column_rest():
        here = out_stage.at[pl.ds(0, (ring - 1) * share_rows), :]
        remote(here, here, wring_send.at[0], wring_recv.at[0], sibling).wait_recv()

    def column_swap():
        start(
            remote(
                out_stage.at[
                    :, pl.ds(pl.multiple_of((1 - core) * out_width, out_width), out_width)
                ],
                out_cols.at[across_part],
                wcol_send.at[2],
                wcol_recv.at[2],
                sibling,
            )
        )

    def column_wait():
        loads["out_own"].wait()
        for i, owner in ((0, sib_part), (2, corner_part)):
            here = out_cols.at[owner]
            remote(here, here, wcol_send.at[i], wcol_recv.at[i], sibling).wait_recv()

    def finish_mixer(i):
        rows = pl.ds(i * WINDOW, WINDOW)
        att.rest(i)
        total = jnp.dot(
            att_all[across_part, rows, :],
            out_stage[:, pl.ds(pl.multiple_of(core * out_width, out_width), out_width)],
            preferred_element_type=f32,
        )
        for owner in (part, sib_part, corner_part):
            total = total + jnp.dot(
                att_all[owner, rows, :], out_cols[owner], preferred_element_type=f32
            )
        mixer_result[rows, :] = total.astype(bf16)

    diagonal = lax.broadcasted_iota(jnp.int32, (block, block), 0) == lax.broadcasted_iota(
        jnp.int32, (block, block), 1
    )

    def weight_column(slot):
        row = dense_all[slot, pl.ds(index, 1), :]
        return jnp.sum(jnp.where(diagonal, row, 0.0), axis=1, keepdims=True)

    def weighted(slots):
        for slot in slots:
            hidden.rest(slot)
        first = min(place_of(slot, ring) for slot in slots) * block
        count = len(slots) * block
        total = jnp.dot(
            hidden_all[0, pl.ds(first, count), :],
            down_v[pl.ds(0, inner), :],
            preferred_element_type=f32,
        )
        for owner in range(1, parts):
            total = total + jnp.dot(
                hidden_all[owner, pl.ds(first, count), :],
                down_v[pl.ds(owner * inner, inner), :],
                preferred_element_type=f32,
            )
        rounded = total.astype(bf16).astype(f32)
        ordered = sorted(slots, key=lambda slot: place_of(slot, ring))
        ready[pl.ds(first, count), :] = rounded * jnp.concatenate(
            [weight_column(slot) for slot in ordered], axis=0
        )

    def own_rows():
        weighted([0])
        shared.rest(0)
        own = ready[pl.ds(0, block), :]
        for owner in range(parts):
            own = own + jnp.dot(
                shared_all[owner],
                shared_down_v[pl.ds(owner * shared_width, shared_width), :],
                preferred_element_type=f32,
            )
        ready[pl.ds(0, block), :] = own

    back_rows = block // PARTS_BACK

    def longest(direction, part_back):
        return limit(direction, part_back * CHUNKS // PARTS_BACK, ring)

    def back_wait(direction, distance, b):
        here = coming.at[direction, distance, pl.ds(b * back_rows, back_rows), :]
        got = back_recv.at[direction, distance - 1, b]
        remote(here, here, back_send.at[0], got, ahead).wait_recv()
        return here[...].astype(f32)

    def push(distance, long, directions=(0, 1)):
        for b in range(PARTS_BACK):
            for direction in directions:
                if (longest(direction, b) == steps) != long:
                    continue
                slot = slot_at(1 - direction, distance, ring)
                first = place_of(slot, ring) * block + b * back_rows
                value = ready[pl.ds(first, back_rows), :]
                hops = 1
                if long and distance == steps:
                    hops = 2
                elif long and distance == steps - 2:
                    hops = 2
                    value = value + back_wait(direction, distance + 1, b)
                    value = value + back_wait(direction, distance + 2, b)
                elif not long and distance < steps - 1:
                    value = value + back_wait(direction, distance + 1, b)
                rows = pl.ds(b * back_rows, back_rows)
                at = direction * steps + distance - 1
                going[at, rows, :] = value.astype(bf16)
                start(
                    remote(
                        going.at[at, rows, :],
                        coming.at[direction, distance, rows, :],
                        back_send.at[0],
                        back_recv.at[direction, distance - 1, b],
                        peers[hops - 1 if direction == 0 else -hops],
                    )
                )

    def finish_expert(b):
        rows = pl.ds(b * back_rows, back_rows)
        total = ready[rows, :]
        for direction in range(2):
            total = total + back_wait(direction, 1, b)
            if longest(direction, b) == steps:
                total = total + back_wait(direction, 2, b)
        expert_result[rows, :] = total.astype(bf16)

    with scope("c_h0"):
        loads["gate"].wait()
        loads["up"].wait()
        compute([0])
    spread_columns()
    mixer.to_across(1)
    with scope("A1c0"):
        arrive(1, 0)
    with scope("fwd_m3"):
        mixer.forward(3)
    with scope("A1c1"):
        arrive(1, 1)
    with scope("fwd_m2"):
        mixer.forward(2)
    with scope("w_qkv"):
        for name in ("mixer_gain", "query_gain", "key_gain", "sink", "qkv"):
            loads[name].wait()
    with scope("qkv3"):
        project(3)
        send_halo()
    with scope("S1"):
        swapped(1)
    with scope("c_h1"):
        compute([1, ring - 1])
    with scope("A2c0"):
        arrive(2, 0)
    with scope("qkv2"):
        project(2)
    with scope("att3"):
        attend(3)
        att.to_sibling(3)
    with scope("A2c1"):
        arrive(2, 1)
    with scope("fwd_sh_h0"):
        shared.forward(0)
        hidden.forward(0)
    with scope("S2"):
        swapped(2)
    with scope("c_h2"):
        compute([2, ring - 2])
    with scope("A3c0"):
        arrive(3, 0)
    with scope("fwd_m1"):
        mixer.forward(1)
    with scope("own"):
        loads["down"].wait()
        loads["shared_down"].wait()
        here = dense_all.at[pl.ds(1, ring - 1)]
        remote(here, here, dense_send.at[0], dense_recv.at[0], sibling).wait_recv()
        own_rows()
    with scope("qkv1"):
        project(1)
    with scope("A3c1"):
        arrive(3, 1)
    with scope("w0"):
        column_start()
    with scope("fwd_h1"):
        hidden.forward(1)
    with scope("S3"):
        swapped(3)
    with scope("c_h3"):
        compute([3, ring - 3])
    with scope("A4"):
        arrive(4, 0)
    with scope("fwd_h7"):
        hidden.forward(ring - 1)
    with scope("att2"):
        attend(2)
        att.to_sibling(2)
    with scope("S4"):
        swapped(4)
    with scope("c_h4"):
        compute([4])
    mixer.to_across(0)
    att.to_across(3)
    att.to_across(2)
    with scope("down1"):
        weighted([1, ring - 1])
    push(1, True)
    with scope("fwd_h2"):
        hidden.forward(2)
        hidden.forward(ring - 2)
    with scope("halo"):
        wait_halo()
    with scope("fwd_h3"):
        hidden.forward(3)
    with scope("down2"):
        weighted([2, ring - 2])
    with scope("down3"):
        weighted([3])
        push(3, False, (1,))
        push(3, True, (1,))
    with scope("fwd_h5"):
        hidden.forward(ring - 3)
    with scope("col_rest"):
        column_rest()
        column_swap()
    with scope("down5"):
        weighted([ring - 3])
        push(3, False, (0,))
        push(3, True, (0,))
    with scope("fwd_h4"):
        hidden.forward(4)
    with scope("down4"):
        weighted([4])
        push(4, True)
    with scope("fwd_m0"):
        mixer.forward(0)
    with scope("push2s"):
        push(2, False)
    with scope("qkv0"):
        project(0)
    with scope("att1"):
        attend(1)
        att.both(1)
    with scope("push2l"):
        push(2, True)
    with scope("push1s"):
        push(1, False)
    with scope("att0"):
        attend(0)
        att.both(0)
    with scope("fwd_a32"):
        att.forward(3)
        att.forward(2)
    with scope("fwd_a1"):
        att.forward(1)
    with scope("out3"):
        column_wait()
        finish_mixer(3)
    with scope("out2"):
        finish_mixer(2)
    with scope("fin_exp"):
        for b in range(PARTS_BACK):
            finish_expert(b)
    with scope("fwd_a0"):
        att.forward(0)
    with scope("out1"):
        finish_mixer(1)
    with scope("out0"):
        finish_mixer(0)
    with scope("w_end"):
        for ref, send in (
            (tok.at[:, pl.ds(0, (ring - 1) * block), :], tok_send.at[0]),
            (mixer_all.at[pl.ds(0, parts - 1)], mix_send.at[0]),
            (hidden_all.at[pl.ds(0, parts - 1)], hid_send.at[0]),
            (shared_all.at[pl.ds(0, parts - 1)], sh_send.at[0]),
            (att_all.at[pl.ds(0, parts - 1)], att_send.at[0]),
            (dense_all.at[pl.ds(0, ring - 1)], dense_send.at[0]),
            (halo, halo_send.at[0]),
            (out_cols.at[part], wcol_send.at[0]),
            (out_stage.at[pl.ds(0, share_rows), :], wcol_send.at[1]),
            (out_cols.at[part], wcol_send.at[2]),
            (out_stage.at[pl.ds(0, (ring - 1) * share_rows), :], wring_send.at[0]),
            (going.at[pl.ds(0, ring - 1)], back_send.at[0]),
        ):
            remote(ref, ref, send, halo_recv.at[0], sibling).wait_send()


def settle_kernel(mixer_in, expert_in, mixer_out, expert_out, sem):
    copies = [
        pltpu.make_async_copy(mixer_in, mixer_out, sem.at[0]),
        pltpu.make_async_copy(expert_in, expert_out, sem.at[1]),
    ]
    for copy in copies:
        copy.start()
    for copy in copies:
        copy.wait()


def shards(
    mixer_input,
    mixer_gain,
    w_query,
    w_key,
    w_value,
    query_gain,
    key_gain,
    sink_logit,
    w_output,
    expert_input,
    expert_gain,
    route_ids,
    route_weight,
    expert_gate,
    expert_up,
    expert_down,
    shared_gate,
    shared_up,
    shared_down,
):
    ring = lax.axis_size("ep")
    parts = lax.axis_size("tp")
    rows_local, mixer_cols = mixer_input.shape
    tokens_local, width = expert_input.shape
    hidden_width = expert_gate.shape[2]
    shared_width = shared_gate.shape[1]
    out_width = expert_down.shape[2]
    head_width = w_query.shape[1]
    pieces = rows_local // WINDOW
    half = ring // 2
    hbm = pl.BlockSpec(memory_space=pl.ANY)
    bf16, f32 = jnp.bfloat16, jnp.float32
    vm = pltpu.VMEM

    dma = pltpu.SemaphoreType.DMA
    outputs = pl.pallas_call(
        functools.partial(layer_kernel, ring),
        out_shape=(vm((rows_local, out_width), bf16), vm((tokens_local, out_width), bf16)),
        in_specs=[hbm] * 19,
        out_specs=(pl.BlockSpec(memory_space=vm),) * 2,
        scratch_shapes=[
            vm((tokens_local, width), bf16),
            vm((1, width), f32),
            vm((TOPK, tokens_local), jnp.int32),
            vm((TOPK, tokens_local), f32),
            vm((1, parts * mixer_cols), f32),
            vm((1, HEAD), f32),
            vm((1, HEAD), f32),
            vm((1, sink_logit.shape[0]), f32),
            vm((parts, rows_local, mixer_cols), bf16),
            vm((parts, ring * tokens_local, hidden_width), bf16),
            vm((parts, tokens_local, shared_width), bf16),
            vm((parts, rows_local, head_width), bf16),
            vm((ring, ring, tokens_local), f32),
            vm((2, ring * tokens_local, width // 2), bf16),
            vm((width, hidden_width), bf16),
            vm((width, hidden_width), bf16),
            vm((width, shared_width), bf16),
            vm((width, shared_width), bf16),
            vm((width, head_width + w_key.shape[1] + w_value.shape[1]), bf16),
            vm(expert_down.shape[1:], bf16),
            vm(shared_down.shape, bf16),
            vm((parts, head_width, out_width), bf16),
            vm((head_width, 2 * out_width), bf16),
            vm((WINDOW, parts * mixer_cols), bf16),
            vm((head_width // HEAD, rows_local, 2 * HEAD), bf16),
            vm((WINDOW + rows_local, 4 * HEAD), bf16),
            vm((WINDOW, 2 * WINDOW), f32),
            vm((ring * tokens_local, out_width), f32),
            vm((2 * half, tokens_local, out_width), bf16),
            vm((2, half + 1, tokens_local, out_width), bf16),
            dma((17,)),
            dma((1,)),
            dma((2, half, CHUNKS)),
            dma((half,)),
            dma((1,)),
            dma((2, pieces)),
            dma((1,)),
            dma((2, ring)),
            dma((1,)),
            dma((2, 1)),
            dma((1,)),
            dma((2, pieces)),
            dma((1,)),
            dma((1,)),
            dma((1,)),
            dma((1,)),
            dma((3,)),
            dma((3,)),
            dma((1,)),
            dma((1,)),
            dma((1,)),
            dma((2, half, PARTS_BACK)),
        ],
        compiler_params=pltpu.CompilerParams(
            collective_id=0, has_side_effects=True, vmem_limit_bytes=VMEM_LIMIT
        ),
        name="layer",
    )(
        expert_input,
        expert_gain[None, :],
        route_ids.T,
        route_weight.T,
        mixer_input,
        mixer_gain[None, :],
        query_gain[None, :],
        key_gain[None, :],
        sink_logit[None, :],
        expert_gate[0],
        expert_up[0],
        shared_gate,
        shared_up,
        w_query,
        w_key,
        w_value,
        w_output,
        expert_down[0],
        shared_down,
    )
    return pl.pallas_call(
        settle_kernel,
        out_shape=tuple(jax.ShapeDtypeStruct(o.shape, o.dtype) for o in outputs),
        in_specs=[pl.BlockSpec(memory_space=vm)] * 2,
        out_specs=(hbm,) * 2,
        scratch_shapes=[dma((2,))],
        compiler_params=pltpu.CompilerParams(vmem_limit_bytes=1024 * 1024),
        name="settle",
    )(*outputs)


def plan(*arrays):
    route_ids = arrays[11]
    capacity = 2 * route_ids.size // lax.axis_size("ep")
    whole_blocks = capacity >= route_ids.shape[0]
    fits = lax.axis_size("ep") == 8 and lax.axis_size("tp") == 4
    if whole_blocks and fits and arrays[0].shape[0] == 4 * WINDOW:
        return shards(*arrays)
    return shards_routed(*arrays)


def solution(mesh):
    in_specs = (
        P("ep", "tp"),
        P(),
        P(None, "tp"),
        P(),
        P(),
        P(),
        P(),
        P("tp"),
        P("tp", None),
        P("ep", None),
        P(),
        P("ep", None),
        P("ep", None),
        P("ep", None, "tp"),
        P("ep", None, "tp"),
        P("ep", None, "tp"),
        P(None, "tp"),
        P(None, "tp"),
        P(None, "tp"),
    )
    out_specs = (P("ep", "tp"), P("ep", "tp"))
    return jax.shard_map(plan, mesh=mesh, in_specs=in_specs, out_specs=out_specs, check_vma=False)
```

```python
import functools

import jax
import jax.numpy as jnp
from jax import lax
from jax.experimental import pallas as pl
from jax.experimental.pallas import tpu as pltpu
from jax.sharding import PartitionSpec as P

D = 2048
HEAD = 64
KV_HEADS = 2
WINDOW = 128
TOPK = 4


EPSILON = 1e-06


def from_behind(value, axis, steps):
    count = lax.axis_size(axis)
    first, last = (max(0, -steps), min(count, count - steps))
    return lax.ppermute(value, axis, [(source, source + steps) for source in range(first, last)])


def head_norm(matrix, gain_vector):
    return (
        matrix
        * lax.rsqrt(jnp.mean(matrix * matrix, axis=-1, keepdims=True) + EPSILON)
        * gain_vector
    )


def band_attend(queries, keys_own, values_own, keys_prev, values_prev, sink_logit, first_row):
    row_count = queries.shape[0]
    head_count = queries.shape[1]
    blocks = row_count // WINDOW
    keys_all = jnp.concatenate([keys_prev, keys_own], axis=0)
    values_all = jnp.concatenate([values_prev, values_own], axis=0)
    key_band = jnp.concatenate(
        [
            keys_all[:row_count].reshape(blocks, WINDOW, HEAD),
            keys_own.reshape(blocks, WINDOW, HEAD),
        ],
        axis=1,
    )
    value_band = jnp.concatenate(
        [
            values_all[:row_count].reshape(blocks, WINDOW, HEAD),
            values_own.reshape(blocks, WINDOW, HEAD),
        ],
        axis=1,
    )
    query_blocks = queries.reshape(blocks, WINDOW, head_count, HEAD)
    scores = jnp.einsum(
        "nqhd,nkd->nhqk", query_blocks, key_band, preferred_element_type=jnp.float32
    ) * HEAD ** (-0.5)
    query_idx = jnp.arange(WINDOW, dtype=jnp.int32)[:, None]
    key_idx = jnp.arange(2 * WINDOW, dtype=jnp.int32)[None, :]
    relative = query_idx + WINDOW - key_idx
    block_idx = jnp.arange(blocks, dtype=jnp.int32)[:, None, None]
    key_pos = first_row + block_idx * WINDOW - WINDOW + key_idx[None]
    allowed = ((relative >= 0) & (relative < WINDOW))[None] & (key_pos >= 0)
    allowed = allowed[:, None]
    masked = jnp.where(allowed, scores, -jnp.inf)
    sink_column = sink_logit.reshape(1, head_count, 1, 1)
    peak_score = jnp.maximum(jnp.max(masked, axis=-1, keepdims=True), sink_column)
    exponent = jnp.exp(masked - peak_score)
    denominator = jnp.sum(exponent, axis=-1, keepdims=True) + jnp.exp(sink_column - peak_score)
    probability = (exponent / denominator).astype(jnp.bfloat16)
    mixed_rows = jnp.einsum(
        "nhqk,nkd->nqhd", probability, value_band, preferred_element_type=jnp.float32
    )
    return mixed_rows.reshape(row_count, head_count * HEAD).astype(jnp.bfloat16)


def shards_routed(
    mixer_input,
    mixer_gain,
    w_query,
    w_key,
    w_value,
    query_gain,
    key_gain,
    sink_logit,
    w_output,
    expert_input,
    expert_gain,
    route_ids,
    route_weight,
    expert_gate,
    expert_up,
    expert_down,
    shared_gate,
    shared_up,
    shared_down,
):
    tp_count = lax.axis_size("tp")
    ep_count = lax.axis_size("ep")
    rows_local = mixer_input.shape[0]
    heads_local = w_query.shape[1] // HEAD
    kv_index = lax.axis_index("tp") // (tp_count // KV_HEADS)
    key_cols = lax.dynamic_slice_in_dim(w_key, kv_index * HEAD, HEAD, 1)
    value_cols = lax.dynamic_slice_in_dim(w_value, kv_index * HEAD, HEAD, 1)
    portion_float = lax.all_gather(mixer_input, "tp", axis=1, tiled=True).astype(jnp.float32)
    scaled = (portion_float * mixer_gain).astype(jnp.bfloat16)
    query_raw = jnp.dot(scaled, w_query, preferred_element_type=jnp.float32)
    key_raw = jnp.dot(scaled, key_cols, preferred_element_type=jnp.float32)
    value_raw = jnp.dot(scaled, value_cols, preferred_element_type=jnp.float32)
    squares = jnp.sum(portion_float * portion_float, axis=1)
    inv_rms = lax.rsqrt(squares / D + EPSILON)[:, None]
    queries = head_norm(query_raw.reshape(rows_local, heads_local, HEAD), query_gain).astype(
        jnp.bfloat16
    )
    keys_own = head_norm(key_raw, key_gain).astype(jnp.bfloat16)
    values_own = (value_raw * inv_rms).astype(jnp.bfloat16)
    keys_prev, values_prev = from_behind(
        (keys_own[rows_local - WINDOW :], values_own[rows_local - WINDOW :]), "ep", 1
    )
    first_row = lax.axis_index("ep") * rows_local
    attended = band_attend(
        queries, keys_own, values_own, keys_prev, values_prev, sink_logit, first_row
    )
    head_partial = jnp.dot(attended, w_output, preferred_element_type=jnp.float32)
    mixer_output = lax.psum_scatter(
        head_partial.astype(jnp.bfloat16), "tp", scatter_dimension=1, tiled=True
    )
    tokens_local = expert_input.shape[0]
    expert_float = expert_input.astype(jnp.float32)
    normed = (
        expert_float
        * lax.rsqrt(jnp.mean(expert_float * expert_float, axis=-1, keepdims=True) + EPSILON)
        * expert_gain
    ).astype(jnp.bfloat16)
    capacity = 2 * tokens_local * TOPK // ep_count
    flat_ids = route_ids.reshape(-1)
    onehot = (flat_ids[:, None] == jnp.arange(ep_count, dtype=jnp.int32)[None, :]).astype(jnp.int32)
    earlier = jnp.cumsum(onehot, axis=0) - onehot
    slot_index = jnp.sum(earlier * onehot, axis=-1)
    slot_column = flat_ids * capacity + slot_index
    token_ids = jnp.arange(tokens_local * TOPK, dtype=jnp.int32) // TOPK
    slot_table = (
        jnp.full((ep_count * capacity,), tokens_local, jnp.int32).at[slot_column].set(token_ids)
    )
    col_width = expert_down.shape[2]
    arrived_rows = ep_count * capacity
    own_columns = lax.dynamic_slice_in_dim(normed, lax.axis_index("tp") * col_width, col_width, 1)
    padded = jnp.concatenate([own_columns, jnp.zeros((1, col_width), jnp.bfloat16)], axis=0)
    outgoing = padded[slot_table].reshape(ep_count, capacity, col_width)
    arrived = lax.all_to_all(outgoing, "ep", split_axis=0, concat_axis=0, tiled=True).reshape(
        arrived_rows, col_width
    )
    portion = lax.all_gather(arrived, "tp", axis=1, tiled=True)
    gate_part = expert_gate[0]
    up_part = expert_up[0]
    gate_pre = jnp.dot(portion, gate_part, preferred_element_type=jnp.float32)
    up_pre = jnp.dot(portion, up_part, preferred_element_type=jnp.float32)
    routed_hidden = (jax.nn.silu(gate_pre) * up_pre).astype(jnp.bfloat16)
    shared_hidden = (
        jax.nn.silu(jnp.dot(normed, shared_gate, preferred_element_type=jnp.float32))
        * jnp.dot(normed, shared_up, preferred_element_type=jnp.float32)
    ).astype(jnp.bfloat16)
    routed_part = expert_down[0]
    routed_sum = jnp.dot(
        lax.all_gather(routed_hidden, "tp", axis=1, tiled=True),
        routed_part,
        preferred_element_type=jnp.float32,
    )
    shared_sum = jnp.dot(
        lax.all_gather(shared_hidden, "tp", axis=1, tiled=True),
        shared_down,
        preferred_element_type=jnp.float32,
    )
    expert_rows = routed_sum.astype(jnp.bfloat16).reshape(ep_count, capacity, col_width)
    returned = lax.all_to_all(expert_rows, "ep", split_axis=0, concat_axis=0, tiled=True).reshape(
        arrived_rows, col_width
    )
    picked = returned[slot_column].reshape(tokens_local, TOPK, col_width).astype(jnp.float32)
    expert_output = (shared_sum + jnp.sum(picked * route_weight[:, :, None], axis=1)).astype(
        jnp.bfloat16
    )
    return (mixer_output, expert_output)


CHUNKS = 2
VMEM_LIMIT = 62 * 1024 * 1024
PARTS_BACK = 4
COLUMNS_X = 2


def place_of(slot, ring):
    half = ring // 2
    return 0 if slot == 0 else 2 * slot - 1 if slot <= half else 2 * (ring - slot)


def ring_position(index, ring):
    row, side = index // COLUMNS_X, index % COLUMNS_X
    return row + side * (ring - 1 - 2 * row)


def ring_index(position, ring):
    side = position // (ring // COLUMNS_X)
    return 2 * position + side * (2 * ring - 1 - 4 * position)


def remote(source, target, send, receive, device):
    return pltpu.make_async_remote_copy(
        src_ref=source,
        dst_ref=target,
        send_sem=send,
        recv_sem=receive,
        device_id=device,
        device_id_type=pl.DeviceIdType.MESH,
    )


def limit(direction, chunk, ring):
    return ring // 2 if direction == chunk else ring // 2 - 1


def slot_at(direction, distance, ring):
    return distance if direction == 0 else ring - distance


def layer_kernel(
    ring,
    rows_hbm,
    gain_hbm,
    ids_hbm,
    weight_hbm,
    mixer_hbm,
    mixer_gain_hbm,
    query_gain_hbm,
    key_gain_hbm,
    sink_hbm,
    gate_hbm,
    up_hbm,
    shared_gate_hbm,
    shared_up_hbm,
    query_hbm,
    key_hbm,
    value_hbm,
    w_out_hbm,
    down_hbm,
    shared_down_hbm,
    mixer_result,
    expert_result,
    rows_v,
    gain_v,
    ids_v,
    weight_v,
    mixer_gain_v,
    query_gain_v,
    key_gain_v,
    sink_v,
    mixer_all,
    hidden_all,
    shared_all,
    att_all,
    dense_all,
    tok,
    gate_v,
    up_v,
    shared_gate_v,
    shared_up_v,
    qkv_v,
    down_v,
    shared_down_v,
    out_cols,
    out_stage,
    scaled_v,
    heads_v,
    band_v,
    bias_v,
    ready,
    going,
    coming,
    load_sem,
    tok_send,
    ring_recv,
    sib_recv,
    mix_send,
    mix_recv,
    hid_send,
    hid_recv,
    sh_send,
    sh_recv,
    att_send,
    att_recv,
    dense_send,
    dense_recv,
    halo_send,
    halo_recv,
    wcol_send,
    wcol_recv,
    wring_send,
    wring_recv,
    back_send,
    back_recv,
):
    scope = jax.named_scope
    f32, bf16 = jnp.float32, jnp.bfloat16
    index, part = lax.axis_index("ep"), lax.axis_index("tp")
    far, core = part // 2, part % 2
    position = ring_position(index, ring)
    peer_index = [ring_index((position + k) % ring, ring) for k in range(ring)]
    peers = [(peer_index[k], part) for k in range(1, ring)]
    ahead, behind = peers[0], peers[-1]
    sib_part = 2 * far + 1 - core
    across_part = 2 * (1 - far) + core
    corner_part = 2 * (1 - far) + 1 - core
    sibling, across = (index, sib_part), (index, across_part)
    block, width = rows_v.shape
    half_width = width // 2
    piece = block // CHUNKS
    steps = ring // 2
    parts, rows_local, mixer_cols = mixer_all.shape
    pieces = rows_local // WINDOW
    out_width = down_v.shape[1]
    inner = hidden_all.shape[2]
    shared_width = shared_all.shape[2]
    head_rows = out_cols.shape[1]
    share_rows = head_rows // ring
    share_piece = share_rows // CHUNKS

    barrier = pltpu.get_barrier_semaphore()
    for device in peers + [sibling, across]:
        pl.semaphore_signal(barrier, inc=1, device_id=device, device_id_type=pl.DeviceIdType.MESH)


    def start(copy):
        copy.start()

    loads = {}

    def load(name, source, target):
        loads[name] = pltpu.make_async_copy(source, target, load_sem.at[len(loads)])
        loads[name].start()

    def load_qkv(source, first):
        target = qkv_v.at[:, pl.ds(first, source.shape[1])]
        pltpu.make_async_copy(source, target, load_sem.at[len(loads)]).start()

    own_cols = pl.ds(pl.multiple_of(part * out_width, out_width), out_width)
    load("rows", rows_hbm, rows_v)
    load("gain", gain_hbm, gain_v)
    load("mixer", mixer_hbm, mixer_all.at[part])
    load("shared_gate", shared_gate_hbm, shared_gate_v)
    load("shared_up", shared_up_hbm, shared_up_v)
    load("gate", gate_hbm, gate_v)
    load("up", up_hbm, up_v)
    load("ids", ids_hbm, ids_v)
    load("weight", weight_hbm, weight_v)
    load("mixer_gain", mixer_gain_hbm, mixer_gain_v)
    load("query_gain", query_gain_hbm, query_gain_v)
    load("key_gain", key_gain_hbm, key_gain_v)
    load("sink", sink_hbm, sink_v)
    query_cols, key_cols = query_hbm.shape[1], key_hbm.shape[1]
    load_qkv(query_hbm, 0)
    load_qkv(key_hbm, query_cols)
    load_qkv(value_hbm, query_cols + key_cols)
    loads["qkv"] = pltpu.make_async_copy(qkv_v, qkv_v, load_sem.at[len(loads)])
    load("out_own", w_out_hbm.at[:, own_cols], out_cols.at[part])
    load("down", down_hbm, down_v)
    load("shared_down", shared_down_hbm, shared_down_v)

    band_shape = (2 * WINDOW, WINDOW)
    relative = (
        lax.broadcasted_iota(jnp.int32, band_shape, 1)
        + WINDOW
        - lax.broadcasted_iota(jnp.int32, band_shape, 0)
    )
    bias_v[...] = jnp.where((relative >= 0) & (relative < WINDOW), 0.0, -jnp.inf)
    low = lax.broadcasted_iota(jnp.int32, (WINDOW, 2 * HEAD), 1) < HEAD

    with scope("norm"):
        loads["rows"].wait()
        loads["gain"].wait()
        value = rows_v[...].astype(f32)
        normed = (
            value
            * lax.rsqrt(jnp.mean(value * value, axis=-1, keepdims=True) + EPSILON)
            * gain_v[...]
        ).astype(bf16)
        tok[0, pl.ds(0, block), :] = normed[:, :half_width]
        tok[1, pl.ds(0, block), :] = normed[:, half_width:]
        loads["mixer"].wait()

    with scope("greet"):
        pl.semaphore_wait(barrier, ring + 1)

    def chunk_ref(half, slot, chunk):
        return tok.at[half, pl.ds(place_of(slot, ring) * block + chunk * piece, piece), :]

    def hop(direction, distance, chunk):
        start(
            remote(
                chunk_ref(core, slot_at(direction, distance - 1, ring) % ring, chunk),
                chunk_ref(core, slot_at(direction, distance, ring), chunk),
                tok_send.at[0],
                ring_recv.at[direction, distance - 1, chunk],
                ahead if direction == 0 else behind,
            )
        )

    def arrive(distance, k):
        for direction in range(2):
            chunk = k if direction == 0 else CHUNKS - 1 - k
            if distance > limit(direction, chunk, ring):
                continue
            here = chunk_ref(core, slot_at(direction, distance, ring), chunk)
            got = ring_recv.at[direction, distance - 1, chunk]
            remote(here, here, tok_send.at[0], got, sibling).wait_recv()
            if distance < limit(direction, chunk, ring):
                hop(direction, distance + 1, chunk)
            start(remote(here, here, tok_send.at[0], sib_recv.at[distance - 1], sibling))

    def swapped(distance):
        count = 2 if distance < steps else 1
        there = tok.at[1 - core, pl.ds((2 * distance - 1) * block, count * block), :]
        remote(there, there, tok_send.at[0], sib_recv.at[distance - 1], sibling).wait_recv()

    class Share:
        def __init__(self, view, send, receive):
            self.view, self.send, self.receive = view, send, receive

        def copy(self, owner, i, path, device):
            here = self.view(owner, i)
            return remote(here, here, self.send.at[0], self.receive.at[path, i], device)

        def to_across(self, i):
            start(self.copy(part, i, 0, across))

        def to_sibling(self, i):
            start(self.copy(part, i, 1, sibling))

        def both(self, i):
            self.to_across(i)
            self.to_sibling(i)

        def forward(self, i):
            self.copy(across_part, i, 0, sibling).wait_recv()
            start(self.copy(across_part, i, 1, sibling))

        def rest(self, i):
            self.copy(pl.ds(0, 2), i, 1, sibling).wait_recv()

    mixer = Share(
        lambda owner, i: mixer_all.at[owner, pl.ds(i * WINDOW, WINDOW), :], mix_send, mix_recv
    )
    shared = Share(lambda owner, i: shared_all.at[owner], sh_send, sh_recv)
    hidden = Share(
        lambda owner, i: hidden_all.at[owner, pl.ds(place_of(i, ring) * block, block), :],
        hid_send,
        hid_recv,
    )
    att = Share(
        lambda owner, i: att_all.at[owner, pl.ds(i * WINDOW, WINDOW), :], att_send, att_recv
    )

    for k in range(CHUNKS):
        for direction in range(2):
            hop(direction, 1, k if direction == 0 else CHUNKS - 1 - k)
    mixer.both(3)
    mixer.both(2)
    mixer.to_sibling(1)
    mixer.to_sibling(0)

    loads["ids"].wait()
    loads["weight"].wait()
    experts = lax.broadcasted_iota(jnp.int32, (ring, block), 0)
    dense = jnp.zeros((ring, block), f32)
    for k in range(TOPK):
        dense = dense + jnp.where(ids_v[k : k + 1, :] == experts, weight_v[k : k + 1, :], 0.0)
    dense_all[0] = dense
    for k in range(1, ring):
        start(
            remote(
                dense_all.at[0], dense_all.at[k], dense_send.at[0], dense_recv.at[0], peers[k - 1]
            )
        )

    def product(first, count, weights, columns):
        lower = tok[0, pl.ds(first, count), :]
        upper = tok[1, pl.ds(first, count), :]
        return jnp.dot(
            lower, weights[pl.ds(0, half_width), columns], preferred_element_type=f32
        ) + jnp.dot(
            upper, weights[pl.ds(half_width, half_width), columns], preferred_element_type=f32
        )

    with scope("c_shared"):
        loads["shared_gate"].wait()
        loads["shared_up"].wait()
        everything = pl.ds(0, shared_width)
        shared_all[part] = (
            jax.nn.silu(product(0, block, shared_gate_v, everything))
            * product(0, block, shared_up_v, everything)
        ).astype(bf16)
        shared.both(0)

    tile = 256

    def compute(slots, now):
        first = min(place_of(slot, ring) for slot in slots) * block
        count = len(slots) * block

        def one(j, carry):
            columns = pl.ds(pl.multiple_of(j * tile, tile), tile)
            hidden_all[part, pl.ds(first, count), columns] = (
                jax.nn.silu(product(first, count, gate_v, columns))
                * product(first, count, up_v, columns)
            ).astype(bf16)
            return carry

        lax.fori_loop(0, inner // tile, one, 0)
        for slot in slots:
            hidden.to_sibling(slot)
            if slot in now:
                hidden.to_across(slot)

    def project(i):
        rows = pl.ds(i * WINDOW, WINDOW)
        mixer.rest(i)
        squares = jnp.zeros((WINDOW, 1), f32)
        for owner in range(parts):
            columns = pl.ds(owner * mixer_cols, mixer_cols)
            value = mixer_all[owner, rows, :].astype(f32)
            squares = squares + jnp.sum(value * value, axis=1, keepdims=True)
            scaled_v[:, columns] = (value * mixer_gain_v[:, columns]).astype(bf16)
        raw = jnp.dot(scaled_v[...], qkv_v[...], preferred_element_type=f32)
        lanes = 2 * HEAD
        heads = heads_v.shape[0]
        gain = query_gain_v[...] * HEAD ** (-0.5)
        gain = jnp.concatenate([gain, gain], axis=1)
        for pair in range(heads // 2):
            two = raw[:, pair * lanes : (pair + 1) * lanes]
            square = two * two
            first_sum = jnp.sum(jnp.where(low, square, 0.0), axis=1, keepdims=True)
            second_sum = jnp.sum(jnp.where(low, 0.0, square), axis=1, keepdims=True)
            inverse = lax.rsqrt(jnp.where(low, first_sum, second_sum) / HEAD + EPSILON)
            two = two * inverse * gain
            heads_v[2 * pair, rows, :] = jnp.where(low, two, 0.0).astype(bf16)
            heads_v[2 * pair + 1, rows, :] = jnp.where(low, 0.0, two).astype(bf16)
        queries_end = heads * HEAD
        second = part // (parts // KV_HEADS)
        mine = low == (second == 0)

        def twice(columns):
            return jnp.where(mine, columns, pltpu.roll(columns, HEAD, 1))

        key = twice(raw[:, queries_end : queries_end + lanes])
        gain = jnp.concatenate([key_gain_v[...], key_gain_v[...]], axis=1)
        key = key * lax.rsqrt(jnp.mean(key * key, axis=1, keepdims=True) + EPSILON) * gain
        val = twice(raw[:, queries_end + lanes : queries_end + 2 * lanes])
        val = val * lax.rsqrt(squares / D + EPSILON)
        band_v[pl.ds(WINDOW + i * WINDOW, WINDOW), :] = jnp.concatenate(
            [key, val], axis=1
        ).astype(bf16)

    halo = band_v.at[pl.ds(0, WINDOW), :]

    def send_halo():
        start(
            remote(
                band_v.at[pl.ds(rows_local, WINDOW), :],
                halo,
                halo_send.at[0],
                halo_recv.at[0],
                ((index + 1) % ring, part),
            )
        )

    def wait_halo():
        remote(halo, halo, halo_send.at[0], halo_recv.at[0], sibling).wait_recv()

    def attend(i):
        rows = pl.ds(i * WINDOW, WINDOW)
        heads = heads_v.shape[0]
        keys = band_v[pl.ds(i * WINDOW, 2 * WINDOW), pl.ds(0, 2 * HEAD)]
        values = band_v[pl.ds(i * WINDOW, 2 * WINDOW), pl.ds(2 * HEAD, 2 * HEAD)]
        bias = bias_v[...]
        if i == 0:
            before = lax.broadcasted_iota(jnp.int32, band_shape, 0) < WINDOW
            bias = jnp.where(before & (index == 0), -jnp.inf, bias)
        scores = lax.dot_general(
            keys,
            heads_v[:, rows, :].reshape(heads * WINDOW, 2 * HEAD),
            (((1,), (1,)), ((), ())),
            preferred_element_type=f32,
        )
        columns = []
        for head in range(heads):
            masked = scores[:, head * WINDOW : (head + 1) * WINDOW] + bias
            sink = sink_v[:, head : head + 1]
            peak = jnp.maximum(jnp.max(masked, axis=0, keepdims=True), sink)
            exponent = jnp.exp(masked - peak)
            denominator = jnp.sum(exponent, axis=0, keepdims=True) + jnp.exp(sink - peak)
            columns.append((exponent * (1.0 / denominator)).astype(bf16))
        mixed = lax.dot_general(
            values[:, :HEAD],
            jnp.concatenate(columns, axis=1),
            (((0,), (0,)), ((), ())),
            preferred_element_type=f32,
        )
        for pair in range(heads // 2):
            first = 2 * pair * WINDOW
            two = jnp.concatenate(
                [mixed[:, first : first + WINDOW], mixed[:, first + WINDOW : first + 2 * WINDOW]],
                axis=0,
            )
            att_all[part, rows, pl.ds(pair * 2 * HEAD, 2 * HEAD)] = two.T.astype(bf16)

    chip_cols = 2 * out_width

    def spread_columns():
        start(
            remote(
                w_out_hbm.at[:, pl.ds(pl.multiple_of(sib_part * out_width, out_width), out_width)],
                out_cols.at[part],
                wcol_send.at[0],
                wcol_recv.at[0],
                sibling,
            )
        )
        mine = pl.ds(pl.multiple_of(index * share_rows, share_rows), share_rows)
        start(
            remote(
                w_out_hbm.at[
                    mine, pl.ds(pl.multiple_of((1 - far) * chip_cols, chip_cols), chip_cols)
                ],
                out_stage.at[mine, :],
                wcol_send.at[1],
                wcol_recv.at[1],
                across,
            )
        )

    def stage_ref(slot, chunk):
        owner = peer_index[(ring - slot) % ring]
        first = owner * share_rows + chunk * share_piece
        return out_stage.at[pl.ds(pl.multiple_of(first, share_piece), share_piece), :]

    def column_hop(direction, distance, chunk):
        here = stage_ref(slot_at(direction, distance - 1, ring) % ring, chunk)
        to = ahead if direction == 0 else behind
        start(remote(here, here, wring_send.at[0], wring_recv.at[distance - 1], to))

    def column_start():
        mine = out_stage.at[pl.ds(pl.multiple_of(index * share_rows, share_rows), share_rows), :]
        remote(mine, mine, wcol_send.at[1], wcol_recv.at[1], across).wait_recv()
        for chunk in range(CHUNKS):
            for direction in range(2):
                column_hop(direction, 1, chunk)

    def column_arrive(distance):
        count = 2 if distance < steps else 1
        here = out_stage.at[pl.ds(0, count * share_rows), :]
        remote(here, here, wring_send.at[0], wring_recv.at[distance - 1], sibling).wait_recv()
        for chunk in range(CHUNKS):
            for direction in range(2):
                if distance < limit(direction, chunk, ring):
                    column_hop(direction, distance + 1, chunk)

    def column_swap():
        start(
            remote(
                out_stage.at[
                    :, pl.ds(pl.multiple_of((1 - core) * out_width, out_width), out_width)
                ],
                out_cols.at[across_part],
                wcol_send.at[2],
                wcol_recv.at[2],
                sibling,
            )
        )

    def column_wait():
        loads["out_own"].wait()
        for i, owner in ((0, sib_part), (2, corner_part)):
            here = out_cols.at[owner]
            remote(here, here, wcol_send.at[i], wcol_recv.at[i], sibling).wait_recv()

    def finish_mixer(i):
        rows = pl.ds(i * WINDOW, WINDOW)
        att.rest(i)
        total = jnp.dot(
            att_all[across_part, rows, :],
            out_stage[:, pl.ds(pl.multiple_of(core * out_width, out_width), out_width)],
            preferred_element_type=f32,
        )
        for owner in (part, sib_part, corner_part):
            total = total + jnp.dot(
                att_all[owner, rows, :], out_cols[owner], preferred_element_type=f32
            )
        mixer_result[rows, :] = total.astype(bf16)

    diagonal = lax.broadcasted_iota(jnp.int32, (block, block), 0) == lax.broadcasted_iota(
        jnp.int32, (block, block), 1
    )

    def weight_column(slot):
        row = dense_all[slot, pl.ds(index, 1), :]
        return jnp.sum(jnp.where(diagonal, row, 0.0), axis=1, keepdims=True)

    def weighted(slots):
        for slot in slots:
            hidden.rest(slot)
        first = min(place_of(slot, ring) for slot in slots) * block
        count = len(slots) * block
        total = jnp.dot(
            hidden_all[0, pl.ds(first, count), :],
            down_v[pl.ds(0, inner), :],
            preferred_element_type=f32,
        )
        for owner in range(1, parts):
            total = total + jnp.dot(
                hidden_all[owner, pl.ds(first, count), :],
                down_v[pl.ds(owner * inner, inner), :],
                preferred_element_type=f32,
            )
        rounded = total.astype(bf16).astype(f32)
        ordered = sorted(slots, key=lambda slot: place_of(slot, ring))
        ready[pl.ds(first, count), :] = rounded * jnp.concatenate(
            [weight_column(slot) for slot in ordered], axis=0
        )

    def own_rows():
        weighted([0])
        shared.rest(0)
        own = ready[pl.ds(0, block), :]
        for owner in range(parts):
            own = own + jnp.dot(
                shared_all[owner],
                shared_down_v[pl.ds(owner * shared_width, shared_width), :],
                preferred_element_type=f32,
            )
        ready[pl.ds(0, block), :] = own

    back_rows = block // PARTS_BACK

    def longest(direction, part_back):
        return limit(direction, part_back * CHUNKS // PARTS_BACK, ring)

    def back_wait(direction, distance, b):
        here = coming.at[direction, distance, pl.ds(b * back_rows, back_rows), :]
        got = back_recv.at[direction, distance - 1, b]
        remote(here, here, back_send.at[0], got, ahead).wait_recv()
        return here[...].astype(f32)

    def push(distance, long, directions=(0, 1)):
        for b in range(PARTS_BACK):
            for direction in directions:
                if (longest(direction, b) == steps) != long:
                    continue
                slot = slot_at(1 - direction, distance, ring)
                first = place_of(slot, ring) * block + b * back_rows
                value = ready[pl.ds(first, back_rows), :]
                hops = 1
                if long and distance == steps:
                    hops = 2
                elif long and distance == steps - 2:
                    hops = 2
                    value = value + back_wait(direction, distance + 1, b)
                    value = value + back_wait(direction, distance + 2, b)
                elif not long and distance < steps - 1:
                    value = value + back_wait(direction, distance + 1, b)
                rows = pl.ds(b * back_rows, back_rows)
                at = direction * steps + distance - 1
                going[at, rows, :] = value.astype(bf16)
                start(
                    remote(
                        going.at[at, rows, :],
                        coming.at[direction, distance, rows, :],
                        back_send.at[0],
                        back_recv.at[direction, distance - 1, b],
                        peers[hops - 1 if direction == 0 else -hops],
                    )
                )

    def finish_expert(b):
        rows = pl.ds(b * back_rows, back_rows)
        total = ready[rows, :]
        for direction in range(2):
            total = total + back_wait(direction, 1, b)
            if longest(direction, b) == steps:
                total = total + back_wait(direction, 2, b)
        expert_result[rows, :] = total.astype(bf16)

    with scope("c_h0"):
        loads["gate"].wait()
        loads["up"].wait()
        compute([0], [])
    spread_columns()
    mixer.to_across(1)
    mixer.to_across(0)
    with scope("A1c0"):
        arrive(1, 0)
    with scope("fwd_m3"):
        mixer.forward(3)
    with scope("A1c1"):
        arrive(1, 1)
    with scope("fwd_m2"):
        mixer.forward(2)
    with scope("w_qkv"):
        for name in ("mixer_gain", "query_gain", "key_gain", "sink", "qkv"):
            loads[name].wait()
    with scope("qkv3"):
        project(3)
        send_halo()
    with scope("S1"):
        swapped(1)
    with scope("c_h1"):
        compute([1, ring - 1], [1, ring - 1])
    with scope("A2c0"):
        arrive(2, 0)
    with scope("qkv2"):
        project(2)
    with scope("att3"):
        attend(3)
        att.to_sibling(3)
    with scope("fwd_sh_m1"):
        shared.forward(0)
        mixer.forward(1)
    with scope("A2c1"):
        arrive(2, 1)
    with scope("S2"):
        swapped(2)
    with scope("c_h2"):
        compute([2, ring - 2], [2])
    with scope("A3c0"):
        arrive(3, 0)
    with scope("fwd_m0"):
        mixer.forward(0)
    att.to_across(3)
    with scope("qkv1"):
        project(1)
    with scope("att2"):
        attend(2)
        att.to_sibling(2)
    with scope("A3c1"):
        arrive(3, 1)
    with scope("w0"):
        column_start()
    with scope("fwd_h1"):
        hidden.forward(1)
    with scope("qkv0"):
        project(0)
    with scope("S3"):
        swapped(3)
    with scope("c_h3"):
        compute([3, ring - 3], [3, ring - 3])
    with scope("A4"):
        arrive(4, 0)
    with scope("w1"):
        column_arrive(1)
    with scope("fwd_h7"):
        hidden.forward(ring - 1)
    with scope("att1"):
        attend(1)
        att.to_sibling(1)
    with scope("halo"):
        wait_halo()
    with scope("att0"):
        attend(0)
        att.to_sibling(0)
    with scope("S4"):
        swapped(4)
    with scope("c_h4"):
        compute([4], [4])
    hidden.to_across(ring - 2)
    hidden.to_across(0)
    for i in (2, 1, 0):
        att.to_across(i)
    with scope("fwd_h2"):
        hidden.forward(2)
    with scope("w_dense"):
        loads["down"].wait()
        loads["shared_down"].wait()
        here = dense_all.at[pl.ds(1, ring - 1)]
        remote(here, here, dense_send.at[0], dense_recv.at[0], sibling).wait_recv()
    with scope("down1"):
        weighted([1, ring - 1])
        push(1, True)
    with scope("w2"):
        column_arrive(2)
    with scope("down2"):
        weighted([2])
    with scope("fwd_h3"):
        att.forward(3)
        hidden.forward(3)
    with scope("down3"):
        weighted([3])
        push(3, False, (1,))
        push(3, True, (1,))
    with scope("fwd_h5"):
        hidden.forward(ring - 3)
    with scope("w3"):
        column_arrive(3)
    with scope("down5"):
        weighted([ring - 3])
        push(3, False, (0,))
        push(3, True, (0,))
    with scope("fwd_h4"):
        hidden.forward(4)
    with scope("push2s1"):
        push(2, False, (1,))
    with scope("down4"):
        weighted([4])
        push(4, True)
    with scope("fwd_h6"):
        hidden.forward(ring - 2)
    with scope("w4"):
        column_arrive(4)
        column_swap()
    with scope("down6"):
        weighted([ring - 2])
    with scope("push1s1"):
        push(1, False, (1,))
    with scope("push2s0"):
        push(2, False, (0,))
    with scope("fwd_h0"):
        hidden.forward(0)
    with scope("push2l1"):
        push(2, True, (1,))
    with scope("push2l0"):
        push(2, True, (0,))
    with scope("fwd_a2"):
        att.forward(2)
    with scope("own"):
        own_rows()
    with scope("push1s0"):
        push(1, False, (0,))
    with scope("fwd_a1"):
        att.forward(1)
    with scope("out3"):
        column_wait()
        finish_mixer(3)
    with scope("out2"):
        finish_mixer(2)
    with scope("fwd_a0"):
        att.forward(0)
    with scope("out1"):
        finish_mixer(1)
    with scope("out0"):
        finish_mixer(0)
    with scope("fin_exp"):
        for b in range(PARTS_BACK):
            finish_expert(b)
    with scope("w_end"):
        for ref, send in (
            (tok.at[:, pl.ds(0, (ring - 1) * block), :], tok_send.at[0]),
            (mixer_all.at[pl.ds(0, parts - 1)], mix_send.at[0]),
            (hidden_all.at[pl.ds(0, parts - 1)], hid_send.at[0]),
            (shared_all.at[pl.ds(0, parts - 1)], sh_send.at[0]),
            (att_all.at[pl.ds(0, parts - 1)], att_send.at[0]),
            (dense_all.at[pl.ds(0, ring - 1)], dense_send.at[0]),
            (halo, halo_send.at[0]),
            (out_cols.at[part], wcol_send.at[0]),
            (out_stage.at[pl.ds(0, share_rows), :], wcol_send.at[1]),
            (out_cols.at[part], wcol_send.at[2]),
            (out_stage.at[pl.ds(0, (ring - 1) * share_rows), :], wring_send.at[0]),
            (going.at[pl.ds(0, ring - 1)], back_send.at[0]),
        ):
            remote(ref, ref, send, halo_recv.at[0], sibling).wait_send()


def settle_kernel(mixer_in, expert_in, mixer_out, expert_out, sem):
    copies = [
        pltpu.make_async_copy(mixer_in, mixer_out, sem.at[0]),
        pltpu.make_async_copy(expert_in, expert_out, sem.at[1]),
    ]
    for copy in copies:
        copy.start()
    for copy in copies:
        copy.wait()


def shards(
    mixer_input,
    mixer_gain,
    w_query,
    w_key,
    w_value,
    query_gain,
    key_gain,
    sink_logit,
    w_output,
    expert_input,
    expert_gain,
    route_ids,
    route_weight,
    expert_gate,
    expert_up,
    expert_down,
    shared_gate,
    shared_up,
    shared_down,
):
    ring = lax.axis_size("ep")
    parts = lax.axis_size("tp")
    rows_local, mixer_cols = mixer_input.shape
    tokens_local, width = expert_input.shape
    hidden_width = expert_gate.shape[2]
    shared_width = shared_gate.shape[1]
    out_width = expert_down.shape[2]
    head_width = w_query.shape[1]
    pieces = rows_local // WINDOW
    half = ring // 2
    hbm = pl.BlockSpec(memory_space=pl.ANY)
    bf16, f32 = jnp.bfloat16, jnp.float32
    vm = pltpu.VMEM

    dma = pltpu.SemaphoreType.DMA
    outputs = pl.pallas_call(
        functools.partial(layer_kernel, ring),
        out_shape=(vm((rows_local, out_width), bf16), vm((tokens_local, out_width), bf16)),
        in_specs=[hbm] * 19,
        out_specs=(pl.BlockSpec(memory_space=vm),) * 2,
        scratch_shapes=[
            vm((tokens_local, width), bf16),
            vm((1, width), f32),
            vm((TOPK, tokens_local), jnp.int32),
            vm((TOPK, tokens_local), f32),
            vm((1, parts * mixer_cols), f32),
            vm((1, HEAD), f32),
            vm((1, HEAD), f32),
            vm((1, sink_logit.shape[0]), f32),
            vm((parts, rows_local, mixer_cols), bf16),
            vm((parts, ring * tokens_local, hidden_width), bf16),
            vm((parts, tokens_local, shared_width), bf16),
            vm((parts, rows_local, head_width), bf16),
            vm((ring, ring, tokens_local), f32),
            vm((2, ring * tokens_local, width // 2), bf16),
            vm((width, hidden_width), bf16),
            vm((width, hidden_width), bf16),
            vm((width, shared_width), bf16),
            vm((width, shared_width), bf16),
            vm((width, head_width + w_key.shape[1] + w_value.shape[1]), bf16),
            vm(expert_down.shape[1:], bf16),
            vm(shared_down.shape, bf16),
            vm((parts, head_width, out_width), bf16),
            vm((head_width, 2 * out_width), bf16),
            vm((WINDOW, parts * mixer_cols), bf16),
            vm((head_width // HEAD, rows_local, 2 * HEAD), bf16),
            vm((WINDOW + rows_local, 4 * HEAD), bf16),
            vm((2 * WINDOW, WINDOW), f32),
            vm((ring * tokens_local, out_width), f32),
            vm((2 * half, tokens_local, out_width), bf16),
            vm((2, half + 1, tokens_local, out_width), bf16),
            dma((17,)),
            dma((1,)),
            dma((2, half, CHUNKS)),
            dma((half,)),
            dma((1,)),
            dma((2, pieces)),
            dma((1,)),
            dma((2, ring)),
            dma((1,)),
            dma((2, 1)),
            dma((1,)),
            dma((2, pieces)),
            dma((1,)),
            dma((1,)),
            dma((1,)),
            dma((1,)),
            dma((3,)),
            dma((3,)),
            dma((1,)),
            dma((half,)),
            dma((1,)),
            dma((2, half, PARTS_BACK)),
        ],
        compiler_params=pltpu.CompilerParams(
            collective_id=0, has_side_effects=True, vmem_limit_bytes=VMEM_LIMIT
        ),
        name="layer",
    )(
        expert_input,
        expert_gain[None, :],
        route_ids.T,
        route_weight.T,
        mixer_input,
        mixer_gain[None, :],
        query_gain[None, :],
        key_gain[None, :],
        sink_logit[None, :],
        expert_gate[0],
        expert_up[0],
        shared_gate,
        shared_up,
        w_query,
        w_key,
        w_value,
        w_output,
        expert_down[0],
        shared_down,
    )
    return pl.pallas_call(
        settle_kernel,
        out_shape=tuple(jax.ShapeDtypeStruct(o.shape, o.dtype) for o in outputs),
        in_specs=[pl.BlockSpec(memory_space=vm)] * 2,
        out_specs=(hbm,) * 2,
        scratch_shapes=[dma((2,))],
        compiler_params=pltpu.CompilerParams(vmem_limit_bytes=1024 * 1024),
        name="settle",
    )(*outputs)


def plan(*arrays):
    route_ids = arrays[11]
    capacity = 2 * route_ids.size // lax.axis_size("ep")
    whole_blocks = capacity >= route_ids.shape[0]
    fits = lax.axis_size("ep") == 8 and lax.axis_size("tp") == 4
    if whole_blocks and fits and arrays[0].shape[0] == 4 * WINDOW:
        return shards(*arrays)
    return shards_routed(*arrays)


def solution(mesh):
    in_specs = (
        P("ep", "tp"),
        P(),
        P(None, "tp"),
        P(),
        P(),
        P(),
        P(),
        P("tp"),
        P("tp", None),
        P("ep", None),
        P(),
        P("ep", None),
        P("ep", None),
        P("ep", None, "tp"),
        P("ep", None, "tp"),
        P("ep", None, "tp"),
        P(None, "tp"),
        P(None, "tp"),
        P(None, "tp"),
    )
    out_specs = (P("ep", "tp"), P("ep", "tp"))
    return jax.shard_map(plan, mesh=mesh, in_specs=in_specs, out_specs=out_specs, check_vma=False)
```

```python
import functools

import jax
import jax.numpy as jnp
from jax import lax
from jax.experimental import pallas as pl
from jax.experimental.pallas import tpu as pltpu
from jax.sharding import PartitionSpec as P

D = 2048
HEAD = 64
KV_HEADS = 2
WINDOW = 128
TOPK = 4


EPSILON = 1e-06


def from_behind(value, axis, steps):
    count = lax.axis_size(axis)
    first, last = (max(0, -steps), min(count, count - steps))
    return lax.ppermute(value, axis, [(source, source + steps) for source in range(first, last)])


def head_norm(matrix, gain_vector):
    return (
        matrix
        * lax.rsqrt(jnp.mean(matrix * matrix, axis=-1, keepdims=True) + EPSILON)
        * gain_vector
    )


def band_attend(queries, keys_own, values_own, keys_prev, values_prev, sink_logit, first_row):
    row_count = queries.shape[0]
    head_count = queries.shape[1]
    blocks = row_count // WINDOW
    keys_all = jnp.concatenate([keys_prev, keys_own], axis=0)
    values_all = jnp.concatenate([values_prev, values_own], axis=0)
    key_band = jnp.concatenate(
        [
            keys_all[:row_count].reshape(blocks, WINDOW, HEAD),
            keys_own.reshape(blocks, WINDOW, HEAD),
        ],
        axis=1,
    )
    value_band = jnp.concatenate(
        [
            values_all[:row_count].reshape(blocks, WINDOW, HEAD),
            values_own.reshape(blocks, WINDOW, HEAD),
        ],
        axis=1,
    )
    query_blocks = queries.reshape(blocks, WINDOW, head_count, HEAD)
    scores = jnp.einsum(
        "nqhd,nkd->nhqk", query_blocks, key_band, preferred_element_type=jnp.float32
    ) * HEAD ** (-0.5)
    query_idx = jnp.arange(WINDOW, dtype=jnp.int32)[:, None]
    key_idx = jnp.arange(2 * WINDOW, dtype=jnp.int32)[None, :]
    relative = query_idx + WINDOW - key_idx
    block_idx = jnp.arange(blocks, dtype=jnp.int32)[:, None, None]
    key_pos = first_row + block_idx * WINDOW - WINDOW + key_idx[None]
    allowed = ((relative >= 0) & (relative < WINDOW))[None] & (key_pos >= 0)
    allowed = allowed[:, None]
    masked = jnp.where(allowed, scores, -jnp.inf)
    sink_column = sink_logit.reshape(1, head_count, 1, 1)
    peak_score = jnp.maximum(jnp.max(masked, axis=-1, keepdims=True), sink_column)
    exponent = jnp.exp(masked - peak_score)
    denominator = jnp.sum(exponent, axis=-1, keepdims=True) + jnp.exp(sink_column - peak_score)
    probability = (exponent / denominator).astype(jnp.bfloat16)
    mixed_rows = jnp.einsum(
        "nhqk,nkd->nqhd", probability, value_band, preferred_element_type=jnp.float32
    )
    return mixed_rows.reshape(row_count, head_count * HEAD).astype(jnp.bfloat16)


def shards_routed(
    mixer_input,
    mixer_gain,
    w_query,
    w_key,
    w_value,
    query_gain,
    key_gain,
    sink_logit,
    w_output,
    expert_input,
    expert_gain,
    route_ids,
    route_weight,
    expert_gate,
    expert_up,
    expert_down,
    shared_gate,
    shared_up,
    shared_down,
):
    tp_count = lax.axis_size("tp")
    ep_count = lax.axis_size("ep")
    rows_local = mixer_input.shape[0]
    heads_local = w_query.shape[1] // HEAD
    kv_index = lax.axis_index("tp") // (tp_count // KV_HEADS)
    key_cols = lax.dynamic_slice_in_dim(w_key, kv_index * HEAD, HEAD, 1)
    value_cols = lax.dynamic_slice_in_dim(w_value, kv_index * HEAD, HEAD, 1)
    portion_float = lax.all_gather(mixer_input, "tp", axis=1, tiled=True).astype(jnp.float32)
    scaled = (portion_float * mixer_gain).astype(jnp.bfloat16)
    query_raw = jnp.dot(scaled, w_query, preferred_element_type=jnp.float32)
    key_raw = jnp.dot(scaled, key_cols, preferred_element_type=jnp.float32)
    value_raw = jnp.dot(scaled, value_cols, preferred_element_type=jnp.float32)
    squares = jnp.sum(portion_float * portion_float, axis=1)
    inv_rms = lax.rsqrt(squares / D + EPSILON)[:, None]
    queries = head_norm(query_raw.reshape(rows_local, heads_local, HEAD), query_gain).astype(
        jnp.bfloat16
    )
    keys_own = head_norm(key_raw, key_gain).astype(jnp.bfloat16)
    values_own = (value_raw * inv_rms).astype(jnp.bfloat16)
    keys_prev, values_prev = from_behind(
        (keys_own[rows_local - WINDOW :], values_own[rows_local - WINDOW :]), "ep", 1
    )
    first_row = lax.axis_index("ep") * rows_local
    attended = band_attend(
        queries, keys_own, values_own, keys_prev, values_prev, sink_logit, first_row
    )
    head_partial = jnp.dot(attended, w_output, preferred_element_type=jnp.float32)
    mixer_output = lax.psum_scatter(
        head_partial.astype(jnp.bfloat16), "tp", scatter_dimension=1, tiled=True
    )
    tokens_local = expert_input.shape[0]
    expert_float = expert_input.astype(jnp.float32)
    normed = (
        expert_float
        * lax.rsqrt(jnp.mean(expert_float * expert_float, axis=-1, keepdims=True) + EPSILON)
        * expert_gain
    ).astype(jnp.bfloat16)
    capacity = 2 * tokens_local * TOPK // ep_count
    flat_ids = route_ids.reshape(-1)
    onehot = (flat_ids[:, None] == jnp.arange(ep_count, dtype=jnp.int32)[None, :]).astype(jnp.int32)
    earlier = jnp.cumsum(onehot, axis=0) - onehot
    slot_index = jnp.sum(earlier * onehot, axis=-1)
    slot_column = flat_ids * capacity + slot_index
    token_ids = jnp.arange(tokens_local * TOPK, dtype=jnp.int32) // TOPK
    slot_table = (
        jnp.full((ep_count * capacity,), tokens_local, jnp.int32).at[slot_column].set(token_ids)
    )
    col_width = expert_down.shape[2]
    arrived_rows = ep_count * capacity
    own_columns = lax.dynamic_slice_in_dim(normed, lax.axis_index("tp") * col_width, col_width, 1)
    padded = jnp.concatenate([own_columns, jnp.zeros((1, col_width), jnp.bfloat16)], axis=0)
    outgoing = padded[slot_table].reshape(ep_count, capacity, col_width)
    arrived = lax.all_to_all(outgoing, "ep", split_axis=0, concat_axis=0, tiled=True).reshape(
        arrived_rows, col_width
    )
    portion = lax.all_gather(arrived, "tp", axis=1, tiled=True)
    gate_part = expert_gate[0]
    up_part = expert_up[0]
    gate_pre = jnp.dot(portion, gate_part, preferred_element_type=jnp.float32)
    up_pre = jnp.dot(portion, up_part, preferred_element_type=jnp.float32)
    routed_hidden = (jax.nn.silu(gate_pre) * up_pre).astype(jnp.bfloat16)
    shared_hidden = (
        jax.nn.silu(jnp.dot(normed, shared_gate, preferred_element_type=jnp.float32))
        * jnp.dot(normed, shared_up, preferred_element_type=jnp.float32)
    ).astype(jnp.bfloat16)
    routed_part = expert_down[0]
    routed_sum = jnp.dot(
        lax.all_gather(routed_hidden, "tp", axis=1, tiled=True),
        routed_part,
        preferred_element_type=jnp.float32,
    )
    shared_sum = jnp.dot(
        lax.all_gather(shared_hidden, "tp", axis=1, tiled=True),
        shared_down,
        preferred_element_type=jnp.float32,
    )
    expert_rows = routed_sum.astype(jnp.bfloat16).reshape(ep_count, capacity, col_width)
    returned = lax.all_to_all(expert_rows, "ep", split_axis=0, concat_axis=0, tiled=True).reshape(
        arrived_rows, col_width
    )
    picked = returned[slot_column].reshape(tokens_local, TOPK, col_width).astype(jnp.float32)
    expert_output = (shared_sum + jnp.sum(picked * route_weight[:, :, None], axis=1)).astype(
        jnp.bfloat16
    )
    return (mixer_output, expert_output)


CHUNKS = 2
VMEM_LIMIT = 62 * 1024 * 1024
PARTS_BACK = 4
COLUMNS_X = 2


def place_of(slot, ring):
    half = ring // 2
    return 0 if slot == 0 else 2 * slot - 1 if slot <= half else 2 * (ring - slot)


def ring_position(index, ring):
    row, side = index // COLUMNS_X, index % COLUMNS_X
    return row + side * (ring - 1 - 2 * row)


def ring_index(position, ring):
    side = position // (ring // COLUMNS_X)
    return 2 * position + side * (2 * ring - 1 - 4 * position)


def remote(source, target, send, receive, device):
    return pltpu.make_async_remote_copy(
        src_ref=source,
        dst_ref=target,
        send_sem=send,
        recv_sem=receive,
        device_id=device,
        device_id_type=pl.DeviceIdType.MESH,
    )


def limit(direction, chunk, ring):
    return ring // 2 if direction == chunk else ring // 2 - 1


def slot_at(direction, distance, ring):
    return distance if direction == 0 else ring - distance


def layer_kernel(
    ring,
    rows_hbm,
    gain_hbm,
    ids_hbm,
    weight_hbm,
    mixer_hbm,
    mixer_gain_hbm,
    query_gain_hbm,
    key_gain_hbm,
    sink_hbm,
    gate_hbm,
    up_hbm,
    shared_gate_hbm,
    shared_up_hbm,
    query_hbm,
    key_hbm,
    value_hbm,
    w_out_hbm,
    down_hbm,
    shared_down_hbm,
    mixer_result,
    expert_result,
    rows_v,
    gain_v,
    ids_v,
    weight_v,
    mixer_gain_v,
    query_gain_v,
    key_gain_v,
    sink_v,
    mixer_all,
    hidden_all,
    shared_all,
    att_all,
    dense_all,
    tok,
    gate_v,
    up_v,
    shared_gate_v,
    shared_up_v,
    qkv_v,
    down_v,
    shared_down_v,
    out_cols,
    out_stage,
    scaled_v,
    heads_v,
    band_v,
    bias_v,
    ready,
    going,
    coming,
    load_sem,
    tok_send,
    ring_recv,
    sib_recv,
    mix_send,
    mix_recv,
    hid_send,
    hid_recv,
    sh_send,
    sh_recv,
    att_send,
    att_recv,
    dense_send,
    dense_recv,
    halo_send,
    halo_recv,
    wcol_send,
    wcol_recv,
    wring_send,
    wring_recv,
    back_send,
    back_recv,
):
    scope = jax.named_scope
    f32, bf16 = jnp.float32, jnp.bfloat16
    index, part = lax.axis_index("ep"), lax.axis_index("tp")
    far, core = part // 2, part % 2
    position = ring_position(index, ring)
    peer_index = [ring_index((position + k) % ring, ring) for k in range(ring)]
    peers = [(peer_index[k], part) for k in range(1, ring)]
    ahead, behind = peers[0], peers[-1]
    sib_part = 2 * far + 1 - core
    across_part = 2 * (1 - far) + core
    corner_part = 2 * (1 - far) + 1 - core
    sibling, across = (index, sib_part), (index, across_part)
    block, width = rows_v.shape
    half_width = width // 2
    piece = block // CHUNKS
    steps = ring // 2
    parts, rows_local, mixer_cols = mixer_all.shape
    pieces = rows_local // WINDOW
    out_width = down_v.shape[1]
    inner = hidden_all.shape[2]
    shared_width = shared_all.shape[2]
    head_rows = out_cols.shape[1]
    share_rows = head_rows // ring
    share_piece = share_rows // CHUNKS

    barrier = pltpu.get_barrier_semaphore()
    for device in peers + [sibling, across]:
        pl.semaphore_signal(barrier, inc=1, device_id=device, device_id_type=pl.DeviceIdType.MESH)


    def start(copy):
        copy.start()

    loads = {}

    def load(name, source, target):
        loads[name] = pltpu.make_async_copy(source, target, load_sem.at[len(loads)])
        loads[name].start()

    def load_qkv(source, first):
        target = qkv_v.at[:, pl.ds(first, source.shape[1])]
        pltpu.make_async_copy(source, target, load_sem.at[len(loads)]).start()

    own_cols = pl.ds(pl.multiple_of(part * out_width, out_width), out_width)
    load("rows", rows_hbm, rows_v)
    load("gain", gain_hbm, gain_v)
    load("mixer", mixer_hbm, mixer_all.at[part])
    load("shared_gate", shared_gate_hbm, shared_gate_v)
    load("shared_up", shared_up_hbm, shared_up_v)
    load("gate", gate_hbm, gate_v)
    load("up", up_hbm, up_v)
    load("ids", ids_hbm, ids_v)
    load("weight", weight_hbm, weight_v)
    load("mixer_gain", mixer_gain_hbm, mixer_gain_v)
    load("query_gain", query_gain_hbm, query_gain_v)
    load("key_gain", key_gain_hbm, key_gain_v)
    load("sink", sink_hbm, sink_v)
    query_cols, key_cols = query_hbm.shape[1], key_hbm.shape[1]
    load_qkv(query_hbm, 0)
    load_qkv(key_hbm, query_cols)
    load_qkv(value_hbm, query_cols + key_cols)
    loads["qkv"] = pltpu.make_async_copy(qkv_v, qkv_v, load_sem.at[len(loads)])
    load("out_own", w_out_hbm.at[:, own_cols], out_cols.at[part])
    load("down", down_hbm, down_v)
    load("shared_down", shared_down_hbm, shared_down_v)

    band_shape = (2 * WINDOW, WINDOW)
    relative = (
        lax.broadcasted_iota(jnp.int32, band_shape, 1)
        + WINDOW
        - lax.broadcasted_iota(jnp.int32, band_shape, 0)
    )
    bias_v[...] = jnp.where((relative >= 0) & (relative < WINDOW), 0.0, -jnp.inf)
    low = lax.broadcasted_iota(jnp.int32, (WINDOW, 2 * HEAD), 1) < HEAD

    with scope("norm"):
        loads["rows"].wait()
        loads["gain"].wait()
        value = rows_v[...].astype(f32)
        normed = (
            value
            * lax.rsqrt(jnp.mean(value * value, axis=-1, keepdims=True) + EPSILON)
            * gain_v[...]
        ).astype(bf16)
        tok[0, pl.ds(0, block), :] = normed[:, :half_width]
        tok[1, pl.ds(0, block), :] = normed[:, half_width:]
        loads["mixer"].wait()

    with scope("greet"):
        pl.semaphore_wait(barrier, ring + 1)

    def chunk_ref(half, slot, chunk):
        return tok.at[half, pl.ds(place_of(slot, ring) * block + chunk * piece, piece), :]

    def hop(direction, distance, chunk):
        start(
            remote(
                chunk_ref(core, slot_at(direction, distance - 1, ring) % ring, chunk),
                chunk_ref(core, slot_at(direction, distance, ring), chunk),
                tok_send.at[0],
                ring_recv.at[direction, distance - 1, chunk],
                ahead if direction == 0 else behind,
            )
        )

    def arrive(distance, k):
        for direction in range(2):
            chunk = k if direction == 0 else CHUNKS - 1 - k
            if distance > limit(direction, chunk, ring):
                continue
            here = chunk_ref(core, slot_at(direction, distance, ring), chunk)
            got = ring_recv.at[direction, distance - 1, chunk]
            remote(here, here, tok_send.at[0], got, sibling).wait_recv()
            if distance < limit(direction, chunk, ring):
                hop(direction, distance + 1, chunk)
            start(remote(here, here, tok_send.at[0], sib_recv.at[distance - 1], sibling))

    def swapped(distance):
        count = 2 if distance < steps else 1
        there = tok.at[1 - core, pl.ds((2 * distance - 1) * block, count * block), :]
        remote(there, there, tok_send.at[0], sib_recv.at[distance - 1], sibling).wait_recv()

    class Share:
        def __init__(self, view, send, receive):
            self.view, self.send, self.receive = view, send, receive

        def copy(self, owner, i, path, device):
            here = self.view(owner, i)
            return remote(here, here, self.send.at[0], self.receive.at[path, i], device)

        def to_across(self, i):
            start(self.copy(part, i, 0, across))

        def to_sibling(self, i):
            start(self.copy(part, i, 1, sibling))

        def both(self, i):
            self.to_across(i)
            self.to_sibling(i)

        def forward(self, i):
            self.copy(across_part, i, 0, sibling).wait_recv()
            start(self.copy(across_part, i, 1, sibling))

        def rest(self, i):
            self.copy(pl.ds(0, 2), i, 1, sibling).wait_recv()

    mixer = Share(
        lambda owner, i: mixer_all.at[owner, pl.ds(i * WINDOW, WINDOW), :], mix_send, mix_recv
    )
    shared = Share(lambda owner, i: shared_all.at[owner], sh_send, sh_recv)
    hidden = Share(
        lambda owner, i: hidden_all.at[owner, pl.ds(place_of(i, ring) * block, block), :],
        hid_send,
        hid_recv,
    )
    att = Share(
        lambda owner, i: att_all.at[owner, pl.ds(i * WINDOW, WINDOW), :], att_send, att_recv
    )

    for k in range(CHUNKS):
        for direction in range(2):
            hop(direction, 1, k if direction == 0 else CHUNKS - 1 - k)
    mixer.both(3)
    mixer.both(2)
    mixer.to_sibling(1)
    mixer.to_sibling(0)

    loads["ids"].wait()
    loads["weight"].wait()
    experts = lax.broadcasted_iota(jnp.int32, (ring, block), 0)
    dense = jnp.zeros((ring, block), f32)
    for k in range(TOPK):
        dense = dense + jnp.where(ids_v[k : k + 1, :] == experts, weight_v[k : k + 1, :], 0.0)
    dense_all[0] = dense
    for k in range(1, ring):
        start(
            remote(
                dense_all.at[0], dense_all.at[k], dense_send.at[0], dense_recv.at[0], peers[k - 1]
            )
        )

    def product(first, count, weights, columns):
        lower = tok[0, pl.ds(first, count), :]
        upper = tok[1, pl.ds(first, count), :]
        return jnp.dot(
            lower, weights[pl.ds(0, half_width), columns], preferred_element_type=f32
        ) + jnp.dot(
            upper, weights[pl.ds(half_width, half_width), columns], preferred_element_type=f32
        )

    with scope("c_shared"):
        loads["shared_gate"].wait()
        loads["shared_up"].wait()
        everything = pl.ds(0, shared_width)
        shared_all[part] = (
            jax.nn.silu(product(0, block, shared_gate_v, everything))
            * product(0, block, shared_up_v, everything)
        ).astype(bf16)
        shared.both(0)

    tile = 256

    def compute(slots, now):
        first = min(place_of(slot, ring) for slot in slots) * block
        count = len(slots) * block

        def one(j, carry):
            columns = pl.ds(pl.multiple_of(j * tile, tile), tile)
            hidden_all[part, pl.ds(first, count), columns] = (
                jax.nn.silu(product(first, count, gate_v, columns))
                * product(first, count, up_v, columns)
            ).astype(bf16)
            return carry

        lax.fori_loop(0, inner // tile, one, 0)
        for slot in slots:
            hidden.to_sibling(slot)
            if slot in now:
                hidden.to_across(slot)

    def project(i):
        rows = pl.ds(i * WINDOW, WINDOW)
        mixer.rest(i)
        squares = jnp.zeros((WINDOW, 1), f32)
        for owner in range(parts):
            columns = pl.ds(owner * mixer_cols, mixer_cols)
            value = mixer_all[owner, rows, :].astype(f32)
            squares = squares + jnp.sum(value * value, axis=1, keepdims=True)
            scaled_v[:, columns] = (value * mixer_gain_v[:, columns]).astype(bf16)
        raw = jnp.dot(scaled_v[...], qkv_v[...], preferred_element_type=f32)
        lanes = 2 * HEAD
        heads = heads_v.shape[0]
        gain = query_gain_v[...] * HEAD ** (-0.5)
        gain = jnp.concatenate([gain, gain], axis=1)
        for pair in range(heads // 2):
            two = raw[:, pair * lanes : (pair + 1) * lanes]
            square = two * two
            first_sum = jnp.sum(jnp.where(low, square, 0.0), axis=1, keepdims=True)
            second_sum = jnp.sum(jnp.where(low, 0.0, square), axis=1, keepdims=True)
            inverse = lax.rsqrt(jnp.where(low, first_sum, second_sum) / HEAD + EPSILON)
            two = two * inverse * gain
            heads_v[2 * pair, rows, :] = jnp.where(low, two, 0.0).astype(bf16)
            heads_v[2 * pair + 1, rows, :] = jnp.where(low, 0.0, two).astype(bf16)
        queries_end = heads * HEAD
        second = part // (parts // KV_HEADS)
        mine = low == (second == 0)

        def twice(columns):
            return jnp.where(mine, columns, pltpu.roll(columns, HEAD, 1))

        key = twice(raw[:, queries_end : queries_end + lanes])
        gain = jnp.concatenate([key_gain_v[...], key_gain_v[...]], axis=1)
        key = key * lax.rsqrt(jnp.mean(key * key, axis=1, keepdims=True) + EPSILON) * gain
        val = twice(raw[:, queries_end + lanes : queries_end + 2 * lanes])
        val = val * lax.rsqrt(squares / D + EPSILON)
        band_v[pl.ds(WINDOW + i * WINDOW, WINDOW), :] = jnp.concatenate(
            [key, val], axis=1
        ).astype(bf16)

    halo = band_v.at[pl.ds(0, WINDOW), :]

    def send_halo():
        start(
            remote(
                band_v.at[pl.ds(rows_local, WINDOW), :],
                halo,
                halo_send.at[0],
                halo_recv.at[0],
                ((index + 1) % ring, part),
            )
        )

    def wait_halo():
        remote(halo, halo, halo_send.at[0], halo_recv.at[0], sibling).wait_recv()

    def attend(i):
        rows = pl.ds(i * WINDOW, WINDOW)
        heads = heads_v.shape[0]
        keys = band_v[pl.ds(i * WINDOW, 2 * WINDOW), pl.ds(0, 2 * HEAD)]
        values = band_v[pl.ds(i * WINDOW, 2 * WINDOW), pl.ds(2 * HEAD, 2 * HEAD)]
        bias = bias_v[...]
        if i == 0:
            before = lax.broadcasted_iota(jnp.int32, band_shape, 0) < WINDOW
            bias = jnp.where(before & (index == 0), -jnp.inf, bias)
        scores = lax.dot_general(
            keys,
            heads_v[:, rows, :].reshape(heads * WINDOW, 2 * HEAD),
            (((1,), (1,)), ((), ())),
            preferred_element_type=f32,
        )
        columns = []
        for head in range(heads):
            masked = scores[:, head * WINDOW : (head + 1) * WINDOW] + bias
            sink = sink_v[:, head : head + 1]
            peak = jnp.maximum(jnp.max(masked, axis=0, keepdims=True), sink)
            exponent = jnp.exp(masked - peak)
            denominator = jnp.sum(exponent, axis=0, keepdims=True) + jnp.exp(sink - peak)
            columns.append((exponent * (1.0 / denominator)).astype(bf16))
        mixed = lax.dot_general(
            values[:, :HEAD],
            jnp.concatenate(columns, axis=1),
            (((0,), (0,)), ((), ())),
            preferred_element_type=f32,
        )
        for pair in range(heads // 2):
            first = 2 * pair * WINDOW
            two = jnp.concatenate(
                [mixed[:, first : first + WINDOW], mixed[:, first + WINDOW : first + 2 * WINDOW]],
                axis=0,
            )
            att_all[part, rows, pl.ds(pair * 2 * HEAD, 2 * HEAD)] = two.T.astype(bf16)

    chip_cols = 2 * out_width

    def spread_columns():
        start(
            remote(
                w_out_hbm.at[:, pl.ds(pl.multiple_of(sib_part * out_width, out_width), out_width)],
                out_cols.at[part],
                wcol_send.at[0],
                wcol_recv.at[0],
                sibling,
            )
        )
        mine = pl.ds(pl.multiple_of(index * share_rows, share_rows), share_rows)
        start(
            remote(
                w_out_hbm.at[
                    mine, pl.ds(pl.multiple_of((1 - far) * chip_cols, chip_cols), chip_cols)
                ],
                out_stage.at[mine, :],
                wcol_send.at[1],
                wcol_recv.at[1],
                across,
            )
        )

    def stage_ref(slot, chunk):
        owner = peer_index[(ring - slot) % ring]
        first = owner * share_rows + chunk * share_piece
        return out_stage.at[pl.ds(pl.multiple_of(first, share_piece), share_piece), :]

    def column_hop(direction, distance, chunk):
        here = stage_ref(slot_at(direction, distance - 1, ring) % ring, chunk)
        to = ahead if direction == 0 else behind
        start(remote(here, here, wring_send.at[0], wring_recv.at[distance - 1], to))

    def column_start():
        mine = out_stage.at[pl.ds(pl.multiple_of(index * share_rows, share_rows), share_rows), :]
        remote(mine, mine, wcol_send.at[1], wcol_recv.at[1], across).wait_recv()
        for chunk in range(CHUNKS):
            for direction in range(2):
                column_hop(direction, 1, chunk)

    def column_arrive(distance):
        count = 2 if distance < steps else 1
        here = out_stage.at[pl.ds(0, count * share_rows), :]
        remote(here, here, wring_send.at[0], wring_recv.at[distance - 1], sibling).wait_recv()
        for chunk in range(CHUNKS):
            for direction in range(2):
                if distance < limit(direction, chunk, ring):
                    column_hop(direction, distance + 1, chunk)

    def column_swap():
        start(
            remote(
                out_stage.at[
                    :, pl.ds(pl.multiple_of((1 - core) * out_width, out_width), out_width)
                ],
                out_cols.at[across_part],
                wcol_send.at[2],
                wcol_recv.at[2],
                sibling,
            )
        )

    def column_wait():
        loads["out_own"].wait()
        for i, owner in ((0, sib_part), (2, corner_part)):
            here = out_cols.at[owner]
            remote(here, here, wcol_send.at[i], wcol_recv.at[i], sibling).wait_recv()

    def finish_mixer(i):
        rows = pl.ds(i * WINDOW, WINDOW)
        att.rest(i)
        total = jnp.dot(
            att_all[across_part, rows, :],
            out_stage[:, pl.ds(pl.multiple_of(core * out_width, out_width), out_width)],
            preferred_element_type=f32,
        )
        for owner in (part, sib_part, corner_part):
            total = total + jnp.dot(
                att_all[owner, rows, :], out_cols[owner], preferred_element_type=f32
            )
        mixer_result[rows, :] = total.astype(bf16)

    diagonal = lax.broadcasted_iota(jnp.int32, (block, block), 0) == lax.broadcasted_iota(
        jnp.int32, (block, block), 1
    )

    def weight_column(slot):
        row = dense_all[slot, pl.ds(index, 1), :]
        return jnp.sum(jnp.where(diagonal, row, 0.0), axis=1, keepdims=True)

    def weighted(slots):
        for slot in slots:
            hidden.rest(slot)
        first = min(place_of(slot, ring) for slot in slots) * block
        count = len(slots) * block
        total = jnp.dot(
            hidden_all[0, pl.ds(first, count), :],
            down_v[pl.ds(0, inner), :],
            preferred_element_type=f32,
        )
        for owner in range(1, parts):
            total = total + jnp.dot(
                hidden_all[owner, pl.ds(first, count), :],
                down_v[pl.ds(owner * inner, inner), :],
                preferred_element_type=f32,
            )
        rounded = total.astype(bf16).astype(f32)
        ordered = sorted(slots, key=lambda slot: place_of(slot, ring))
        ready[pl.ds(first, count), :] = rounded * jnp.concatenate(
            [weight_column(slot) for slot in ordered], axis=0
        )

    def own_rows():
        weighted([0])
        shared.rest(0)
        own = ready[pl.ds(0, block), :]
        for owner in range(parts):
            own = own + jnp.dot(
                shared_all[owner],
                shared_down_v[pl.ds(owner * shared_width, shared_width), :],
                preferred_element_type=f32,
            )
        ready[pl.ds(0, block), :] = own

    back_rows = block // PARTS_BACK

    def longest(direction, part_back):
        return limit(direction, part_back * CHUNKS // PARTS_BACK, ring)

    def back_wait(direction, distance, b):
        here = coming.at[direction, distance, pl.ds(b * back_rows, back_rows), :]
        got = back_recv.at[direction, distance - 1, b]
        remote(here, here, back_send.at[0], got, ahead).wait_recv()
        return here[...].astype(f32)

    def push(distance, long, directions=(0, 1)):
        for b in range(PARTS_BACK):
            for direction in directions:
                if (longest(direction, b) == steps) != long:
                    continue
                slot = slot_at(1 - direction, distance, ring)
                first = place_of(slot, ring) * block + b * back_rows
                value = ready[pl.ds(first, back_rows), :]
                hops = 1
                if long and distance == steps:
                    hops = 2
                elif long and distance == steps - 2:
                    hops = 2
                    value = value + back_wait(direction, distance + 1, b)
                    value = value + back_wait(direction, distance + 2, b)
                elif not long and distance < steps - 1:
                    value = value + back_wait(direction, distance + 1, b)
                rows = pl.ds(b * back_rows, back_rows)
                at = direction * steps + distance - 1
                going[at, rows, :] = value.astype(bf16)
                start(
                    remote(
                        going.at[at, rows, :],
                        coming.at[direction, distance, rows, :],
                        back_send.at[0],
                        back_recv.at[direction, distance - 1, b],
                        peers[hops - 1 if direction == 0 else -hops],
                    )
                )

    def finish_expert(b):
        rows = pl.ds(b * back_rows, back_rows)
        total = ready[rows, :]
        for direction in range(2):
            total = total + back_wait(direction, 1, b)
            if longest(direction, b) == steps:
                total = total + back_wait(direction, 2, b)
        expert_result[rows, :] = total.astype(bf16)

    with scope("c_h0"):
        loads["gate"].wait()
        loads["up"].wait()
        compute([0], [])
    spread_columns()
    mixer.to_across(1)
    mixer.to_across(0)
    with scope("A1c0"):
        arrive(1, 0)
    with scope("fwd_m3"):
        mixer.forward(3)
    with scope("A1c1"):
        arrive(1, 1)
    with scope("fwd_m2"):
        mixer.forward(2)
    with scope("w_qkv"):
        for name in ("mixer_gain", "query_gain", "key_gain", "sink", "qkv"):
            loads[name].wait()
    with scope("qkv3"):
        project(3)
        send_halo()
    with scope("S1"):
        swapped(1)
    with scope("c_h1"):
        compute([1, ring - 1], [1, ring - 1])
    with scope("A2c0"):
        arrive(2, 0)
    with scope("qkv2"):
        project(2)
    with scope("att3"):
        attend(3)
        att.to_sibling(3)
    with scope("fwd_sh_m1"):
        shared.forward(0)
        mixer.forward(1)
    with scope("A2c1"):
        arrive(2, 1)
    with scope("S2"):
        swapped(2)
    with scope("c_h2"):
        compute([2, ring - 2], [2])
    with scope("A3c0"):
        arrive(3, 0)
    with scope("fwd_m0"):
        mixer.forward(0)
    with scope("qkv1"):
        project(1)
    with scope("att2"):
        attend(2)
        att.to_sibling(2)
    with scope("A3c1"):
        arrive(3, 1)
    with scope("w0"):
        column_start()
    with scope("fwd_h1"):
        hidden.forward(1)
    with scope("qkv0"):
        project(0)
    with scope("S3"):
        swapped(3)
    with scope("c_h3"):
        compute([3], [3])
        compute([ring - 3], [ring - 3])
    with scope("A4"):
        arrive(4, 0)
    with scope("w1"):
        column_arrive(1)
    with scope("fwd_h7"):
        hidden.forward(ring - 1)
    with scope("att1"):
        attend(1)
        att.to_sibling(1)
    with scope("halo"):
        wait_halo()
    with scope("att0"):
        attend(0)
        att.to_sibling(0)
    with scope("S4"):
        swapped(4)
    with scope("c_h4"):
        compute([4], [4])
    hidden.to_across(ring - 2)
    hidden.to_across(0)
    for i in (3, 2, 1, 0):
        att.to_across(i)
    with scope("fwd_h2"):
        hidden.forward(2)
    with scope("w_dense"):
        loads["down"].wait()
        loads["shared_down"].wait()
        here = dense_all.at[pl.ds(1, ring - 1)]
        remote(here, here, dense_send.at[0], dense_recv.at[0], sibling).wait_recv()
    with scope("down1"):
        weighted([1, ring - 1])
        push(1, True)
    with scope("w2"):
        column_arrive(2)
    with scope("down2"):
        weighted([2])
    with scope("fwd_h3"):
        hidden.forward(3)
    with scope("down3"):
        weighted([3])
        push(3, False, (1,))
        push(3, True, (1,))
    with scope("fwd_h5"):
        hidden.forward(ring - 3)
    with scope("w3"):
        column_arrive(3)
    with scope("down5"):
        weighted([ring - 3])
        push(3, False, (0,))
        push(3, True, (0,))
    with scope("fwd_h4"):
        hidden.forward(4)
    with scope("push2s1"):
        push(2, False, (1,))
    with scope("down4"):
        weighted([4])
        push(4, True)
    with scope("fwd_h6"):
        hidden.forward(ring - 2)
    with scope("w4"):
        column_arrive(4)
        column_swap()
    with scope("down6"):
        weighted([ring - 2])
    with scope("push1s1"):
        push(1, False, (1,))
    with scope("push2s0"):
        push(2, False, (0,))
    with scope("fwd_h0"):
        hidden.forward(0)
    with scope("push2l1"):
        push(2, True, (1,))
    with scope("push2l0"):
        push(2, True, (0,))
    with scope("push1s0"):
        push(1, False, (0,))
    with scope("fwd_a2"):
        att.forward(3)
        att.forward(2)
    with scope("own"):
        own_rows()
    with scope("fwd_a1"):
        att.forward(1)
    with scope("out3"):
        column_wait()
        finish_mixer(3)
    with scope("out2"):
        finish_mixer(2)
    with scope("fwd_a0"):
        att.forward(0)
    with scope("out1"):
        finish_mixer(1)
    with scope("out0"):
        finish_mixer(0)
    with scope("fin_exp"):
        for b in range(PARTS_BACK):
            finish_expert(b)
    with scope("w_end"):
        for ref, send in (
            (tok.at[:, pl.ds(0, (ring - 1) * block), :], tok_send.at[0]),
            (mixer_all.at[pl.ds(0, parts - 1)], mix_send.at[0]),
            (hidden_all.at[pl.ds(0, parts - 1)], hid_send.at[0]),
            (shared_all.at[pl.ds(0, parts - 1)], sh_send.at[0]),
            (att_all.at[pl.ds(0, parts - 1)], att_send.at[0]),
            (dense_all.at[pl.ds(0, ring - 1)], dense_send.at[0]),
            (halo, halo_send.at[0]),
            (out_cols.at[part], wcol_send.at[0]),
            (out_stage.at[pl.ds(0, share_rows), :], wcol_send.at[1]),
            (out_cols.at[part], wcol_send.at[2]),
            (out_stage.at[pl.ds(0, (ring - 1) * share_rows), :], wring_send.at[0]),
            (going.at[pl.ds(0, ring - 1)], back_send.at[0]),
        ):
            remote(ref, ref, send, halo_recv.at[0], sibling).wait_send()


def settle_kernel(mixer_in, expert_in, mixer_out, expert_out, sem):
    copies = [
        pltpu.make_async_copy(mixer_in, mixer_out, sem.at[0]),
        pltpu.make_async_copy(expert_in, expert_out, sem.at[1]),
    ]
    for copy in copies:
        copy.start()
    for copy in copies:
        copy.wait()


def shards(
    mixer_input,
    mixer_gain,
    w_query,
    w_key,
    w_value,
    query_gain,
    key_gain,
    sink_logit,
    w_output,
    expert_input,
    expert_gain,
    route_ids,
    route_weight,
    expert_gate,
    expert_up,
    expert_down,
    shared_gate,
    shared_up,
    shared_down,
):
    ring = lax.axis_size("ep")
    parts = lax.axis_size("tp")
    rows_local, mixer_cols = mixer_input.shape
    tokens_local, width = expert_input.shape
    hidden_width = expert_gate.shape[2]
    shared_width = shared_gate.shape[1]
    out_width = expert_down.shape[2]
    head_width = w_query.shape[1]
    pieces = rows_local // WINDOW
    half = ring // 2
    hbm = pl.BlockSpec(memory_space=pl.ANY)
    bf16, f32 = jnp.bfloat16, jnp.float32
    vm = pltpu.VMEM

    dma = pltpu.SemaphoreType.DMA
    outputs = pl.pallas_call(
        functools.partial(layer_kernel, ring),
        out_shape=(vm((rows_local, out_width), bf16), vm((tokens_local, out_width), bf16)),
        in_specs=[hbm] * 19,
        out_specs=(pl.BlockSpec(memory_space=vm),) * 2,
        scratch_shapes=[
            vm((tokens_local, width), bf16),
            vm((1, width), f32),
            vm((TOPK, tokens_local), jnp.int32),
            vm((TOPK, tokens_local), f32),
            vm((1, parts * mixer_cols), f32),
            vm((1, HEAD), f32),
            vm((1, HEAD), f32),
            vm((1, sink_logit.shape[0]), f32),
            vm((parts, rows_local, mixer_cols), bf16),
            vm((parts, ring * tokens_local, hidden_width), bf16),
            vm((parts, tokens_local, shared_width), bf16),
            vm((parts, rows_local, head_width), bf16),
            vm((ring, ring, tokens_local), f32),
            vm((2, ring * tokens_local, width // 2), bf16),
            vm((width, hidden_width), bf16),
            vm((width, hidden_width), bf16),
            vm((width, shared_width), bf16),
            vm((width, shared_width), bf16),
            vm((width, head_width + w_key.shape[1] + w_value.shape[1]), bf16),
            vm(expert_down.shape[1:], bf16),
            vm(shared_down.shape, bf16),
            vm((parts, head_width, out_width), bf16),
            vm((head_width, 2 * out_width), bf16),
            vm((WINDOW, parts * mixer_cols), bf16),
            vm((head_width // HEAD, rows_local, 2 * HEAD), bf16),
            vm((WINDOW + rows_local, 4 * HEAD), bf16),
            vm((2 * WINDOW, WINDOW), f32),
            vm((ring * tokens_local, out_width), f32),
            vm((2 * half, tokens_local, out_width), bf16),
            vm((2, half + 1, tokens_local, out_width), bf16),
            dma((17,)),
            dma((1,)),
            dma((2, half, CHUNKS)),
            dma((half,)),
            dma((1,)),
            dma((2, pieces)),
            dma((1,)),
            dma((2, ring)),
            dma((1,)),
            dma((2, 1)),
            dma((1,)),
            dma((2, pieces)),
            dma((1,)),
            dma((1,)),
            dma((1,)),
            dma((1,)),
            dma((3,)),
            dma((3,)),
            dma((1,)),
            dma((half,)),
            dma((1,)),
            dma((2, half, PARTS_BACK)),
        ],
        compiler_params=pltpu.CompilerParams(
            collective_id=0, has_side_effects=True, vmem_limit_bytes=VMEM_LIMIT
        ),
        name="layer",
    )(
        expert_input,
        expert_gain[None, :],
        route_ids.T,
        route_weight.T,
        mixer_input,
        mixer_gain[None, :],
        query_gain[None, :],
        key_gain[None, :],
        sink_logit[None, :],
        expert_gate[0],
        expert_up[0],
        shared_gate,
        shared_up,
        w_query,
        w_key,
        w_value,
        w_output,
        expert_down[0],
        shared_down,
    )
    return pl.pallas_call(
        settle_kernel,
        out_shape=tuple(jax.ShapeDtypeStruct(o.shape, o.dtype) for o in outputs),
        in_specs=[pl.BlockSpec(memory_space=vm)] * 2,
        out_specs=(hbm,) * 2,
        scratch_shapes=[dma((2,))],
        compiler_params=pltpu.CompilerParams(vmem_limit_bytes=1024 * 1024),
        name="settle",
    )(*outputs)


def plan(*arrays):
    route_ids = arrays[11]
    capacity = 2 * route_ids.size // lax.axis_size("ep")
    whole_blocks = capacity >= route_ids.shape[0]
    fits = lax.axis_size("ep") == 8 and lax.axis_size("tp") == 4
    if whole_blocks and fits and arrays[0].shape[0] == 4 * WINDOW:
        return shards(*arrays)
    return shards_routed(*arrays)


def solution(mesh):
    in_specs = (
        P("ep", "tp"),
        P(),
        P(None, "tp"),
        P(),
        P(),
        P(),
        P(),
        P("tp"),
        P("tp", None),
        P("ep", None),
        P(),
        P("ep", None),
        P("ep", None),
        P("ep", None, "tp"),
        P("ep", None, "tp"),
        P("ep", None, "tp"),
        P(None, "tp"),
        P(None, "tp"),
        P(None, "tp"),
    )
    out_specs = (P("ep", "tp"), P("ep", "tp"))
    return jax.shard_map(plan, mesh=mesh, in_specs=in_specs, out_specs=out_specs, check_vma=False)
```

```python
import functools

import jax
import jax.numpy as jnp
from jax import lax
from jax.experimental import pallas as pl
from jax.experimental.pallas import tpu as pltpu
from jax.sharding import PartitionSpec as P

D = 2048
HEAD = 64
KV_HEADS = 2
WINDOW = 128
TOPK = 4


EPSILON = 1e-06


def from_behind(value, axis, steps):
    count = lax.axis_size(axis)
    first, last = (max(0, -steps), min(count, count - steps))
    return lax.ppermute(value, axis, [(source, source + steps) for source in range(first, last)])


def head_norm(matrix, gain_vector):
    return (
        matrix
        * lax.rsqrt(jnp.mean(matrix * matrix, axis=-1, keepdims=True) + EPSILON)
        * gain_vector
    )


def band_attend(queries, keys_own, values_own, keys_prev, values_prev, sink_logit, first_row):
    row_count = queries.shape[0]
    head_count = queries.shape[1]
    blocks = row_count // WINDOW
    keys_all = jnp.concatenate([keys_prev, keys_own], axis=0)
    values_all = jnp.concatenate([values_prev, values_own], axis=0)
    key_band = jnp.concatenate(
        [
            keys_all[:row_count].reshape(blocks, WINDOW, HEAD),
            keys_own.reshape(blocks, WINDOW, HEAD),
        ],
        axis=1,
    )
    value_band = jnp.concatenate(
        [
            values_all[:row_count].reshape(blocks, WINDOW, HEAD),
            values_own.reshape(blocks, WINDOW, HEAD),
        ],
        axis=1,
    )
    query_blocks = queries.reshape(blocks, WINDOW, head_count, HEAD)
    scores = jnp.einsum(
        "nqhd,nkd->nhqk", query_blocks, key_band, preferred_element_type=jnp.float32
    ) * HEAD ** (-0.5)
    query_idx = jnp.arange(WINDOW, dtype=jnp.int32)[:, None]
    key_idx = jnp.arange(2 * WINDOW, dtype=jnp.int32)[None, :]
    relative = query_idx + WINDOW - key_idx
    block_idx = jnp.arange(blocks, dtype=jnp.int32)[:, None, None]
    key_pos = first_row + block_idx * WINDOW - WINDOW + key_idx[None]
    allowed = ((relative >= 0) & (relative < WINDOW))[None] & (key_pos >= 0)
    allowed = allowed[:, None]
    masked = jnp.where(allowed, scores, -jnp.inf)
    sink_column = sink_logit.reshape(1, head_count, 1, 1)
    peak_score = jnp.maximum(jnp.max(masked, axis=-1, keepdims=True), sink_column)
    exponent = jnp.exp(masked - peak_score)
    denominator = jnp.sum(exponent, axis=-1, keepdims=True) + jnp.exp(sink_column - peak_score)
    probability = (exponent / denominator).astype(jnp.bfloat16)
    mixed_rows = jnp.einsum(
        "nhqk,nkd->nqhd", probability, value_band, preferred_element_type=jnp.float32
    )
    return mixed_rows.reshape(row_count, head_count * HEAD).astype(jnp.bfloat16)


def shards_routed(
    mixer_input,
    mixer_gain,
    w_query,
    w_key,
    w_value,
    query_gain,
    key_gain,
    sink_logit,
    w_output,
    expert_input,
    expert_gain,
    route_ids,
    route_weight,
    expert_gate,
    expert_up,
    expert_down,
    shared_gate,
    shared_up,
    shared_down,
):
    tp_count = lax.axis_size("tp")
    ep_count = lax.axis_size("ep")
    rows_local = mixer_input.shape[0]
    heads_local = w_query.shape[1] // HEAD
    kv_index = lax.axis_index("tp") // (tp_count // KV_HEADS)
    key_cols = lax.dynamic_slice_in_dim(w_key, kv_index * HEAD, HEAD, 1)
    value_cols = lax.dynamic_slice_in_dim(w_value, kv_index * HEAD, HEAD, 1)
    portion_float = lax.all_gather(mixer_input, "tp", axis=1, tiled=True).astype(jnp.float32)
    scaled = (portion_float * mixer_gain).astype(jnp.bfloat16)
    query_raw = jnp.dot(scaled, w_query, preferred_element_type=jnp.float32)
    key_raw = jnp.dot(scaled, key_cols, preferred_element_type=jnp.float32)
    value_raw = jnp.dot(scaled, value_cols, preferred_element_type=jnp.float32)
    squares = jnp.sum(portion_float * portion_float, axis=1)
    inv_rms = lax.rsqrt(squares / D + EPSILON)[:, None]
    queries = head_norm(query_raw.reshape(rows_local, heads_local, HEAD), query_gain).astype(
        jnp.bfloat16
    )
    keys_own = head_norm(key_raw, key_gain).astype(jnp.bfloat16)
    values_own = (value_raw * inv_rms).astype(jnp.bfloat16)
    keys_prev, values_prev = from_behind(
        (keys_own[rows_local - WINDOW :], values_own[rows_local - WINDOW :]), "ep", 1
    )
    first_row = lax.axis_index("ep") * rows_local
    attended = band_attend(
        queries, keys_own, values_own, keys_prev, values_prev, sink_logit, first_row
    )
    head_partial = jnp.dot(attended, w_output, preferred_element_type=jnp.float32)
    mixer_output = lax.psum_scatter(
        head_partial.astype(jnp.bfloat16), "tp", scatter_dimension=1, tiled=True
    )
    tokens_local = expert_input.shape[0]
    expert_float = expert_input.astype(jnp.float32)
    normed = (
        expert_float
        * lax.rsqrt(jnp.mean(expert_float * expert_float, axis=-1, keepdims=True) + EPSILON)
        * expert_gain
    ).astype(jnp.bfloat16)
    capacity = 2 * tokens_local * TOPK // ep_count
    flat_ids = route_ids.reshape(-1)
    onehot = (flat_ids[:, None] == jnp.arange(ep_count, dtype=jnp.int32)[None, :]).astype(jnp.int32)
    earlier = jnp.cumsum(onehot, axis=0) - onehot
    slot_index = jnp.sum(earlier * onehot, axis=-1)
    slot_column = flat_ids * capacity + slot_index
    token_ids = jnp.arange(tokens_local * TOPK, dtype=jnp.int32) // TOPK
    slot_table = (
        jnp.full((ep_count * capacity,), tokens_local, jnp.int32).at[slot_column].set(token_ids)
    )
    col_width = expert_down.shape[2]
    arrived_rows = ep_count * capacity
    own_columns = lax.dynamic_slice_in_dim(normed, lax.axis_index("tp") * col_width, col_width, 1)
    padded = jnp.concatenate([own_columns, jnp.zeros((1, col_width), jnp.bfloat16)], axis=0)
    outgoing = padded[slot_table].reshape(ep_count, capacity, col_width)
    arrived = lax.all_to_all(outgoing, "ep", split_axis=0, concat_axis=0, tiled=True).reshape(
        arrived_rows, col_width
    )
    portion = lax.all_gather(arrived, "tp", axis=1, tiled=True)
    gate_part = expert_gate[0]
    up_part = expert_up[0]
    gate_pre = jnp.dot(portion, gate_part, preferred_element_type=jnp.float32)
    up_pre = jnp.dot(portion, up_part, preferred_element_type=jnp.float32)
    routed_hidden = (jax.nn.silu(gate_pre) * up_pre).astype(jnp.bfloat16)
    shared_hidden = (
        jax.nn.silu(jnp.dot(normed, shared_gate, preferred_element_type=jnp.float32))
        * jnp.dot(normed, shared_up, preferred_element_type=jnp.float32)
    ).astype(jnp.bfloat16)
    routed_part = expert_down[0]
    routed_sum = jnp.dot(
        lax.all_gather(routed_hidden, "tp", axis=1, tiled=True),
        routed_part,
        preferred_element_type=jnp.float32,
    )
    shared_sum = jnp.dot(
        lax.all_gather(shared_hidden, "tp", axis=1, tiled=True),
        shared_down,
        preferred_element_type=jnp.float32,
    )
    expert_rows = routed_sum.astype(jnp.bfloat16).reshape(ep_count, capacity, col_width)
    returned = lax.all_to_all(expert_rows, "ep", split_axis=0, concat_axis=0, tiled=True).reshape(
        arrived_rows, col_width
    )
    picked = returned[slot_column].reshape(tokens_local, TOPK, col_width).astype(jnp.float32)
    expert_output = (shared_sum + jnp.sum(picked * route_weight[:, :, None], axis=1)).astype(
        jnp.bfloat16
    )
    return (mixer_output, expert_output)


CHUNKS = 2
VMEM_LIMIT = 62 * 1024 * 1024
PARTS_BACK = 4
COLUMNS_X = 2


def place_of(slot, ring):
    half = ring // 2
    return 0 if slot == 0 else 2 * slot - 1 if slot <= half else 2 * (ring - slot)


def ring_position(index, ring):
    row, side = index // COLUMNS_X, index % COLUMNS_X
    return row + side * (ring - 1 - 2 * row)


def ring_index(position, ring):
    side = position // (ring // COLUMNS_X)
    return 2 * position + side * (2 * ring - 1 - 4 * position)


def remote(source, target, send, receive, device):
    return pltpu.make_async_remote_copy(
        src_ref=source,
        dst_ref=target,
        send_sem=send,
        recv_sem=receive,
        device_id=device,
        device_id_type=pl.DeviceIdType.MESH,
    )


def limit(direction, chunk, ring):
    return ring // 2 if direction == chunk else ring // 2 - 1


def slot_at(direction, distance, ring):
    return distance if direction == 0 else ring - distance


def layer_kernel(
    ring,
    rows_hbm,
    gain_hbm,
    ids_hbm,
    weight_hbm,
    mixer_hbm,
    mixer_gain_hbm,
    query_gain_hbm,
    key_gain_hbm,
    sink_hbm,
    gate_hbm,
    up_hbm,
    shared_gate_hbm,
    shared_up_hbm,
    query_hbm,
    key_hbm,
    value_hbm,
    w_out_hbm,
    down_hbm,
    shared_down_hbm,
    mixer_result,
    expert_result,
    rows_v,
    gain_v,
    ids_v,
    weight_v,
    mixer_gain_v,
    query_gain_v,
    key_gain_v,
    sink_v,
    mixer_all,
    hidden_all,
    shared_all,
    att_all,
    dense_all,
    tok,
    gate_v,
    up_v,
    shared_gate_v,
    shared_up_v,
    qkv_v,
    down_v,
    shared_down_v,
    out_cols,
    out_stage,
    scaled_v,
    heads_v,
    band_v,
    bias_v,
    ready,
    going,
    coming,
    load_sem,
    tok_send,
    ring_recv,
    sib_recv,
    mix_send,
    mix_recv,
    hid_send,
    hid_recv,
    sh_send,
    sh_recv,
    att_send,
    att_recv,
    dense_send,
    dense_recv,
    halo_send,
    halo_recv,
    wcol_send,
    wcol_recv,
    wring_send,
    wring_recv,
    back_send,
    back_recv,
):
    scope = jax.named_scope
    f32, bf16 = jnp.float32, jnp.bfloat16
    index, part = lax.axis_index("ep"), lax.axis_index("tp")
    far, core = part // 2, part % 2
    position = ring_position(index, ring)
    peer_index = [ring_index((position + k) % ring, ring) for k in range(ring)]
    peers = [(peer_index[k], part) for k in range(1, ring)]
    ahead, behind = peers[0], peers[-1]
    sib_part = 2 * far + 1 - core
    across_part = 2 * (1 - far) + core
    corner_part = 2 * (1 - far) + 1 - core
    sibling, across = (index, sib_part), (index, across_part)
    block, width = rows_v.shape
    half_width = width // 2
    piece = block // CHUNKS
    steps = ring // 2
    parts, rows_local, mixer_cols = mixer_all.shape
    pieces = rows_local // WINDOW
    out_width = down_v.shape[1]
    inner = hidden_all.shape[2]
    shared_width = shared_all.shape[2]
    head_rows = out_cols.shape[1]
    share_rows = head_rows // ring
    share_piece = share_rows // CHUNKS

    barrier = pltpu.get_barrier_semaphore()
    for device in peers + [sibling, across]:
        pl.semaphore_signal(barrier, inc=1, device_id=device, device_id_type=pl.DeviceIdType.MESH)


    def start(copy):
        copy.start()

    loads = {}

    def load(name, source, target):
        loads[name] = pltpu.make_async_copy(source, target, load_sem.at[len(loads)])
        loads[name].start()

    def load_qkv(source, first):
        target = qkv_v.at[:, pl.ds(first, source.shape[1])]
        pltpu.make_async_copy(source, target, load_sem.at[len(loads)]).start()

    own_cols = pl.ds(pl.multiple_of(part * out_width, out_width), out_width)
    load("rows", rows_hbm, rows_v)
    load("gain", gain_hbm, gain_v)
    load("mixer", mixer_hbm, mixer_all.at[part])
    load("shared_gate", shared_gate_hbm, shared_gate_v)
    load("shared_up", shared_up_hbm, shared_up_v)
    load("gate", gate_hbm, gate_v)
    load("up", up_hbm, up_v)
    load("ids", ids_hbm, ids_v)
    load("weight", weight_hbm, weight_v)
    load("mixer_gain", mixer_gain_hbm, mixer_gain_v)
    load("query_gain", query_gain_hbm, query_gain_v)
    load("key_gain", key_gain_hbm, key_gain_v)
    load("sink", sink_hbm, sink_v)
    query_cols, key_cols = query_hbm.shape[1], key_hbm.shape[1]
    load_qkv(query_hbm, 0)
    load_qkv(key_hbm, query_cols)
    load_qkv(value_hbm, query_cols + key_cols)
    loads["qkv"] = pltpu.make_async_copy(qkv_v, qkv_v, load_sem.at[len(loads)])
    load("out_own", w_out_hbm.at[:, own_cols], out_cols.at[part])
    load("down", down_hbm, down_v)
    load("shared_down", shared_down_hbm, shared_down_v)

    band_shape = (2 * WINDOW, WINDOW)
    relative = (
        lax.broadcasted_iota(jnp.int32, band_shape, 1)
        + WINDOW
        - lax.broadcasted_iota(jnp.int32, band_shape, 0)
    )
    bias_v[...] = jnp.where((relative >= 0) & (relative < WINDOW), 0.0, -jnp.inf)
    low = lax.broadcasted_iota(jnp.int32, (WINDOW, 2 * HEAD), 1) < HEAD

    with scope("norm"):
        loads["rows"].wait()
        loads["gain"].wait()
        value = rows_v[...].astype(f32)
        normed = (
            value
            * lax.rsqrt(jnp.mean(value * value, axis=-1, keepdims=True) + EPSILON)
            * gain_v[...]
        ).astype(bf16)
        tok[0, pl.ds(0, block), :] = normed[:, :half_width]
        tok[1, pl.ds(0, block), :] = normed[:, half_width:]
        loads["mixer"].wait()

    with scope("greet"):
        pl.semaphore_wait(barrier, ring + 1)

    def chunk_ref(half, slot, chunk):
        return tok.at[half, pl.ds(place_of(slot, ring) * block + chunk * piece, piece), :]

    def hop(direction, distance, chunk):
        start(
            remote(
                chunk_ref(core, slot_at(direction, distance - 1, ring) % ring, chunk),
                chunk_ref(core, slot_at(direction, distance, ring), chunk),
                tok_send.at[0],
                ring_recv.at[direction, distance - 1, chunk],
                ahead if direction == 0 else behind,
            )
        )

    def arrive(distance, k):
        for direction in range(2):
            chunk = k if direction == 0 else CHUNKS - 1 - k
            if distance > limit(direction, chunk, ring):
                continue
            here = chunk_ref(core, slot_at(direction, distance, ring), chunk)
            got = ring_recv.at[direction, distance - 1, chunk]
            remote(here, here, tok_send.at[0], got, sibling).wait_recv()
            if distance < limit(direction, chunk, ring):
                hop(direction, distance + 1, chunk)
            start(remote(here, here, tok_send.at[0], sib_recv.at[distance - 1], sibling))

    def swapped(distance):
        count = 2 if distance < steps else 1
        there = tok.at[1 - core, pl.ds((2 * distance - 1) * block, count * block), :]
        remote(there, there, tok_send.at[0], sib_recv.at[distance - 1], sibling).wait_recv()

    class Share:
        def __init__(self, view, send, receive):
            self.view, self.send, self.receive = view, send, receive

        def copy(self, owner, i, path, device):
            here = self.view(owner, i)
            return remote(here, here, self.send.at[0], self.receive.at[path, i], device)

        def to_across(self, i):
            start(self.copy(part, i, 0, across))

        def to_sibling(self, i):
            start(self.copy(part, i, 1, sibling))

        def both(self, i):
            self.to_across(i)
            self.to_sibling(i)

        def forward(self, i):
            self.copy(across_part, i, 0, sibling).wait_recv()
            start(self.copy(across_part, i, 1, sibling))

        def rest(self, i):
            self.copy(pl.ds(0, 2), i, 1, sibling).wait_recv()

    mixer = Share(
        lambda owner, i: mixer_all.at[owner, pl.ds(i * WINDOW, WINDOW), :], mix_send, mix_recv
    )
    shared = Share(lambda owner, i: shared_all.at[owner], sh_send, sh_recv)
    hidden = Share(
        lambda owner, i: hidden_all.at[owner, pl.ds(place_of(i, ring) * block, block), :],
        hid_send,
        hid_recv,
    )
    att = Share(
        lambda owner, i: att_all.at[owner, pl.ds(i * WINDOW, WINDOW), :], att_send, att_recv
    )

    for k in range(CHUNKS):
        for direction in range(2):
            hop(direction, 1, k if direction == 0 else CHUNKS - 1 - k)
    mixer.both(3)
    mixer.both(2)
    mixer.to_sibling(1)
    mixer.to_sibling(0)

    loads["ids"].wait()
    loads["weight"].wait()
    experts = lax.broadcasted_iota(jnp.int32, (ring, block), 0)
    dense = jnp.zeros((ring, block), f32)
    for k in range(TOPK):
        dense = dense + jnp.where(ids_v[k : k + 1, :] == experts, weight_v[k : k + 1, :], 0.0)
    dense_all[0] = dense
    for k in range(1, ring):
        start(
            remote(
                dense_all.at[0], dense_all.at[k], dense_send.at[0], dense_recv.at[0], peers[k - 1]
            )
        )

    def product(first, count, weights, columns):
        lower = tok[0, pl.ds(first, count), :]
        upper = tok[1, pl.ds(first, count), :]
        return jnp.dot(
            lower, weights[pl.ds(0, half_width), columns], preferred_element_type=f32
        ) + jnp.dot(
            upper, weights[pl.ds(half_width, half_width), columns], preferred_element_type=f32
        )

    with scope("c_shared"):
        loads["shared_gate"].wait()
        loads["shared_up"].wait()
        everything = pl.ds(0, shared_width)
        shared_all[part] = (
            jax.nn.silu(product(0, block, shared_gate_v, everything))
            * product(0, block, shared_up_v, everything)
        ).astype(bf16)
        shared.both(0)

    tile = 256

    def compute(slots, now):
        first = min(place_of(slot, ring) for slot in slots) * block
        count = len(slots) * block

        def one(j, carry):
            columns = pl.ds(pl.multiple_of(j * tile, tile), tile)
            hidden_all[part, pl.ds(first, count), columns] = (
                jax.nn.silu(product(first, count, gate_v, columns))
                * product(first, count, up_v, columns)
            ).astype(bf16)
            return carry

        lax.fori_loop(0, inner // tile, one, 0)
        for slot in slots:
            hidden.to_sibling(slot)
            if slot in now:
                hidden.to_across(slot)

    def project(i):
        rows = pl.ds(i * WINDOW, WINDOW)
        mixer.rest(i)
        squares = jnp.zeros((WINDOW, 1), f32)
        for owner in range(parts):
            columns = pl.ds(owner * mixer_cols, mixer_cols)
            value = mixer_all[owner, rows, :].astype(f32)
            squares = squares + jnp.sum(value * value, axis=1, keepdims=True)
            scaled_v[:, columns] = (value * mixer_gain_v[:, columns]).astype(bf16)
        raw = jnp.dot(scaled_v[...], qkv_v[...], preferred_element_type=f32)
        lanes = 2 * HEAD
        heads = heads_v.shape[0]
        gain = query_gain_v[...] * HEAD ** (-0.5)
        gain = jnp.concatenate([gain, gain], axis=1)
        for pair in range(heads // 2):
            two = raw[:, pair * lanes : (pair + 1) * lanes]
            square = two * two
            first_sum = jnp.sum(jnp.where(low, square, 0.0), axis=1, keepdims=True)
            second_sum = jnp.sum(jnp.where(low, 0.0, square), axis=1, keepdims=True)
            inverse = lax.rsqrt(jnp.where(low, first_sum, second_sum) / HEAD + EPSILON)
            two = two * inverse * gain
            heads_v[2 * pair, rows, :] = jnp.where(low, two, 0.0).astype(bf16)
            heads_v[2 * pair + 1, rows, :] = jnp.where(low, 0.0, two).astype(bf16)
        queries_end = heads * HEAD
        second = part // (parts // KV_HEADS)
        mine = low == (second == 0)

        def twice(columns):
            return jnp.where(mine, columns, pltpu.roll(columns, HEAD, 1))

        key = twice(raw[:, queries_end : queries_end + lanes])
        gain = jnp.concatenate([key_gain_v[...], key_gain_v[...]], axis=1)
        key = key * lax.rsqrt(jnp.mean(key * key, axis=1, keepdims=True) + EPSILON) * gain
        val = twice(raw[:, queries_end + lanes : queries_end + 2 * lanes])
        val = val * lax.rsqrt(squares / D + EPSILON)
        band_v[pl.ds(WINDOW + i * WINDOW, WINDOW), :] = jnp.concatenate(
            [key, val], axis=1
        ).astype(bf16)

    halo = band_v.at[pl.ds(0, WINDOW), :]

    def send_halo():
        start(
            remote(
                band_v.at[pl.ds(rows_local, WINDOW), :],
                halo,
                halo_send.at[0],
                halo_recv.at[0],
                ((index + 1) % ring, part),
            )
        )

    def wait_halo():
        remote(halo, halo, halo_send.at[0], halo_recv.at[0], sibling).wait_recv()

    def attend(i):
        rows = pl.ds(i * WINDOW, WINDOW)
        heads = heads_v.shape[0]
        keys = band_v[pl.ds(i * WINDOW, 2 * WINDOW), pl.ds(0, 2 * HEAD)]
        values = band_v[pl.ds(i * WINDOW, 2 * WINDOW), pl.ds(2 * HEAD, 2 * HEAD)]
        bias = bias_v[...]
        if i == 0:
            before = lax.broadcasted_iota(jnp.int32, band_shape, 0) < WINDOW
            bias = jnp.where(before & (index == 0), -jnp.inf, bias)
        scores = lax.dot_general(
            keys,
            heads_v[:, rows, :].reshape(heads * WINDOW, 2 * HEAD),
            (((1,), (1,)), ((), ())),
            preferred_element_type=f32,
        )
        columns = []
        for head in range(heads):
            masked = scores[:, head * WINDOW : (head + 1) * WINDOW] + bias
            sink = sink_v[:, head : head + 1]
            peak = jnp.maximum(jnp.max(masked, axis=0, keepdims=True), sink)
            exponent = jnp.exp(masked - peak)
            denominator = jnp.sum(exponent, axis=0, keepdims=True) + jnp.exp(sink - peak)
            columns.append((exponent * (1.0 / denominator)).astype(bf16))
        mixed = lax.dot_general(
            values[:, :HEAD],
            jnp.concatenate(columns, axis=1),
            (((0,), (0,)), ((), ())),
            preferred_element_type=f32,
        )
        for pair in range(heads // 2):
            first = 2 * pair * WINDOW
            two = jnp.concatenate(
                [mixed[:, first : first + WINDOW], mixed[:, first + WINDOW : first + 2 * WINDOW]],
                axis=0,
            )
            att_all[part, rows, pl.ds(pair * 2 * HEAD, 2 * HEAD)] = two.T.astype(bf16)

    chip_cols = 2 * out_width

    def spread_columns():
        start(
            remote(
                w_out_hbm.at[:, pl.ds(pl.multiple_of(sib_part * out_width, out_width), out_width)],
                out_cols.at[part],
                wcol_send.at[0],
                wcol_recv.at[0],
                sibling,
            )
        )
        mine = pl.ds(pl.multiple_of(index * share_rows, share_rows), share_rows)
        start(
            remote(
                w_out_hbm.at[
                    mine, pl.ds(pl.multiple_of((1 - far) * chip_cols, chip_cols), chip_cols)
                ],
                out_stage.at[mine, :],
                wcol_send.at[1],
                wcol_recv.at[1],
                across,
            )
        )

    def stage_ref(slot, chunk):
        owner = peer_index[(ring - slot) % ring]
        first = owner * share_rows + chunk * share_piece
        return out_stage.at[pl.ds(pl.multiple_of(first, share_piece), share_piece), :]

    def column_hop(direction, distance, chunk):
        here = stage_ref(slot_at(direction, distance - 1, ring) % ring, chunk)
        to = ahead if direction == 0 else behind
        start(remote(here, here, wring_send.at[0], wring_recv.at[distance - 1], to))

    def column_start():
        mine = out_stage.at[pl.ds(pl.multiple_of(index * share_rows, share_rows), share_rows), :]
        remote(mine, mine, wcol_send.at[1], wcol_recv.at[1], across).wait_recv()
        for chunk in range(CHUNKS):
            for direction in range(2):
                column_hop(direction, 1, chunk)

    def column_arrive(distance):
        count = 2 if distance < steps else 1
        here = out_stage.at[pl.ds(0, count * share_rows), :]
        remote(here, here, wring_send.at[0], wring_recv.at[distance - 1], sibling).wait_recv()
        for chunk in range(CHUNKS):
            for direction in range(2):
                if distance < limit(direction, chunk, ring):
                    column_hop(direction, distance + 1, chunk)

    def column_swap():
        start(
            remote(
                out_stage.at[
                    :, pl.ds(pl.multiple_of((1 - core) * out_width, out_width), out_width)
                ],
                out_cols.at[across_part],
                wcol_send.at[2],
                wcol_recv.at[2],
                sibling,
            )
        )

    def column_wait():
        loads["out_own"].wait()
        for i, owner in ((0, sib_part), (2, corner_part)):
            here = out_cols.at[owner]
            remote(here, here, wcol_send.at[i], wcol_recv.at[i], sibling).wait_recv()

    def finish_mixer(i):
        rows = pl.ds(i * WINDOW, WINDOW)
        total = jnp.dot(
            att_all[across_part, rows, :],
            out_stage[:, pl.ds(pl.multiple_of(core * out_width, out_width), out_width)],
            preferred_element_type=f32,
        )
        total = total + jnp.dot(
            att_all[part, rows, :], out_cols[part], preferred_element_type=f32
        )
        att.rest(i)
        for owner in (sib_part, corner_part):
            total = total + jnp.dot(
                att_all[owner, rows, :], out_cols[owner], preferred_element_type=f32
            )
        mixer_result[rows, :] = total.astype(bf16)

    diagonal = lax.broadcasted_iota(jnp.int32, (block, block), 0) == lax.broadcasted_iota(
        jnp.int32, (block, block), 1
    )

    def weight_column(slot):
        row = dense_all[slot, pl.ds(index, 1), :]
        return jnp.sum(jnp.where(diagonal, row, 0.0), axis=1, keepdims=True)

    def weighted(slots):
        first = min(place_of(slot, ring) for slot in slots) * block
        count = len(slots) * block

        def share(owner):
            return jnp.dot(
                hidden_all[owner, pl.ds(first, count), :],
                down_v[pl.ds(pl.multiple_of(owner * inner, inner), inner), :],
                preferred_element_type=f32,
            )

        total = share(part) + share(across_part)
        for slot in slots:
            hidden.rest(slot)
        total = total + share(sib_part) + share(corner_part)
        rounded = total.astype(bf16).astype(f32)
        ordered = sorted(slots, key=lambda slot: place_of(slot, ring))
        ready[pl.ds(first, count), :] = rounded * jnp.concatenate(
            [weight_column(slot) for slot in ordered], axis=0
        )

    def own_rows():
        weighted([0])
        shared.rest(0)
        own = ready[pl.ds(0, block), :]
        for owner in range(parts):
            own = own + jnp.dot(
                shared_all[owner],
                shared_down_v[pl.ds(owner * shared_width, shared_width), :],
                preferred_element_type=f32,
            )
        ready[pl.ds(0, block), :] = own

    back_rows = block // PARTS_BACK

    def longest(direction, part_back):
        return limit(direction, part_back * CHUNKS // PARTS_BACK, ring)

    def back_wait(direction, distance, b):
        here = coming.at[direction, distance, pl.ds(b * back_rows, back_rows), :]
        got = back_recv.at[direction, distance - 1, b]
        remote(here, here, back_send.at[0], got, ahead).wait_recv()
        return here[...].astype(f32)

    def push(distance, long, directions=(0, 1)):
        for b in range(PARTS_BACK):
            for direction in directions:
                if (longest(direction, b) == steps) != long:
                    continue
                slot = slot_at(1 - direction, distance, ring)
                first = place_of(slot, ring) * block + b * back_rows
                value = ready[pl.ds(first, back_rows), :]
                hops = 1
                if long and distance == steps:
                    hops = 2
                elif long and distance == steps - 2:
                    hops = 2
                    value = value + back_wait(direction, distance + 1, b)
                    value = value + back_wait(direction, distance + 2, b)
                elif not long and distance < steps - 1:
                    value = value + back_wait(direction, distance + 1, b)
                rows = pl.ds(b * back_rows, back_rows)
                at = direction * steps + distance - 1
                going[at, rows, :] = value.astype(bf16)
                start(
                    remote(
                        going.at[at, rows, :],
                        coming.at[direction, distance, rows, :],
                        back_send.at[0],
                        back_recv.at[direction, distance - 1, b],
                        peers[hops - 1 if direction == 0 else -hops],
                    )
                )

    def finish_expert(b):
        rows = pl.ds(b * back_rows, back_rows)
        total = ready[rows, :]
        for direction in range(2):
            total = total + back_wait(direction, 1, b)
            if longest(direction, b) == steps:
                total = total + back_wait(direction, 2, b)
        expert_result[rows, :] = total.astype(bf16)

    with scope("c_h0"):
        loads["gate"].wait()
        loads["up"].wait()
        compute([0], [])
    spread_columns()
    mixer.to_across(1)
    mixer.to_across(0)
    with scope("A1c0"):
        arrive(1, 0)
    with scope("fwd_m3"):
        mixer.forward(3)
    with scope("A1c1"):
        arrive(1, 1)
    with scope("fwd_m2"):
        mixer.forward(2)
    with scope("w_qkv"):
        for name in ("mixer_gain", "query_gain", "key_gain", "sink", "qkv"):
            loads[name].wait()
    with scope("qkv3"):
        project(3)
        send_halo()
    with scope("S1"):
        swapped(1)
    with scope("c_h1"):
        compute([1, ring - 1], [1, ring - 1])
    with scope("A2c0"):
        arrive(2, 0)
    with scope("qkv2"):
        project(2)
    with scope("att3"):
        attend(3)
        att.to_sibling(3)
    with scope("fwd_sh_m1"):
        shared.forward(0)
        mixer.forward(1)
    with scope("A2c1"):
        arrive(2, 1)
    with scope("S2"):
        swapped(2)
    with scope("c_h2"):
        compute([2, ring - 2], [2])
    with scope("A3c0"):
        arrive(3, 0)
    with scope("fwd_m0"):
        mixer.forward(0)
    with scope("qkv1"):
        project(1)
    with scope("att2"):
        attend(2)
        att.to_sibling(2)
    with scope("A3c1"):
        arrive(3, 1)
    with scope("w0"):
        column_start()
    with scope("fwd_h1"):
        hidden.forward(1)
    with scope("qkv0"):
        project(0)
    with scope("S3"):
        swapped(3)
    with scope("c_h3"):
        compute([3], [3])
        compute([ring - 3], [ring - 3])
    with scope("A4"):
        arrive(4, 0)
    with scope("w1"):
        column_arrive(1)
    with scope("fwd_h7"):
        hidden.forward(ring - 1)
    with scope("att1"):
        attend(1)
        att.to_sibling(1)
    with scope("halo"):
        wait_halo()
    with scope("att0"):
        attend(0)
        att.to_sibling(0)
    with scope("S4"):
        swapped(4)
    with scope("c_h4"):
        compute([4], [4])
    hidden.to_across(ring - 2)
    hidden.to_across(0)
    for i in (3, 2, 1, 0):
        att.to_across(i)
    with scope("fwd_h2"):
        hidden.forward(2)
    with scope("w_dense"):
        loads["down"].wait()
        loads["shared_down"].wait()
        here = dense_all.at[pl.ds(1, ring - 1)]
        remote(here, here, dense_send.at[0], dense_recv.at[0], sibling).wait_recv()
    with scope("down1"):
        weighted([1, ring - 1])
        push(1, True)
    with scope("w2"):
        column_arrive(2)
    with scope("down2"):
        weighted([2])
    with scope("fwd_h3"):
        hidden.forward(3)
    with scope("down3"):
        weighted([3])
        push(3, False, (1,))
        push(3, True, (1,))
    with scope("fwd_h5"):
        hidden.forward(ring - 3)
    with scope("w3"):
        column_arrive(3)
    with scope("down5"):
        weighted([ring - 3])
        push(3, False, (0,))
        push(3, True, (0,))
    with scope("fwd_h4"):
        hidden.forward(4)
    with scope("push2s1"):
        push(2, False, (1,))
    with scope("down4"):
        weighted([4])
        push(4, True)
    with scope("fwd_h6"):
        hidden.forward(ring - 2)
    with scope("w4"):
        column_arrive(4)
        column_swap()
    with scope("down6"):
        weighted([ring - 2])
    with scope("push1s1"):
        push(1, False, (1,))
    with scope("push2s0"):
        push(2, False, (0,))
    with scope("fwd_h0"):
        hidden.forward(0)
    with scope("push2l1"):
        push(2, True, (1,))
    with scope("push2l0"):
        push(2, True, (0,))
    with scope("push1s0"):
        push(1, False, (0,))
    with scope("fwd_a2"):
        att.forward(3)
        att.forward(2)
    with scope("own"):
        own_rows()
    with scope("fwd_a1"):
        att.forward(1)
    with scope("out3"):
        column_wait()
        finish_mixer(3)
    with scope("out2"):
        finish_mixer(2)
    with scope("fwd_a0"):
        att.forward(0)
    with scope("out1"):
        finish_mixer(1)
    with scope("out0"):
        finish_mixer(0)
    with scope("fin_exp"):
        for b in range(PARTS_BACK):
            finish_expert(b)
    with scope("w_end"):
        for ref, send in (
            (tok.at[:, pl.ds(0, (ring - 1) * block), :], tok_send.at[0]),
            (mixer_all.at[pl.ds(0, parts - 1)], mix_send.at[0]),
            (hidden_all.at[pl.ds(0, parts - 1)], hid_send.at[0]),
            (shared_all.at[pl.ds(0, parts - 1)], sh_send.at[0]),
            (att_all.at[pl.ds(0, parts - 1)], att_send.at[0]),
            (dense_all.at[pl.ds(0, ring - 1)], dense_send.at[0]),
            (halo, halo_send.at[0]),
            (out_cols.at[part], wcol_send.at[0]),
            (out_stage.at[pl.ds(0, share_rows), :], wcol_send.at[1]),
            (out_cols.at[part], wcol_send.at[2]),
            (out_stage.at[pl.ds(0, (ring - 1) * share_rows), :], wring_send.at[0]),
            (going.at[pl.ds(0, ring - 1)], back_send.at[0]),
        ):
            remote(ref, ref, send, halo_recv.at[0], sibling).wait_send()


def settle_kernel(mixer_in, expert_in, mixer_out, expert_out, sem):
    copies = [
        pltpu.make_async_copy(mixer_in, mixer_out, sem.at[0]),
        pltpu.make_async_copy(expert_in, expert_out, sem.at[1]),
    ]
    for copy in copies:
        copy.start()
    for copy in copies:
        copy.wait()


def shards(
    mixer_input,
    mixer_gain,
    w_query,
    w_key,
    w_value,
    query_gain,
    key_gain,
    sink_logit,
    w_output,
    expert_input,
    expert_gain,
    route_ids,
    route_weight,
    expert_gate,
    expert_up,
    expert_down,
    shared_gate,
    shared_up,
    shared_down,
):
    ring = lax.axis_size("ep")
    parts = lax.axis_size("tp")
    rows_local, mixer_cols = mixer_input.shape
    tokens_local, width = expert_input.shape
    hidden_width = expert_gate.shape[2]
    shared_width = shared_gate.shape[1]
    out_width = expert_down.shape[2]
    head_width = w_query.shape[1]
    pieces = rows_local // WINDOW
    half = ring // 2
    hbm = pl.BlockSpec(memory_space=pl.ANY)
    bf16, f32 = jnp.bfloat16, jnp.float32
    vm = pltpu.VMEM

    dma = pltpu.SemaphoreType.DMA
    outputs = pl.pallas_call(
        functools.partial(layer_kernel, ring),
        out_shape=(vm((rows_local, out_width), bf16), vm((tokens_local, out_width), bf16)),
        in_specs=[hbm] * 19,
        out_specs=(pl.BlockSpec(memory_space=vm),) * 2,
        scratch_shapes=[
            vm((tokens_local, width), bf16),
            vm((1, width), f32),
            vm((TOPK, tokens_local), jnp.int32),
            vm((TOPK, tokens_local), f32),
            vm((1, parts * mixer_cols), f32),
            vm((1, HEAD), f32),
            vm((1, HEAD), f32),
            vm((1, sink_logit.shape[0]), f32),
            vm((parts, rows_local, mixer_cols), bf16),
            vm((parts, ring * tokens_local, hidden_width), bf16),
            vm((parts, tokens_local, shared_width), bf16),
            vm((parts, rows_local, head_width), bf16),
            vm((ring, ring, tokens_local), f32),
            vm((2, ring * tokens_local, width // 2), bf16),
            vm((width, hidden_width), bf16),
            vm((width, hidden_width), bf16),
            vm((width, shared_width), bf16),
            vm((width, shared_width), bf16),
            vm((width, head_width + w_key.shape[1] + w_value.shape[1]), bf16),
            vm(expert_down.shape[1:], bf16),
            vm(shared_down.shape, bf16),
            vm((parts, head_width, out_width), bf16),
            vm((head_width, 2 * out_width), bf16),
            vm((WINDOW, parts * mixer_cols), bf16),
            vm((head_width // HEAD, rows_local, 2 * HEAD), bf16),
            vm((WINDOW + rows_local, 4 * HEAD), bf16),
            vm((2 * WINDOW, WINDOW), f32),
            vm((ring * tokens_local, out_width), f32),
            vm((2 * half, tokens_local, out_width), bf16),
            vm((2, half + 1, tokens_local, out_width), bf16),
            dma((17,)),
            dma((1,)),
            dma((2, half, CHUNKS)),
            dma((half,)),
            dma((1,)),
            dma((2, pieces)),
            dma((1,)),
            dma((2, ring)),
            dma((1,)),
            dma((2, 1)),
            dma((1,)),
            dma((2, pieces)),
            dma((1,)),
            dma((1,)),
            dma((1,)),
            dma((1,)),
            dma((3,)),
            dma((3,)),
            dma((1,)),
            dma((half,)),
            dma((1,)),
            dma((2, half, PARTS_BACK)),
        ],
        compiler_params=pltpu.CompilerParams(
            collective_id=0, has_side_effects=True, vmem_limit_bytes=VMEM_LIMIT
        ),
        name="layer",
    )(
        expert_input,
        expert_gain[None, :],
        route_ids.T,
        route_weight.T,
        mixer_input,
        mixer_gain[None, :],
        query_gain[None, :],
        key_gain[None, :],
        sink_logit[None, :],
        expert_gate[0],
        expert_up[0],
        shared_gate,
        shared_up,
        w_query,
        w_key,
        w_value,
        w_output,
        expert_down[0],
        shared_down,
    )
    return pl.pallas_call(
        settle_kernel,
        out_shape=tuple(jax.ShapeDtypeStruct(o.shape, o.dtype) for o in outputs),
        in_specs=[pl.BlockSpec(memory_space=vm)] * 2,
        out_specs=(hbm,) * 2,
        scratch_shapes=[dma((2,))],
        compiler_params=pltpu.CompilerParams(vmem_limit_bytes=1024 * 1024),
        name="settle",
    )(*outputs)


def plan(*arrays):
    route_ids = arrays[11]
    capacity = 2 * route_ids.size // lax.axis_size("ep")
    whole_blocks = capacity >= route_ids.shape[0]
    fits = lax.axis_size("ep") == 8 and lax.axis_size("tp") == 4
    if whole_blocks and fits and arrays[0].shape[0] == 4 * WINDOW:
        return shards(*arrays)
    return shards_routed(*arrays)


def solution(mesh):
    in_specs = (
        P("ep", "tp"),
        P(),
        P(None, "tp"),
        P(),
        P(),
        P(),
        P(),
        P("tp"),
        P("tp", None),
        P("ep", None),
        P(),
        P("ep", None),
        P("ep", None),
        P("ep", None, "tp"),
        P("ep", None, "tp"),
        P("ep", None, "tp"),
        P(None, "tp"),
        P(None, "tp"),
        P(None, "tp"),
    )
    out_specs = (P("ep", "tp"), P("ep", "tp"))
    return jax.shard_map(plan, mesh=mesh, in_specs=in_specs, out_specs=out_specs, check_vma=False)
```
